32 devices in a mesh: sp: 4 (over z), fs: 4 (over y, x), tp: 2 (over core).
Axes of the slice: x: 2, y: 2, z: 4, core: 2. Of those that a mesh axis runs over, the one named last changes fastest.
Arguments:
- tokens: bfloat16 [4, 512, 4096], P('fs', 'sp'), may hold values from -6 to 6
- norm_gain: float32 [4096], replicated, may hold values from 0.1 to 1.9
- pool_proj: bfloat16 [4096, 1024], P(('sp', 'fs'), 'tp'), may hold values from -0.09375 to 0.09375
- query_proj: bfloat16 [4096, 1024], P(('sp', 'fs'), 'tp'), may hold values from -0.09375 to 0.09375
- key_proj: bfloat16 [4096, 1024], P(('sp', 'fs'), 'tp'), may hold values from -0.09375 to 0.09375
- value_proj: bfloat16 [4096, 1024], P(('sp', 'fs'), 'tp'), may hold values from -0.09375 to 0.09375
- pool_map: bfloat16 [4, 256, 256], replicated, may hold values from -0.375 to 0.375
- pool_scale: float32 [1024], replicated, may hold values from 0.1 to 1.9
- decay_rate: float32 [4], P('tp'), may hold values from 2e-05 to 0.034
- start_state: float32 [4, 4, 256, 256], P('fs', 'tp', 'sp'), may hold values from -96 to 96
- pool_back: bfloat16 [1024, 4096], P('tp', ('sp', 'fs')), may hold values from -0.125 to 0.125
- retention_back: bfloat16 [1024, 4096], P('tp', ('sp', 'fs')), may hold values from -0.125 to 0.125
Outputs:
- mixed: bfloat16 [4, 512, 4096], P('fs', ('sp', 'tp'))
The draws below stay inside these ranges and needn't reach their ends.
All inputs are finite; a program needn't handle non-finite values.
Results may differ from the reference program's by a relative error of at most 0.014.
Values may be sent and summed in bfloat16 or wider, within the bound.
A program may use at most 128 MiB of HBM per device.

```python
import jax
import jax.numpy as jnp
from jax import lax

DMODEL = 4096
GROUPS = 4
GROUP_DIM = 256
RET_HEADS = 4
HEAD_DIM = 256
BLOCK = 128
HALO = 16
POOL_WIDTH = 1024
RET_WIDTH = 1024
SEQS = 4
SEQ_LEN = 512


def draw_decay_rate(key, part):
    order_key, level_key = jax.random.split(jax.random.fold_in(key, 7))
    order = jax.random.permutation(order_key, RET_HEADS)
    quick = order < RET_HEADS // 2
    level = jax.random.uniform(level_key, (RET_HEADS,), jnp.float32)
    quick_rate = jnp.exp(jnp.log(0.01) + level * (jnp.log(1.0 / 30.0) - jnp.log(0.01)))
    slow_rate = jnp.exp(jnp.log(2e-05) + level * (jnp.log(0.00012) - jnp.log(2e-05)))
    return jnp.where(quick, quick_rate, slow_rate).astype(jnp.float32)


def levels(rng, dims, cuts, smallest, high):
    factor_of = 1.0
    for dim, parts in cuts:
        steps = jax.random.uniform(jax.random.fold_in(jax.random.fold_in(rng, 6), dim), (parts,), jnp.float32, smallest / len(cuts), high / len(cuts))
        factor_of = factor_of * jnp.repeat(jnp.exp(steps), dims[dim] // parts).reshape((-1,) + (1,) * (len(dims) - 1 - dim))
    return factor_of


def normal_values(stream_key, dims, spread, most, cuts=(), held_as=jnp.bfloat16):
    drawn = jax.random.normal(stream_key, dims, jnp.float32) * spread
    if len(cuts) > 0:
        drawn = levels(stream_key, dims, cuts, -0.22, 0.18) * drawn
    return jnp.clip(drawn, min=-most, max=most).astype(held_as)


def setup_inputs(seed: int = 0) -> dict:
    streams_of = jax.random.split(jax.random.key(seed), 13)
    tokens = normal_values(streams_of[0], (SEQS, SEQ_LEN, DMODEL), 1.0, 6.0, ((0, 4), (1, 4)))
    norm_gain = jnp.clip(1.0 + 0.18 * jax.random.normal(streams_of[1], (DMODEL,), jnp.float32), 0.1, 1.9)
    pool_proj = normal_values(streams_of[2], (DMODEL, POOL_WIDTH), DMODEL ** -0.5, 0.09375, ((0, 16), (1, 2)))
    query_proj = normal_values(streams_of[3], (DMODEL, RET_WIDTH), DMODEL ** -0.5, 0.09375, ((0, 16), (1, 2)))
    key_proj = normal_values(streams_of[4], (DMODEL, RET_WIDTH), DMODEL ** -0.5, 0.09375, ((0, 16), (1, 2)))
    value_proj = normal_values(streams_of[5], (DMODEL, RET_WIDTH), DMODEL ** -0.5, 0.09375, ((0, 16), (1, 2)))
    pool_map = normal_values(streams_of[6], (GROUPS, GROUP_DIM, GROUP_DIM), GROUP_DIM ** -0.5, 0.375)
    pool_scale = jnp.clip(1.0 + 0.18 * jax.random.normal(streams_of[7], (POOL_WIDTH,), jnp.float32), 0.1, 1.9)
    decay_rate = draw_decay_rate(jax.random.fold_in(streams_of[12], 71), 0)
    start_state = normal_values(streams_of[9], (SEQS, RET_HEADS, HEAD_DIM, HEAD_DIM), 16.0, 96.0, ((0, 4), (1, 2), (2, 4)), jnp.float32)
    pool_back = normal_values(streams_of[10], (POOL_WIDTH, DMODEL), (POOL_WIDTH + RET_WIDTH) ** -0.5, 0.125, ((0, 2), (1, 16)))
    retention_back = normal_values(streams_of[11], (RET_WIDTH, DMODEL), (POOL_WIDTH + RET_WIDTH) ** -0.5, 0.125, ((0, 2), (1, 16)))
    return {"tokens": tokens, "norm_gain": norm_gain, "pool_proj": pool_proj, "query_proj": query_proj, "key_proj": key_proj, "value_proj": value_proj, "pool_map": pool_map, "pool_scale": pool_scale, "decay_rate": decay_rate, "start_state": start_state, "pool_back": pool_back, "retention_back": retention_back}


eps = 1e-06
rope_base = 10000.0
highest_precision = lax.Precision.HIGHEST
window_list = (2, 4, 8, 16)

def rotate(values, positions):
    half_dim = values.shape[-1] // 2
    inv_freq = 1.0 / rope_base ** jnp.linspace(0.0, 1.0, half_dim, dtype=jnp.float32)
    angles = positions.astype(jnp.float32)[:, None] * inv_freq[None, :]
    cosine = jnp.cos(angles)[:, None, :]
    sine = jnp.sin(angles)[:, None, :]
    first_half = values[..., :half_dim]
    second_half = values[..., half_dim:]
    return jnp.concatenate([first_half * cosine - second_half * sine, first_half * sine + second_half * cosine], axis=-1)

def trailing_sums(extended, length):
    begin = extended.shape[0] - length
    running = extended[begin:]
    results = []
    for behind in range(1, 16):
        running = running + extended[begin - behind:begin - behind + length]
        if behind + 1 in window_list:
            results.append(running)
    return results

def reshape_blocks(array):
    return array.reshape((array.shape[0] // BLOCK, BLOCK) + array.shape[1:])

def block_retention(queries, keys_in, values_in, decay_rate, initial):
    length, head_count, head_dim = queries.shape
    within = jnp.arange(BLOCK, dtype=jnp.float32)
    distance = within[:, None] - within[None, :]
    decay_mask = jnp.where(distance[None] >= 0, jnp.exp(-jnp.maximum(distance, 0.0)[None] * decay_rate[:, None, None]), 0.0)
    query_decay_factor = jnp.exp(-(within + 1.0)[:, None] * decay_rate[None, :])
    key_decay_factor = jnp.exp(-(BLOCK - 1.0 - within)[:, None] * decay_rate[None, :])
    block_decay_factor = jnp.exp(-BLOCK * decay_rate)

    def advance(state_carry, inputs):
        block_queries, block_keys, block_values = inputs
        scores = jnp.einsum('ihk,jhk->hij', block_queries, block_keys, precision=highest_precision) * decay_mask
        inside = jnp.einsum('hij,jhv->ihv', scores, block_values, precision=highest_precision)
        across_blocks = jnp.einsum('bzy,zyx->bzx', block_queries * query_decay_factor[:, :, None], state_carry, precision=highest_precision)
        state_carry = state_carry * block_decay_factor[:, None, None] + jnp.einsum('flm,fld->lmd', block_keys * key_decay_factor[:, :, None], block_values, precision=highest_precision)
        return (state_carry, inside + across_blocks)
    final_state, outputs = lax.scan(advance, initial, (reshape_blocks(queries), reshape_blocks(keys_in), reshape_blocks(values_in)))
    return (outputs.reshape(length, head_count, values_in.shape[-1]), final_state)

def reference(tokens, norm_gain, pool_proj, query_proj, key_proj, value_proj, pool_map, pool_scale, decay_rate, start_state, pool_back, retention_back):
    weights_back = jnp.concatenate([pool_back, retention_back], axis=0)

    def one_sequence(operands):
        sequence, initial = operands
        floats = sequence.astype(jnp.float32)
        normed = (floats * lax.rsqrt(lax.optimization_barrier(jnp.mean(floats * floats, axis=-1, keepdims=True)) + eps) * norm_gain).astype(jnp.bfloat16)
        pool_in = jnp.dot(normed, pool_proj, preferred_element_type=jnp.float32).astype(jnp.bfloat16)
        query_bf = jnp.dot(normed, query_proj, preferred_element_type=jnp.float32).astype(jnp.bfloat16)
        key_bf = jnp.dot(normed, key_proj, preferred_element_type=jnp.float32).astype(jnp.bfloat16)
        value_bf = jnp.dot(normed, value_proj, preferred_element_type=jnp.float32).astype(jnp.bfloat16)
        positions = jnp.arange(SEQ_LEN, dtype=jnp.int32)
        extended = jnp.concatenate([jnp.zeros((HALO, POOL_WIDTH), jnp.float32), pool_in.astype(jnp.float32)], axis=0)
        sums_all = trailing_sums(extended, SEQ_LEN)
        pieces = []
        for group_idx in range(GROUPS):
            lower = group_idx * GROUP_DIM
            chosen = sums_all[group_idx][:, lower:lower + GROUP_DIM]
            counts = jnp.minimum(window_list[group_idx], positions + 1).astype(jnp.float32)
            inputs = extended[HALO:, lower:lower + GROUP_DIM]
            differ = (chosen / counts[:, None] - inputs).astype(jnp.bfloat16)
            pieces.append(jnp.dot(differ, pool_map[group_idx], preferred_element_type=jnp.float32))
        pool_out = (jnp.concatenate(pieces, axis=1) * pool_scale).astype(jnp.bfloat16)
        queries = rotate(query_bf.astype(jnp.float32).reshape(SEQ_LEN, RET_HEADS, HEAD_DIM), positions)
        keys_in = rotate(key_bf.astype(jnp.float32).reshape(SEQ_LEN, RET_HEADS, HEAD_DIM), positions) * HEAD_DIM ** (-0.5)
        values_in = value_bf.astype(jnp.float32).reshape(SEQ_LEN, RET_HEADS, HEAD_DIM)
        retained_output, final_state = block_retention(queries, keys_in, values_in, decay_rate, initial)
        retained_output = retained_output * lax.rsqrt(lax.optimization_barrier(jnp.mean(retained_output * retained_output, axis=-1, keepdims=True)) + eps)
        ret_out = retained_output.reshape(SEQ_LEN, RET_WIDTH).astype(jnp.bfloat16)
        joined = jnp.concatenate([pool_out, ret_out], axis=1)
        return jnp.dot(joined, weights_back, preferred_element_type=jnp.float32).astype(jnp.bfloat16)
    return lax.map(one_sequence, (tokens, start_state))
```

```python
import numpy as np
from jax.experimental import pallas as pl
from jax.experimental.pallas import tpu as pltpu

import jax
import jax.numpy as jnp
from jax import lax
from jax.sharding import PartitionSpec as P

GROUPS = 4
BLOCK = 128
HALO = 16


eps = 1e-06
rope_base = 10000.0
highest_precision = lax.Precision.HIGHEST
window_list = (2, 4, 8, 16)


def shortened(x):
    return jax.tree.map(lambda a: a.astype(jnp.bfloat16) if a.dtype == jnp.float32 else a, x)


def shifted(x, axis, by):
    devices = lax.axis_size(axis)
    pairs = [(i, i + by) for i in range(devices) if 0 <= i + by < devices]
    return lax.ppermute(x, axis, pairs)


def carried_in(value, axis, join, neutral):
    count, mine = (lax.axis_size(axis), lax.axis_index(axis))
    pieces = jax.tree.map(lambda part: lax.all_gather(part, axis), value)
    running = jax.tree.map(
        lambda part, zero: jnp.full_like(part, 0) + jnp.asarray(zero, part.dtype), value, neutral
    )

    def turn(position, running):
        longer = join(running, jax.tree.map(lambda part: part[position], pieces))
        return jax.tree.map(lambda new, old: jnp.where(position < mine, new, old), longer, running)

    return lax.fori_loop(0, count - 1, turn, running)


def rotate(values, positions):
    half_dim = values.shape[-1] // 2
    inv_freq = 1.0 / rope_base ** jnp.linspace(0.0, 1.0, half_dim, dtype=jnp.float32)
    angles = positions.astype(jnp.float32)[:, None] * inv_freq[None, :]
    cosine = jnp.cos(angles)[:, None, :]
    sine = jnp.sin(angles)[:, None, :]
    first_half = values[..., :half_dim]
    second_half = values[..., half_dim:]
    return jnp.concatenate(
        [first_half * cosine - second_half * sine, first_half * sine + second_half * cosine],
        axis=-1,
    )


def trailing_sums(extended, length):
    begin = extended.shape[0] - length
    running = extended[begin:]
    results = []
    for behind in range(1, 16):
        running = running + extended[begin - behind : begin - behind + length]
        if behind + 1 in window_list:
            results.append(running)
    return results


def reshape_blocks(array):
    return array.reshape((array.shape[0] // BLOCK, BLOCK) + array.shape[1:])


def block_retention(queries, keys_in, values_in, decay_rate, initial):
    length, head_count, head_dim = queries.shape
    within = jnp.arange(BLOCK, dtype=jnp.float32)
    distance = within[:, None] - within[None, :]
    decay_mask = jnp.where(
        distance[None] >= 0,
        jnp.exp(-jnp.maximum(distance, 0.0)[None] * decay_rate[:, None, None]),
        0.0,
    )
    query_decay_factor = jnp.exp(-(within + 1.0)[:, None] * decay_rate[None, :])
    key_decay_factor = jnp.exp(-(BLOCK - 1.0 - within)[:, None] * decay_rate[None, :])
    block_decay_factor = jnp.exp(-BLOCK * decay_rate)

    def advance(state_carry, inputs):
        block_queries, block_keys, block_values = inputs
        scores = (
            jnp.einsum("ihk,jhk->hij", block_queries, block_keys, precision=highest_precision)
            * decay_mask
        )
        inside = jnp.einsum("hij,jhv->ihv", scores, block_values, precision=highest_precision)
        across_blocks = jnp.einsum(
            "bzy,zyx->bzx",
            block_queries * query_decay_factor[:, :, None],
            state_carry,
            precision=highest_precision,
        )
        state_carry = state_carry * block_decay_factor[:, None, None] + jnp.einsum(
            "flm,fld->lmd",
            block_keys * key_decay_factor[:, :, None],
            block_values,
            precision=highest_precision,
        )
        return (state_carry, inside + across_blocks)

    final_state, outputs = lax.scan(
        advance,
        initial,
        (reshape_blocks(queries), reshape_blocks(keys_in), reshape_blocks(values_in)),
    )
    return (outputs.reshape(length, head_count, values_in.shape[-1]), final_state)


def combine_states(earlier, latter):
    return (earlier[0] * latter[0], latter[0][:, None, None] * earlier[1] + latter[1])


def on_device(
    tokens,
    norm_gain,
    pool_proj,
    query_proj,
    key_proj,
    value_proj,
    pool_map,
    pool_scale,
    decay_rate,
    start_state,
    pool_back,
    retention_back,
):
    sequence = tokens[0]
    length = sequence.shape[0]
    tp_index = lax.axis_index("tp")
    sp_index = lax.axis_index("sp")
    tp_count = lax.axis_size("tp")
    floats = sequence.astype(jnp.float32)
    normed = (
        floats * lax.rsqrt(jnp.mean(floats * floats, axis=-1, keepdims=True) + eps) * norm_gain
    ).astype(jnp.bfloat16)
    group_normed = lax.all_gather(normed, "fs", axis=0, tiled=True)
    quarters = (
        lax.all_to_all(pool_proj, "fs", split_axis=1, concat_axis=0, tiled=True),
        lax.all_to_all(query_proj, "fs", split_axis=1, concat_axis=0, tiled=True),
        lax.all_to_all(key_proj, "fs", split_axis=1, concat_axis=0, tiled=True),
        lax.all_to_all(value_proj, "fs", split_axis=1, concat_axis=0, tiled=True),
    )
    pieces = (
        lax.all_gather(quarters[0], "sp", axis=0, tiled=True),
        lax.all_gather(quarters[1], "sp", axis=0, tiled=True),
        lax.all_gather(quarters[2], "sp", axis=0, tiled=True),
        lax.all_gather(quarters[3], "sp", axis=0, tiled=True),
    )
    partial_cols = tuple(
        (jnp.dot(group_normed, piece_w, preferred_element_type=jnp.float32) for piece_w in pieces)
    )
    rounded = tuple((result.astype(jnp.bfloat16) for result in partial_cols))
    pool_in, query_bf, key_bf, value_bf = jax.tree.map(
        lambda part, own: part.astype(own.dtype),
        lax.all_to_all(shortened(rounded), "fs", split_axis=0, concat_axis=1, tiled=True),
        rounded,
    )
    positions = jnp.arange(length, dtype=jnp.int32) + sp_index * length
    before = shifted(pool_in[length - HALO :], "sp", 1)
    extended = jnp.concatenate([before, pool_in], axis=0).astype(jnp.float32)
    stacked = jnp.stack(trailing_sums(extended, length))
    local_groups = GROUPS // tp_count
    channels = pool_in.shape[1]
    group_dim = channels // local_groups
    group_maps = lax.dynamic_slice_in_dim(pool_map, tp_index * local_groups, local_groups, 0)
    scales = lax.dynamic_slice_in_dim(pool_scale, tp_index * channels, channels, 0)
    windows = jnp.array(window_list, dtype=jnp.int32)
    pieces = []
    for group_idx in range(local_groups):
        chosen_group = tp_index * local_groups + group_idx
        lower = group_idx * group_dim
        chosen = lax.dynamic_index_in_dim(stacked, chosen_group, 0, keepdims=False)[
            :, lower : lower + group_dim
        ]
        counts = jnp.minimum(windows[chosen_group], positions + 1).astype(jnp.float32)
        inputs = extended[HALO:, lower : lower + group_dim]
        differ = (chosen / counts[:, None] - inputs).astype(jnp.bfloat16)
        pieces.append(jnp.dot(differ, group_maps[group_idx], preferred_element_type=jnp.float32))
    pool_out = (jnp.concatenate(pieces, axis=1) * scales).astype(jnp.bfloat16)
    head_count = decay_rate.shape[0]
    head_dim = query_bf.shape[1] // head_count
    queries = rotate(query_bf.astype(jnp.float32).reshape(length, head_count, head_dim), positions)
    keys_in = rotate(
        key_bf.astype(jnp.float32).reshape(length, head_count, head_dim), positions
    ) * head_dim ** (-0.5)
    values_in = value_bf.astype(jnp.float32).reshape(length, head_count, head_dim)
    zeros_state = jnp.zeros((head_count, head_dim, head_dim), jnp.float32)
    local_output, local_state = block_retention(
        queries, keys_in, values_in, decay_rate, zeros_state
    )
    span_decay = jnp.exp(-decay_rate * length)
    whole_start = lax.all_gather(start_state, "sp", axis=2, tiled=True)[0]
    span_factor, carried_over = carried_in(
        (span_decay, local_state), "sp", combine_states, (jnp.ones_like(span_decay), zeros_state)
    )
    offset_float = (sp_index * length).astype(jnp.float32)
    carried_over = carried_over + jnp.exp(-decay_rate * offset_float)[:, None, None] * whole_start
    steps_in = jnp.arange(length, dtype=jnp.float32) + 1.0
    query_rows_scaled = queries * jnp.exp(-steps_in[:, None] * decay_rate[None, :])[:, :, None]
    retained_output = local_output + jnp.einsum(
        "lpi,pib->lpb", query_rows_scaled, carried_over, precision=highest_precision
    )
    retained_output = retained_output * lax.rsqrt(
        jnp.mean(retained_output * retained_output, axis=-1, keepdims=True) + eps
    )
    ret_out = retained_output.reshape(length, head_count * head_dim).astype(jnp.bfloat16)
    pool_cols, retention_cols = (
        lax.all_gather(pool_back, ("sp", "fs"), axis=1, tiled=True),
        lax.all_gather(retention_back, ("sp", "fs"), axis=1, tiled=True),
    )
    weight_local = jnp.concatenate([pool_cols, retention_cols], axis=0)
    joined = jnp.concatenate([pool_out, ret_out], axis=1)
    mixed = lax.psum_scatter(
        jnp.dot(joined, weight_local, preferred_element_type=jnp.float32).astype(jnp.bfloat16),
        "tp",
        scatter_dimension=0,
        tiled=True,
    )
    return mixed[None]


MESH = pl.DeviceIdType.MESH
LAG = 2
ORDER = (0, 3, 1, 2)


def where_am_i():
    sp, fs, tp = (lax.axis_index(name) for name in ("sp", "fs", "tp"))
    return sp, fs // 2, fs % 2, tp


def at(z, y, x, p):
    return (z, 2 * y + x, p)


def remote(src, dst, send, recv, target):
    return pltpu.make_async_remote_copy(
        src_ref=src, dst_ref=dst, send_sem=send, recv_sem=recv, device_id=target, device_id_type=MESH
    )


def piece(index, size):
    return pl.ds(pl.multiple_of(index * size, size), size)


def fused_kernel(
    tok, gain, wp, wq, wk, wv, state, pb, rb, pmap, pscale, rate, cos_t, sin_t,
    out,
    xt, xn, xg, wg, obuf, rbuf, backs, gv, st, stb, start, cosv, sinv, mapv, scv,
    krot, pool, mask, yb, yg, keep, give, take, done,
    l_sem, wl_sem, bl_sem, wy_send, wx_send, wf_send, w_recv,
    xz_send, xy_send, xp_send, x_recv,
    s_send, s_recv, b_send, b_recv, r_send, r_recv,
    h_send, c_send, y_recv, g_send, g_recv, o_send, o_recv,
):
    f32, bf = jnp.float32, jnp.bfloat16
    z, y, x, p = where_am_i()
    nz = 4
    half, width = xt.shape
    span = 2 * half
    feats = width // nz
    rows = wp.shape[0]
    group = wp.shape[1] // 2
    steps = 4 * nz
    mats = (wk, wq, wv, wp)
    fs = 2 * y + x
    me = at(z, y, x, p)
    partner = at(z, y, x, 1 - p)
    ypeer = at(z, 1 - y, x, p)
    xpeer = at(z, y, 1 - x, p)
    head = 2 * p + y

    barrier = pltpu.get_barrier_semaphore()
    others = [partner, xpeer]
    for dz in range(nz):
        for dy in range(2):
            if dz or dy:
                others.append(at((z + dz) % nz, (y + dy) % 2, x, p))
    for other in others:
        pl.semaphore_signal(barrier, inc=1, device_id=other, device_id_type=MESH)

    loads = [
        pltpu.make_async_copy(tok.at[piece(p, half)], xt, l_sem.at[0]),
        pltpu.make_async_copy(gain, gv, l_sem.at[1]),
        pltpu.make_async_copy(state, st, l_sem.at[2]),
        pltpu.make_async_copy(cos_t, cosv, l_sem.at[3]),
        pltpu.make_async_copy(sin_t, sinv, l_sem.at[4]),
        pltpu.make_async_copy(pmap.at[head], mapv, l_sem.at[5]),
        pltpu.make_async_copy(pscale.at[head], scv, l_sem.at[6]),
    ]
    for c in loads:
        c.start()
    own_w = []
    for m in range(4):
        c = pltpu.make_async_copy(mats[m].at[:, piece(y, group)], wg.at[m, piece(fs, rows)], wl_sem.at[m])
        c.start()
        own_w.append(c)
    loads[0].wait()
    loads[1].wait()

    block = 16
    for i in range(half // block):
        floats = xt[i * block : (i + 1) * block, :].astype(f32)
        xn[i * block : (i + 1) * block, :] = (
            floats * lax.rsqrt(jnp.mean(floats * floats, axis=-1, keepdims=True) + eps) * gv[...]
        ).astype(bf)

    def slot(ref, s, c, h):
        return ref.at[s, pl.ds(pl.multiple_of(c * span + h * half, half), half)]

    pl.semaphore_wait(barrier, len(others))

    sent = []

    def go(c):
        c.start()
        sent.append(c)

    def w_y(m):
        go(remote(mats[m].at[:, piece(1 - y, group)], wg.at[m, piece(fs, rows)], wy_send.at[m], w_recv.at[m, fs], ypeer))

    def w_x(m):
        go(remote(mats[m].at[:, piece(y, group)], wg.at[m, piece(fs, rows)], wx_send.at[m], w_recv.at[m, fs], xpeer))

    def w_wait(m, f):
        view = wg.at[m, piece(f, rows)]
        remote(view, view, wf_send.at[m], w_recv.at[m, f], partner).wait_recv()

    fy = 2 * (1 - y) + x

    def w_relay(m):
        w_wait(m, fy)
        view = wg.at[m, piece(fy, rows)]
        return remote(view, view, wf_send.at[m], w_recv.at[m, fy], xpeer)

    hi = z // 2
    zz = z * (1 - hi) + (3 - z) * hi
    near = [o * (1 - hi) + (3 - o) * hi for o in (1 - zz, 2, 3)]

    w_y(0)
    w_x(0)
    for i, c in enumerate(near):
        go(remote(xn.at[:, piece(c, feats)], slot(xg, y, z, p), xz_send.at[i], x_recv.at[y, z, p], at(c, y, x, p)))
    xg[y, pl.ds(pl.multiple_of(z * span + p * half, half), half), :] = xn[:, piece(z, feats)]

    def x_wait(s, c, h):
        view = slot(xg, s, c, h)
        remote(view, view, xp_send.at[0], x_recv.at[s, c, h], partner).wait_recv()

    def x_to_y(i, c):
        view = slot(xg, y, c, p)
        go(remote(view, view, xy_send.at[i], x_recv.at[y, c, p], ypeer))

    def x_to_partner(i, s, c):
        view = slot(xg, s, c, p)
        go(remote(view, view, xp_send.at[i], x_recv.at[s, c, p], partner))

    go(remote(xn.at[:, piece(z, feats)], slot(xg, y, z, p), xy_send.at[3], x_recv.at[y, z, p], ypeer))
    go(remote(xn.at[:, piece(z, feats)], slot(xg, y, z, p), xp_send.at[3], x_recv.at[y, z, p], partner))

    loads[2].wait()
    for j in range(2):
        stb[j] = st[j].astype(bf)
    toward = 3 * ((y + p) % 2)
    rs = st.shape[1]
    for j in range(2):
        same = (z == toward) & (y == j)
        dst = start.at[piece(z, rs)]

        @pl.when(same)
        def _():
            pltpu.make_async_copy(stb.at[j], dst, s_recv.at[z]).start()

        @pl.when(jnp.logical_not(same))
        def _():
            remote(stb.at[j], dst, s_send.at[j], s_recv.at[z], at(toward, j, x, p)).start()

    go(w_relay(0))
    w_x(1)
    x_wait(y, near[0], p)
    x_to_y(0, near[0])
    x_to_partner(0, y, near[0])
    w_y(1)
    x_wait(1 - y, z, p)
    x_to_partner(4 + 3, 1 - y, z)
    x_wait(y, near[1], p)
    x_to_y(1, near[1])
    x_to_partner(1, y, near[1])
    x_wait(1 - y, near[0], p)
    x_to_partner(4 + 0, 1 - y, near[0])
    go(w_relay(1))
    w_x(2)
    w_x(3)
    x_wait(y, near[2], p)
    x_to_y(2, near[2])
    x_to_partner(2, y, near[2])
    w_y(2)
    w_y(3)

    own_b = []
    for b, back in enumerate((pb, rb)):
        c = pltpu.make_async_copy(back, backs.at[b, :, piece(fs, rows)], bl_sem.at[b])
        c.start()
        own_b.append(c)
    for b, back in enumerate((pb, rb)):
        view = backs.at[b, :, piece(fs, rows)]
        first, second = ((xpeer, ypeer), (ypeer, xpeer))[b]
        go(remote(back, view, b_send.at[b, 0], b_recv.at[b, fs], first))
        go(remote(back, view, b_send.at[b, 1], b_recv.at[b, fs], second))
    fx = 2 * y + 1 - x
    fd = 2 * (1 - y) + 1 - x

    def b_wait(b, f):
        view = backs.at[b, :, piece(f, rows)]
        remote(view, view, b_send.at[b, 2], b_recv.at[b, f], partner).wait_recv()

    def b_relay(b):
        f, second = ((fx, ypeer), (fy, xpeer))[b]
        view = backs.at[b, :, piece(f, rows)]
        return remote(view, view, b_send.at[b, 2], b_recv.at[b, f], second)

    x_wait(1 - y, near[1], p)
    x_to_partner(4 + 1, 1 - y, near[1])
    x_wait(1 - y, near[2], p)
    x_to_partner(4 + 2, 1 - y, near[2])

    r = rate[y]
    row = lax.broadcasted_iota(jnp.int32, (span, span), 0)
    col = lax.broadcasted_iota(jnp.int32, (span, span), 1)
    gap = row - col
    for k in range(nz):
        dist = (gap + k * span).astype(f32)
        value = jnp.exp(-jnp.maximum(dist, 0.0) * r)
        mask[k] = jnp.where(dist >= 0.0, value, 0.0) if k == 0 else value
    loads[3].wait()
    loads[4].wait()
    loads[5].wait()
    loads[6].wait()

    for s in (y, 1 - y):
        for c in range(nz):
            x_wait(s, c, 1 - p)

    sems = (r_send, r_recv)

    def step(d, j):
        m, cc = j // nz, j % nz
        c = (nz - 1) - cc if d == 0 else cc
        s = p if d == 0 else 1 - p
        begins = (z == nz - 1) if d == 0 else (z == 0)
        ends = (z == 0) if d == 0 else (z == nz - 1)
        nxt = z - 1 if d == 0 else z + 1
        acc = jnp.dot(xg[s, piece(c, span), :], wg[m], preferred_element_type=f32)
        send, recv = r_send.at[d, j], r_recv.at[d, j]

        @pl.when(begins)
        def _():
            obuf[d, j] = acc.astype(bf)

        @pl.when(jnp.logical_not(begins))
        def _():
            remote(rbuf.at[d, j], rbuf.at[d, j], send, recv, partner).wait_recv()
            obuf[d, j] = (acc + rbuf[d, j].astype(f32)).astype(bf)

        @pl.when(jnp.logical_not(ends))
        def _():
            remote(obuf.at[d, j], rbuf.at[d, j], send, recv, at(nxt, y, x, p)).start()

    def body(k, carry):
        @pl.when(k == 2)
        def _():
            w_relay(2).start()

        @pl.when(k == 4)
        def _():
            w_relay(3).start()

        @pl.when(k == 8)
        def _():
            for b in range(2):
                b_wait(b, (fx, fy)[b])
                b_relay(b).start()

        lead = k - LAG * zz

        @pl.when((lead >= 0) & (lead < steps) & (lead % nz == 0))
        def _():
            m = lead // nz
            pltpu.make_async_copy(wp.at[:, piece(y, group)], wg.at[m, piece(fs, rows)], wl_sem.at[m]).wait()
            w_wait(m, fx)
            w_wait(m, fd)

        for d, j in ((0, k - LAG * (nz - 1 - z)), (1, k - LAG * z)):

            @pl.when((j >= 0) & (j < steps))
            def _():
                step(d, j)

        return carry

    lax.fori_loop(0, steps + LAG * (nz - 1), body, 0)

    owner = ((z == 0) & (y == p)) | ((z == nz - 1) & (y != p))
    is_end = (z == 0) | (z == nz - 1)
    flow = (y + p) % 2
    hop = z * (1 - flow) + (nz - 1 - z) * flow
    onward = at(z + 1 - 2 * flow, y, x, p)

    def chain(b, q, c):
        view = yg.at[b, q, c]
        return remote(view, view, c_send.at[b, q, c], y_recv.at[b, q, c], onward)

    @pl.when(is_end)
    def _():
        for k in range(nz):
            view = start.at[piece(k, rs)]
            remote(view, view, s_send.at[0], s_recv.at[k], partner).wait_recv()
        d = z // (nz - 1)
        small = group // 2

        def value_at(m, c):
            cc = (nz - 1 - c) * (1 - d) + c * d
            return obuf[d, m * nz + cc]

        pool[0:HALO, :] = jnp.zeros((HALO, group), bf)
        for c in range(nz):
            cosine, sine = cosv[c * span : (c + 1) * span, :], sinv[c * span : (c + 1) * span, :]
            k_c = value_at(0, c).astype(f32)
            a, b = k_c[:, :small], k_c[:, small:]
            scale = group ** (-0.5)
            krot[c * span : (c + 1) * span, :small] = ((a * cosine - b * sine) * scale).astype(bf)
            krot[c * span : (c + 1) * span, small:] = ((a * sine + b * cosine) * scale).astype(bf)
            pool[HALO + c * span : HALO + (c + 1) * span, :] = value_at(3, c)
        window = 2 * (1 + y) * (1 + 3 * p)
        brow = lax.broadcasted_iota(jnp.int32, (span, span + HALO), 0)
        bcol = lax.broadcasted_iota(jnp.int32, (span, span + HALO), 1)
        behind = brow + HALO - bcol
        band = jnp.where((behind >= 0) & (behind < window), 1.0, 0.0).astype(bf)
        place = lax.broadcasted_iota(jnp.int32, (span, 1), 0)
        for c in ORDER:
            cosine, sine = cosv[c * span : (c + 1) * span, :], sinv[c * span : (c + 1) * span, :]
            q_c = value_at(1, c).astype(f32)
            a, b = q_c[:, :small], q_c[:, small:]
            rq = jnp.concatenate([a * cosine - b * sine, a * sine + b * cosine], axis=-1)
            fade = jnp.exp(-((place + c * span).astype(f32) + 1.0) * r)
            acc = jnp.dot((rq * fade).astype(bf), start[...], preferred_element_type=f32)
            rq = rq.astype(bf)
            for e in range(c + 1):
                scores = lax.dot_general(
                    rq, krot[e * span : (e + 1) * span, :], (((1,), (1,)), ((), ())), preferred_element_type=f32
                )
                scores = (scores * mask[c - e]).astype(bf)
                acc += jnp.dot(scores, value_at(2, e), preferred_element_type=f32)
            ret = (acc * lax.rsqrt(jnp.mean(acc * acc, axis=-1, keepdims=True) + eps)).astype(bf)
            rows_c = pool[c * span : (c + 1) * span + HALO, :]
            trail = jnp.dot(band, rows_c, preferred_element_type=f32)
            counts = jnp.minimum(window, place + c * span + 1).astype(f32)
            differ = (trail / counts - value_at(3, c).astype(f32)).astype(bf)
            pooled = (jnp.dot(differ, mapv[...], preferred_element_type=f32) * scv[...]).astype(bf)

            @pl.when(owner)
            def _():
                yg[1, y, c] = ret
                yg[0, y, c] = pooled
                chain(1, y, c).start()
                chain(0, y, c).start()

            @pl.when(jnp.logical_not(owner))
            def _():
                yb[1, c] = ret
                yb[0, c] = pooled
                for b in (1, 0):
                    remote(yb.at[b, c], yg.at[b, y, c], h_send.at[b, c], y_recv.at[b, y, c], ypeer).start()

    for b in range(2):
        own_b[b].wait()
        b_wait(b, (fy, fx)[b])
        b_wait(b, fd)

    def arrive(b, q, c):
        view = yg.at[b, q, c]
        remote(view, view, c_send.at[b, q, c], y_recv.at[b, q, c], partner).wait_recv()

    def collect(c):
        for q in (y, 1 - y):
            for b in (1, 0):
                if q is y:

                    @pl.when(hop > 0)
                    def _():
                        arrive(b, q, c)

                        @pl.when(hop < nz - 1)
                        def _():
                            chain(b, q, c).start()
                else:
                    arrive(b, q, c)

                    @pl.when(hop < nz - 1)
                    def _():
                        chain(b, q, c).start()

    across = backs.shape[2]

    def multiply(c):
        acc = jnp.zeros((span, across), f32)
        for b in range(2):
            for q in range(2):
                acc += jnp.dot(
                    yg[b, q, c], backs[b, q * group : (q + 1) * group, :], preferred_element_type=f32
                )
        keep[c] = acc
        give[c] = keep[c, piece(1 - p, half), :].astype(bf)
        move = remote(give.at[c], take.at[c], g_send.at[c], g_recv.at[c], partner)
        move.start()
        return move

    def finish(c, move):
        move.wait()
        done[c] = (keep[c, piece(p, half), :] + take[c].astype(f32)).astype(bf)
        dst = out.at[:, piece(z, across)]

        @pl.when(z == c)
        def _():
            pltpu.make_async_copy(done.at[c], dst, o_recv.at[z]).start()

        @pl.when(z != c)
        def _():
            remote(done.at[c], dst, o_send.at[c], o_recv.at[z], at(c, y, x, p)).start()

    moves = []
    for i, c in enumerate(ORDER):
        collect(c)
        moves.append(multiply(c))
        if i:
            finish(ORDER[i - 1], moves[i - 1])
    finish(ORDER[-1], moves[-1])

    for k in range(nz):
        view = out.at[:, k * across : (k + 1) * across]
        remote(done.at[k], view, o_send.at[k], o_recv.at[k], partner).wait_recv()

        @pl.when(z != k)
        def _():
            remote(done.at[k], view, o_send.at[k], o_recv.at[k], partner).wait_send()

    @pl.when(hop < nz - 1)
    def _():
        for b in range(2):
            for q in range(2):
                for c in range(nz):
                    chain(b, q, c).wait_send()

    @pl.when(is_end & jnp.logical_not(owner))
    def _():
        for b in range(2):
            for c in range(nz):
                remote(yb.at[b, c], yb.at[b, c], h_send.at[b, c], y_recv.at[b, 0, c], partner).wait_send()

    for d in range(2):

        @pl.when((z > 0) if d == 0 else (z < nz - 1))
        def _():
            def drain(j, carry):
                remote(obuf.at[d, j], rbuf.at[d, j], r_send.at[d, j], r_recv.at[d, j], partner).wait_send()
                return carry

            lax.fori_loop(0, steps, drain, 0)

    for j in range(2):

        @pl.when(jnp.logical_not((z == toward) & (y == j)))
        def _():
            remote(stb.at[j], stb.at[j], s_send.at[j], s_recv.at[0], partner).wait_send()

    for m in (2, 3):
        view = wg.at[m, piece(fy, rows)]
        remote(view, view, wf_send.at[m], w_recv.at[m, fy], partner).wait_send()
    for b in range(2):
        b_relay(b).wait_send()
    for c in sent:
        c.wait_send()


def rotary_tables(length, half_dim):
    inv_freq = np.float32(1.0) / np.power(
        np.float32(rope_base), np.linspace(0.0, 1.0, half_dim, dtype=np.float32)
    )
    angles = np.arange(length, dtype=np.float32)[:, None] * inv_freq[None, :].astype(np.float32)
    return np.cos(angles).astype(np.float32), np.sin(angles).astype(np.float32)


def paired(
    tokens, norm_gain, pool_proj, query_proj, key_proj, value_proj, pool_map, pool_scale,
    decay_rate, start_state, pool_back, retention_back,
):
    bf, f32 = jnp.bfloat16, jnp.float32
    nsp = lax.axis_size("sp")
    tok = tokens[0]
    span, width = tok.shape
    rows, two = pool_proj.shape
    group = two // 2
    length = nsp * span
    half = span // 2
    rs = start_state.shape[2]
    steps = 4 * nsp
    across = 4 * pool_back.shape[1]
    vm, hbm = pl.BlockSpec(memory_space=pltpu.VMEM), pl.BlockSpec(memory_space=pl.ANY)
    dma = pltpu.SemaphoreType.DMA
    cosine, sine = rotary_tables(length, group // 2)
    return pl.pallas_call(
        fused_kernel,
        out_shape=jax.ShapeDtypeStruct((half, width), bf),
        in_specs=[hbm] * 11 + [pl.BlockSpec(memory_space=pltpu.SMEM)] + [hbm] * 2,
        out_specs=vm,
        scratch_shapes=[
            pltpu.VMEM((half, width), bf),
            pltpu.VMEM((half, width), bf),
            pltpu.VMEM((2, length, width // nsp), bf),
            pltpu.VMEM((4, 4 * rows, group), bf),
            pltpu.VMEM((2, steps, span, group), bf),
            pltpu.VMEM((2, steps, span, group), bf),
            pltpu.VMEM((2, pool_back.shape[0], across), bf),
            pltpu.VMEM((1, width), f32),
            pltpu.VMEM((2, rs, group), f32),
            pltpu.VMEM((2, rs, group), bf),
            pltpu.VMEM((nsp * rs, group), bf),
            pltpu.VMEM((length, group // 2), f32),
            pltpu.VMEM((length, group // 2), f32),
            pltpu.VMEM((group, group), bf),
            pltpu.VMEM((1, group), f32),
            pltpu.VMEM((length, group), bf),
            pltpu.VMEM((HALO + length, group), bf),
            pltpu.VMEM((nsp, span, span), f32),
            pltpu.VMEM((2, nsp, span, group), bf),
            pltpu.VMEM((2, 2, nsp, span, group), bf),
            pltpu.VMEM((nsp, span, across), f32),
            pltpu.VMEM((nsp, half, across), bf),
            pltpu.VMEM((nsp, half, across), bf),
            pltpu.VMEM((nsp, half, across), bf),
            dma((7,)), dma((4,)), dma((2,)), dma((4,)), dma((4,)), dma((4,)), dma((4, 4)),
            dma((3,)), dma((4,)), dma((8,)), dma((2, nsp, 2)),
            dma((2,)), dma((nsp,)), dma((2, 3)), dma((2, 4)), dma((2, steps)), dma((2, steps)),
            dma((2, nsp)), dma((2, 2, nsp)), dma((2, 2, nsp)), dma((nsp,)), dma((nsp,)), dma((nsp,)), dma((nsp,)),
        ],
        compiler_params=pltpu.CompilerParams(collective_id=0, has_side_effects=True, vmem_limit_bytes=60 * 2**20),
        name="fused",
    )(
        tok, norm_gain[None, :], pool_proj, query_proj, key_proj, value_proj,
        start_state[0], pool_back, retention_back, pool_map,
        pool_scale.reshape(pool_map.shape[0], 1, group), decay_rate, jnp.asarray(cosine), jnp.asarray(sine),
    )[None]


def solution(mesh):
    sizes = mesh.shape
    small = sizes["sp"] == 4 and sizes["fs"] == 4 and sizes["tp"] == 2
    placed = (
        P("fs", "sp", None),
        P(),
        P(("sp", "fs"), "tp"),
        P(("sp", "fs"), "tp"),
        P(("sp", "fs"), "tp"),
        P(("sp", "fs"), "tp"),
        P(),
        P(),
        P("tp"),
        P("fs", "tp", "sp", None),
        P("tp", ("sp", "fs")),
        P("tp", ("sp", "fs")),
    )
    return jax.shard_map(
        paired if small else on_device,
        mesh=mesh,
        in_specs=placed,
        out_specs=P("fs", ("sp", "tp"), None),
        check_vma=False,
    )
```

```python
import numpy as np
from jax.experimental import pallas as pl
from jax.experimental.pallas import tpu as pltpu

import jax
import jax.numpy as jnp
from jax import lax
from jax.sharding import PartitionSpec as P

GROUPS = 4
BLOCK = 128
HALO = 16


eps = 1e-06
rope_base = 10000.0
highest_precision = lax.Precision.HIGHEST
window_list = (2, 4, 8, 16)


def shortened(x):
    return jax.tree.map(lambda a: a.astype(jnp.bfloat16) if a.dtype == jnp.float32 else a, x)


def shifted(x, axis, by):
    devices = lax.axis_size(axis)
    pairs = [(i, i + by) for i in range(devices) if 0 <= i + by < devices]
    return lax.ppermute(x, axis, pairs)


def carried_in(value, axis, join, neutral):
    count, mine = (lax.axis_size(axis), lax.axis_index(axis))
    pieces = jax.tree.map(lambda part: lax.all_gather(part, axis), value)
    running = jax.tree.map(
        lambda part, zero: jnp.full_like(part, 0) + jnp.asarray(zero, part.dtype), value, neutral
    )

    def turn(position, running):
        longer = join(running, jax.tree.map(lambda part: part[position], pieces))
        return jax.tree.map(lambda new, old: jnp.where(position < mine, new, old), longer, running)

    return lax.fori_loop(0, count - 1, turn, running)


def rotate(values, positions):
    half_dim = values.shape[-1] // 2
    inv_freq = 1.0 / rope_base ** jnp.linspace(0.0, 1.0, half_dim, dtype=jnp.float32)
    angles = positions.astype(jnp.float32)[:, None] * inv_freq[None, :]
    cosine = jnp.cos(angles)[:, None, :]
    sine = jnp.sin(angles)[:, None, :]
    first_half = values[..., :half_dim]
    second_half = values[..., half_dim:]
    return jnp.concatenate(
        [first_half * cosine - second_half * sine, first_half * sine + second_half * cosine],
        axis=-1,
    )


def trailing_sums(extended, length):
    begin = extended.shape[0] - length
    running = extended[begin:]
    results = []
    for behind in range(1, 16):
        running = running + extended[begin - behind : begin - behind + length]
        if behind + 1 in window_list:
            results.append(running)
    return results


def reshape_blocks(array):
    return array.reshape((array.shape[0] // BLOCK, BLOCK) + array.shape[1:])


def block_retention(queries, keys_in, values_in, decay_rate, initial):
    length, head_count, head_dim = queries.shape
    within = jnp.arange(BLOCK, dtype=jnp.float32)
    distance = within[:, None] - within[None, :]
    decay_mask = jnp.where(
        distance[None] >= 0,
        jnp.exp(-jnp.maximum(distance, 0.0)[None] * decay_rate[:, None, None]),
        0.0,
    )
    query_decay_factor = jnp.exp(-(within + 1.0)[:, None] * decay_rate[None, :])
    key_decay_factor = jnp.exp(-(BLOCK - 1.0 - within)[:, None] * decay_rate[None, :])
    block_decay_factor = jnp.exp(-BLOCK * decay_rate)

    def advance(state_carry, inputs):
        block_queries, block_keys, block_values = inputs
        scores = (
            jnp.einsum("ihk,jhk->hij", block_queries, block_keys, precision=highest_precision)
            * decay_mask
        )
        inside = jnp.einsum("hij,jhv->ihv", scores, block_values, precision=highest_precision)
        across_blocks = jnp.einsum(
            "bzy,zyx->bzx",
            block_queries * query_decay_factor[:, :, None],
            state_carry,
            precision=highest_precision,
        )
        state_carry = state_carry * block_decay_factor[:, None, None] + jnp.einsum(
            "flm,fld->lmd",
            block_keys * key_decay_factor[:, :, None],
            block_values,
            precision=highest_precision,
        )
        return (state_carry, inside + across_blocks)

    final_state, outputs = lax.scan(
        advance,
        initial,
        (reshape_blocks(queries), reshape_blocks(keys_in), reshape_blocks(values_in)),
    )
    return (outputs.reshape(length, head_count, values_in.shape[-1]), final_state)


def combine_states(earlier, latter):
    return (earlier[0] * latter[0], latter[0][:, None, None] * earlier[1] + latter[1])


def on_device(
    tokens,
    norm_gain,
    pool_proj,
    query_proj,
    key_proj,
    value_proj,
    pool_map,
    pool_scale,
    decay_rate,
    start_state,
    pool_back,
    retention_back,
):
    sequence = tokens[0]
    length = sequence.shape[0]
    tp_index = lax.axis_index("tp")
    sp_index = lax.axis_index("sp")
    tp_count = lax.axis_size("tp")
    floats = sequence.astype(jnp.float32)
    normed = (
        floats * lax.rsqrt(jnp.mean(floats * floats, axis=-1, keepdims=True) + eps) * norm_gain
    ).astype(jnp.bfloat16)
    group_normed = lax.all_gather(normed, "fs", axis=0, tiled=True)
    quarters = (
        lax.all_to_all(pool_proj, "fs", split_axis=1, concat_axis=0, tiled=True),
        lax.all_to_all(query_proj, "fs", split_axis=1, concat_axis=0, tiled=True),
        lax.all_to_all(key_proj, "fs", split_axis=1, concat_axis=0, tiled=True),
        lax.all_to_all(value_proj, "fs", split_axis=1, concat_axis=0, tiled=True),
    )
    pieces = (
        lax.all_gather(quarters[0], "sp", axis=0, tiled=True),
        lax.all_gather(quarters[1], "sp", axis=0, tiled=True),
        lax.all_gather(quarters[2], "sp", axis=0, tiled=True),
        lax.all_gather(quarters[3], "sp", axis=0, tiled=True),
    )
    partial_cols = tuple(
        (jnp.dot(group_normed, piece_w, preferred_element_type=jnp.float32) for piece_w in pieces)
    )
    rounded = tuple((result.astype(jnp.bfloat16) for result in partial_cols))
    pool_in, query_bf, key_bf, value_bf = jax.tree.map(
        lambda part, own: part.astype(own.dtype),
        lax.all_to_all(shortened(rounded), "fs", split_axis=0, concat_axis=1, tiled=True),
        rounded,
    )
    positions = jnp.arange(length, dtype=jnp.int32) + sp_index * length
    before = shifted(pool_in[length - HALO :], "sp", 1)
    extended = jnp.concatenate([before, pool_in], axis=0).astype(jnp.float32)
    stacked = jnp.stack(trailing_sums(extended, length))
    local_groups = GROUPS // tp_count
    channels = pool_in.shape[1]
    group_dim = channels // local_groups
    group_maps = lax.dynamic_slice_in_dim(pool_map, tp_index * local_groups, local_groups, 0)
    scales = lax.dynamic_slice_in_dim(pool_scale, tp_index * channels, channels, 0)
    windows = jnp.array(window_list, dtype=jnp.int32)
    pieces = []
    for group_idx in range(local_groups):
        chosen_group = tp_index * local_groups + group_idx
        lower = group_idx * group_dim
        chosen = lax.dynamic_index_in_dim(stacked, chosen_group, 0, keepdims=False)[
            :, lower : lower + group_dim
        ]
        counts = jnp.minimum(windows[chosen_group], positions + 1).astype(jnp.float32)
        inputs = extended[HALO:, lower : lower + group_dim]
        differ = (chosen / counts[:, None] - inputs).astype(jnp.bfloat16)
        pieces.append(jnp.dot(differ, group_maps[group_idx], preferred_element_type=jnp.float32))
    pool_out = (jnp.concatenate(pieces, axis=1) * scales).astype(jnp.bfloat16)
    head_count = decay_rate.shape[0]
    head_dim = query_bf.shape[1] // head_count
    queries = rotate(query_bf.astype(jnp.float32).reshape(length, head_count, head_dim), positions)
    keys_in = rotate(
        key_bf.astype(jnp.float32).reshape(length, head_count, head_dim), positions
    ) * head_dim ** (-0.5)
    values_in = value_bf.astype(jnp.float32).reshape(length, head_count, head_dim)
    zeros_state = jnp.zeros((head_count, head_dim, head_dim), jnp.float32)
    local_output, local_state = block_retention(
        queries, keys_in, values_in, decay_rate, zeros_state
    )
    span_decay = jnp.exp(-decay_rate * length)
    whole_start = lax.all_gather(start_state, "sp", axis=2, tiled=True)[0]
    span_factor, carried_over = carried_in(
        (span_decay, local_state), "sp", combine_states, (jnp.ones_like(span_decay), zeros_state)
    )
    offset_float = (sp_index * length).astype(jnp.float32)
    carried_over = carried_over + jnp.exp(-decay_rate * offset_float)[:, None, None] * whole_start
    steps_in = jnp.arange(length, dtype=jnp.float32) + 1.0
    query_rows_scaled = queries * jnp.exp(-steps_in[:, None] * decay_rate[None, :])[:, :, None]
    retained_output = local_output + jnp.einsum(
        "lpi,pib->lpb", query_rows_scaled, carried_over, precision=highest_precision
    )
    retained_output = retained_output * lax.rsqrt(
        jnp.mean(retained_output * retained_output, axis=-1, keepdims=True) + eps
    )
    ret_out = retained_output.reshape(length, head_count * head_dim).astype(jnp.bfloat16)
    pool_cols, retention_cols = (
        lax.all_gather(pool_back, ("sp", "fs"), axis=1, tiled=True),
        lax.all_gather(retention_back, ("sp", "fs"), axis=1, tiled=True),
    )
    weight_local = jnp.concatenate([pool_cols, retention_cols], axis=0)
    joined = jnp.concatenate([pool_out, ret_out], axis=1)
    mixed = lax.psum_scatter(
        jnp.dot(joined, weight_local, preferred_element_type=jnp.float32).astype(jnp.bfloat16),
        "tp",
        scatter_dimension=0,
        tiled=True,
    )
    return mixed[None]


MESH = pl.DeviceIdType.MESH
LAG_E = 2
LAG_L = 3
LATE = 4
LATE_MATS = (0, 1, 0, 1, 2, 2, 0, 1, 2, 3, 3, 3, 0, 1, 2, 3)
LATE_CHUNKS = (0, 0, 1, 1, 0, 1, 2, 2, 2, 0, 1, 2, 3, 3, 3, 3)
ORDER = (0, 3, 1, 2)


def where_am_i():
    sp, fs, tp = (lax.axis_index(name) for name in ("sp", "fs", "tp"))
    return sp, fs // 2, fs % 2, tp


def at(z, y, x, p):
    return (z, 2 * y + x, p)


def remote(src, dst, send, recv, target):
    return pltpu.make_async_remote_copy(
        src_ref=src, dst_ref=dst, send_sem=send, recv_sem=recv, device_id=target, device_id_type=MESH
    )


def piece(index, size):
    return pl.ds(pl.multiple_of(index * size, size), size)


def fused_kernel(
    tok, gain, wp, wq, wk, wv, state, pb, rb, pmap, pscale, rate, cos_t, sin_t,
    out,
    xt, xn, xg, wg, obuf, rbuf, backs, gv, st, stb, start, cosv, sinv, mapv, scv,
    krot, pool, mask, yb, yg, keep, give, take, done,
    l_sem, wl_sem, bl_sem, wy_send, wx_send, wf_send, w_recv,
    xz_send, xy_send, xp_send, x_recv,
    s_send, s_recv, b_send, b_recv, r_send, r_recv,
    h_send, c_send, y_recv, g_send, g_recv, o_send, o_recv,
):
    f32, bf = jnp.float32, jnp.bfloat16
    z, y, x, p = where_am_i()
    nz = 4
    half, width = xt.shape
    span = 2 * half
    feats = width // nz
    rows = wp.shape[0]
    group = wp.shape[1] // 2
    steps = 4 * nz
    mats = (wk, wq, wv, wp)
    fs = 2 * y + x
    me = at(z, y, x, p)
    partner = at(z, y, x, 1 - p)
    ypeer = at(z, 1 - y, x, p)
    xpeer = at(z, y, 1 - x, p)
    head = 2 * p + y

    barrier = pltpu.get_barrier_semaphore()
    others = [partner, xpeer]
    for dz in range(nz):
        for dy in range(2):
            if dz or dy:
                others.append(at((z + dz) % nz, (y + dy) % 2, x, p))
    for other in others:
        pl.semaphore_signal(barrier, inc=1, device_id=other, device_id_type=MESH)

    loads = [
        pltpu.make_async_copy(tok.at[piece(p, half)], xt, l_sem.at[0]),
        pltpu.make_async_copy(gain, gv, l_sem.at[1]),
        pltpu.make_async_copy(state, st, l_sem.at[2]),
        pltpu.make_async_copy(cos_t, cosv, l_sem.at[3]),
        pltpu.make_async_copy(sin_t, sinv, l_sem.at[4]),
        pltpu.make_async_copy(pmap.at[head], mapv, l_sem.at[5]),
        pltpu.make_async_copy(pscale.at[head], scv, l_sem.at[6]),
    ]
    for c in loads:
        c.start()
    own_w = []
    for m in range(4):
        c = pltpu.make_async_copy(mats[m].at[:, piece(y, group)], wg.at[m, piece(fs, rows)], wl_sem.at[m])
        c.start()
        own_w.append(c)
    loads[0].wait()
    loads[1].wait()

    block = 16
    for i in range(half // block):
        floats = xt[i * block : (i + 1) * block, :].astype(f32)
        xn[i * block : (i + 1) * block, :] = (
            floats * lax.rsqrt(jnp.mean(floats * floats, axis=-1, keepdims=True) + eps) * gv[...]
        ).astype(bf)

    def slot(ref, s, c, h):
        return ref.at[s, pl.ds(pl.multiple_of(c * span + h * half, half), half)]

    pl.semaphore_wait(barrier, len(others))

    sent = []

    def go(c):
        c.start()
        sent.append(c)

    def w_y(m):
        go(remote(mats[m].at[:, piece(1 - y, group)], wg.at[m, piece(fs, rows)], wy_send.at[m], w_recv.at[m, fs], ypeer))

    def w_copy_x(m):
        return remote(mats[m].at[:, piece(y, group)], wg.at[m, piece(fs, rows)], wx_send.at[m], w_recv.at[m, fs], xpeer)

    def w_x(m):
        go(w_copy_x(m))

    def w_wait(m, f):
        view = wg.at[m, piece(f, rows)]
        remote(view, view, wf_send.at[m], w_recv.at[m, f], partner).wait_recv()

    fy = 2 * (1 - y) + x

    def w_relay(m):
        w_wait(m, fy)
        view = wg.at[m, piece(fy, rows)]
        return remote(view, view, wf_send.at[m], w_recv.at[m, fy], xpeer)

    hi = z // 2
    zz = z * (1 - hi) + (3 - z) * hi
    near = [o * (1 - hi) + (3 - o) * hi for o in (1 - zz, 2, 3)]
    flow = (y + p) % 2
    hop_e = (nz - 1 - z) * (1 - flow) + z * flow
    hop_l = nz - 1 - hop_e
    toward_e = at(z - 1 + 2 * flow, y, x, p)
    toward_l = at(z + 1 - 2 * flow, y, x, p)

    w_y(0)
    w_x(0)
    for i, c in enumerate(near):
        go(remote(xn.at[:, piece(c, feats)], slot(xg, y, z, p), xz_send.at[i], x_recv.at[y, z, p], at(c, y, x, p)))
    xg[y, pl.ds(pl.multiple_of(z * span + p * half, half), half), :] = xn[:, piece(z, feats)]

    def x_wait(s, c, h):
        view = slot(xg, s, c, h)
        remote(view, view, xp_send.at[0], x_recv.at[s, c, h], partner).wait_recv()

    def x_to_y(i, c):
        view = slot(xg, y, c, p)
        go(remote(view, view, xy_send.at[i], x_recv.at[y, c, p], ypeer))

    def x_to_partner(i, s, c):
        view = slot(xg, s, c, p)
        return remote(view, view, xp_send.at[i], x_recv.at[s, c, p], partner)

    w_y(1)
    w_x(1)
    go(remote(xn.at[:, piece(z, feats)], slot(xg, y, z, p), xp_send.at[3], x_recv.at[y, z, p], partner))
    go(remote(xn.at[:, piece(z, feats)], slot(xg, y, z, p), xy_send.at[3], x_recv.at[y, z, p], ypeer))
    w_y(2)

    loads[2].wait()
    for j in range(2):
        stb[j] = st[j].astype(bf)
    toward = 3 * ((y + p) % 2)
    rs = st.shape[1]
    for j in range(2):
        same = (z == toward) & (y == j)
        dst = start.at[piece(z, rs)]

        @pl.when(same)
        def _():
            pltpu.make_async_copy(stb.at[j], dst, s_recv.at[z]).start()

        @pl.when(jnp.logical_not(same))
        def _():
            remote(stb.at[j], dst, s_send.at[j], s_recv.at[z], at(toward, j, x, p)).start()

    r = rate[y]
    row = lax.broadcasted_iota(jnp.int32, (span, span), 0)
    col = lax.broadcasted_iota(jnp.int32, (span, span), 1)
    gap = row - col
    for k in range(nz):
        dist = (gap + k * span).astype(f32)
        value = jnp.exp(-jnp.maximum(dist, 0.0) * r)
        mask[k] = jnp.where(dist >= 0.0, value, 0.0) if k == 0 else value
    for c in loads[3:]:
        c.wait()

    x_wait(y, near[0], p)
    x_to_y(0, near[0])
    go(x_to_partner(0, y, near[0]))
    go(w_relay(0))
    w_y(3)
    go(w_relay(1))
    w_x(2)
    x_wait(y, near[1], p)
    x_to_y(1, near[1])
    go(x_to_partner(1, y, near[1]))
    x_wait(1 - y, z, p)
    go(x_to_partner(4 + 3, 1 - y, z))

    own_b = []
    for b, back in enumerate((pb, rb)):
        c = pltpu.make_async_copy(back, backs.at[b, :, piece(fs, rows)], bl_sem.at[b])
        c.start()
        own_b.append(c)
    fx = 2 * y + 1 - x
    fd = 2 * (1 - y) + 1 - x

    def b_own(b, i):
        back = (pb, rb)[b]
        target = ((xpeer, ypeer), (ypeer, xpeer))[b][i]
        return remote(back, backs.at[b, :, piece(fs, rows)], b_send.at[b, i], b_recv.at[b, fs], target)

    def b_wait(b, f):
        view = backs.at[b, :, piece(f, rows)]
        remote(view, view, b_send.at[b, 2], b_recv.at[b, f], partner).wait_recv()

    def b_relay(b):
        f, second = ((fx, ypeer), (fy, xpeer))[b]
        view = backs.at[b, :, piece(f, rows)]
        return remote(view, view, b_send.at[b, 2], b_recv.at[b, f], second)

    def listed(table, j):
        word = sum(v << (2 * i) for i, v in enumerate(table))
        word = word - 2**32 if word >= 2**31 else word
        return lax.shift_right_logical(jnp.int32(word), 2 * j) & 3

    def step(e, m, i):
        d = flow if e == 0 else 1 - flow
        hop = hop_e if e == 0 else hop_l
        s = y if e == 0 else 1 - y
        c = (nz - 1 - i) * (1 - d) + i * d
        at_slot = m * nz + c

        @pl.when(m == 0)
        def _():
            x_wait(s, c, 1 - p)

        acc = jnp.dot(xg[s, piece(c, span), :], wg[m], preferred_element_type=f32)
        send, recv = r_send.at[e, at_slot], r_recv.at[e, at_slot]

        @pl.when(hop == 0)
        def _():
            obuf[e, at_slot] = acc.astype(bf)

        @pl.when(hop > 0)
        def _():
            remote(rbuf.at[e, at_slot], rbuf.at[e, at_slot], send, recv, partner).wait_recv()
            obuf[e, at_slot] = (acc + rbuf[e, at_slot].astype(f32)).astype(bf)

        @pl.when(hop < nz - 1)
        def _():
            remote(
                obuf.at[e, at_slot], rbuf.at[e, at_slot], send, recv, toward_e if e == 0 else toward_l
            ).start()

    def w_ready(m):
        own_w[m].wait()
        w_wait(m, fx)
        w_wait(m, fd)

    def event(k, when, act):
        @pl.when(k == when)
        def _():
            act()

    def a3():
        x_wait(y, near[2], p)
        view = slot(xg, y, near[2], p)
        remote(view, view, xy_send.at[2], x_recv.at[y, near[2], p], ypeer).start()
        x_to_partner(2, y, near[2]).start()

    def b_next(i):
        x_wait(1 - y, near[i], p)
        x_to_partner(4 + i, 1 - y, near[i]).start()

    def relay2():
        w_relay(2).start()
        w_copy_x(3).start()

    def back_own():
        for i in range(2):
            for b in range(2):
                b_own(b, i).start()

    def back_relay():
        for b in range(2):
            b_wait(b, (fx, fy)[b])
            b_relay(b).start()

    def body(k, carry):
        event(k, 0, lambda: w_ready(0))
        event(k, 2, a3)
        event(k, 4, lambda: w_ready(1))
        event(k, 4, relay2)
        event(k, 5, lambda: b_next(0))
        event(k, 7, lambda: w_relay(3).start())
        event(k, 8, lambda: w_ready(2))
        event(k, 9, lambda: b_next(1))
        event(k, 10, lambda: b_next(2))
        event(k, 10, back_own)
        event(k, 12, lambda: w_ready(3))
        event(k, 18, back_relay)

        je = k - LAG_E * hop_e

        @pl.when((je >= 0) & (je < steps))
        def _():
            step(0, je // nz, je % nz)

        jl = k - LAG_L * hop_l - LATE

        @pl.when((jl >= 0) & (jl < steps))
        def _():
            step(1, listed(LATE_MATS, jl), listed(LATE_CHUNKS, jl))

        return carry

    lax.fori_loop(0, steps + LATE + LAG_L * (nz - 1), body, 0)

    owner = hop_e == nz - 1
    is_end = (z == 0) | (z == nz - 1)
    hop = hop_l
    onward = toward_l

    def chain(b, q, c):
        view = yg.at[b, q, c]
        return remote(view, view, c_send.at[b, q, c], y_recv.at[b, q, c], onward)

    @pl.when(is_end)
    def _():
        for k in range(nz):
            view = start.at[piece(k, rs)]
            remote(view, view, s_send.at[0], s_recv.at[k], partner).wait_recv()
        e = hop_l // (nz - 1)
        small = group // 2

        def value_at(m, c):
            return obuf[e, m * nz + c]

        pool[0:HALO, :] = jnp.zeros((HALO, group), bf)
        for c in range(nz):
            cosine, sine = cosv[c * span : (c + 1) * span, :], sinv[c * span : (c + 1) * span, :]
            k_c = value_at(0, c).astype(f32)
            a, b = k_c[:, :small], k_c[:, small:]
            scale = group ** (-0.5)
            krot[c * span : (c + 1) * span, :small] = ((a * cosine - b * sine) * scale).astype(bf)
            krot[c * span : (c + 1) * span, small:] = ((a * sine + b * cosine) * scale).astype(bf)
            pool[HALO + c * span : HALO + (c + 1) * span, :] = value_at(3, c)
        window = 2 * (1 + y) * (1 + 3 * p)
        brow = lax.broadcasted_iota(jnp.int32, (span, span + HALO), 0)
        bcol = lax.broadcasted_iota(jnp.int32, (span, span + HALO), 1)
        behind = brow + HALO - bcol
        band = jnp.where((behind >= 0) & (behind < window), 1.0, 0.0).astype(bf)
        place = lax.broadcasted_iota(jnp.int32, (span, 1), 0)
        for c in ORDER:
            cosine, sine = cosv[c * span : (c + 1) * span, :], sinv[c * span : (c + 1) * span, :]
            q_c = value_at(1, c).astype(f32)
            a, b = q_c[:, :small], q_c[:, small:]
            rq = jnp.concatenate([a * cosine - b * sine, a * sine + b * cosine], axis=-1)
            fade = jnp.exp(-((place + c * span).astype(f32) + 1.0) * r)
            acc = jnp.dot((rq * fade).astype(bf), start[...], preferred_element_type=f32)
            rq = rq.astype(bf)
            for g in range(c + 1):
                scores = lax.dot_general(
                    rq, krot[g * span : (g + 1) * span, :], (((1,), (1,)), ((), ())), preferred_element_type=f32
                )
                scores = (scores * mask[c - g]).astype(bf)
                acc += jnp.dot(scores, value_at(2, g), preferred_element_type=f32)
            ret = (acc * lax.rsqrt(jnp.mean(acc * acc, axis=-1, keepdims=True) + eps)).astype(bf)
            rows_c = pool[c * span : (c + 1) * span + HALO, :]
            trail = jnp.dot(band, rows_c, preferred_element_type=f32)
            counts = jnp.minimum(window, place + c * span + 1).astype(f32)
            differ = (trail / counts - value_at(3, c).astype(f32)).astype(bf)
            pooled = (jnp.dot(differ, mapv[...], preferred_element_type=f32) * scv[...]).astype(bf)

            @pl.when(owner)
            def _():
                yg[1, y, c] = ret
                yg[0, y, c] = pooled
                chain(1, y, c).start()
                chain(0, y, c).start()

            @pl.when(jnp.logical_not(owner))
            def _():
                yb[1, c] = ret
                yb[0, c] = pooled
                for b in (1, 0):
                    remote(yb.at[b, c], yg.at[b, y, c], h_send.at[b, c], y_recv.at[b, y, c], ypeer).start()

    for b in range(2):
        own_b[b].wait()
        b_wait(b, (fy, fx)[b])
        b_wait(b, fd)

    def arrive(b, q, c):
        view = yg.at[b, q, c]
        remote(view, view, c_send.at[b, q, c], y_recv.at[b, q, c], partner).wait_recv()

    def pass_on(b, q, c):
        arrive(b, q, c)

        @pl.when(hop < nz - 1)
        def _():
            chain(b, q, c).start()

    across = backs.shape[2]

    def product(q, c):
        acc = jnp.zeros((span, across), f32)
        for b in range(2):
            acc += jnp.dot(yg[b, q, c], backs[b, piece(q, group), :], preferred_element_type=f32)
        return acc

    def early(c):
        @pl.when(hop > 0)
        def _():
            for b in (1, 0):
                pass_on(b, y, c)

    def give_copy(c):
        return remote(give.at[c], take.at[c], g_send.at[c], g_recv.at[c], partner)

    def multiply(c):
        keep[c] = keep[c] + product(1 - y, c)
        give[c] = keep[c, piece(1 - p, half), :].astype(bf)
        give_copy(c).start()

    def finish(c):
        give_copy(c).wait_recv()
        done[c] = (keep[c, piece(p, half), :] + take[c].astype(f32)).astype(bf)
        dst = out.at[:, piece(z, across)]

        @pl.when(z == c)
        def _():
            pltpu.make_async_copy(done.at[c], dst, o_recv.at[z]).start()

        @pl.when(z != c)
        def _():
            remote(done.at[c], dst, o_send.at[c], o_recv.at[z], at(c, y, x, p)).start()

    for c in ORDER:
        early(c)
        keep[c] = product(y, c)
    for i, c in enumerate(ORDER):
        for b in (1, 0):
            pass_on(b, 1 - y, c)
        multiply(c)

        for late in range(3):
            then = i - late
            if late == 0 and then >= 0:

                @pl.when(hop >= 2)
                def _():
                    finish(ORDER[then])
            if late == 2 and then >= 0:

                @pl.when(hop == 1)
                def _():
                    finish(ORDER[then])

    @pl.when(hop == 1)
    def _():
        for c in ORDER[2:]:
            finish(c)

    @pl.when(hop == 0)
    def _():
        for c in ORDER:
            finish(c)

    for k in range(nz):
        view = out.at[:, k * across : (k + 1) * across]
        remote(done.at[k], view, o_send.at[k], o_recv.at[k], partner).wait_recv()

        @pl.when(z != k)
        def _():
            remote(done.at[k], view, o_send.at[k], o_recv.at[k], partner).wait_send()

    @pl.when(hop < nz - 1)
    def _():
        for b in range(2):
            for q in range(2):
                for c in range(nz):
                    chain(b, q, c).wait_send()

    @pl.when(is_end & jnp.logical_not(owner))
    def _():
        for b in range(2):
            for c in range(nz):
                remote(yb.at[b, c], yb.at[b, c], h_send.at[b, c], y_recv.at[b, 0, c], partner).wait_send()

    for e in range(2):

        @pl.when((hop_e if e == 0 else hop_l) < nz - 1)
        def _():
            def drain(j, carry):
                remote(obuf.at[e, j], rbuf.at[e, j], r_send.at[e, j], r_recv.at[e, j], partner).wait_send()
                return carry

            lax.fori_loop(0, steps, drain, 0)

    for j in range(2):

        @pl.when(jnp.logical_not((z == toward) & (y == j)))
        def _():
            remote(stb.at[j], stb.at[j], s_send.at[j], s_recv.at[0], partner).wait_send()

    for c in range(nz):
        give_copy(c).wait_send()
    for m in (2, 3):
        view = wg.at[m, piece(fy, rows)]
        remote(view, view, wf_send.at[m], w_recv.at[m, fy], partner).wait_send()
    for b in range(2):
        for i in range(2):
            b_own(b, i).wait_send()
        b_relay(b).wait_send()
    w_copy_x(3).wait_send()
    for i in (2, 4, 5, 6):
        view = slot(xg, y, z, p)
        remote(view, view, xp_send.at[i], x_recv.at[y, z, p], partner).wait_send()
    view = slot(xg, y, z, p)
    remote(view, view, xy_send.at[2], x_recv.at[y, z, p], partner).wait_send()
    for c in sent:
        c.wait_send()


def rotary_tables(length, half_dim):
    inv_freq = np.float32(1.0) / np.power(
        np.float32(rope_base), np.linspace(0.0, 1.0, half_dim, dtype=np.float32)
    )
    angles = np.arange(length, dtype=np.float32)[:, None] * inv_freq[None, :].astype(np.float32)
    return np.cos(angles).astype(np.float32), np.sin(angles).astype(np.float32)


def paired(
    tokens, norm_gain, pool_proj, query_proj, key_proj, value_proj, pool_map, pool_scale,
    decay_rate, start_state, pool_back, retention_back,
):
    bf, f32 = jnp.bfloat16, jnp.float32
    nsp = lax.axis_size("sp")
    tok = tokens[0]
    span, width = tok.shape
    rows, two = pool_proj.shape
    group = two // 2
    length = nsp * span
    half = span // 2
    rs = start_state.shape[2]
    steps = 4 * nsp
    across = 4 * pool_back.shape[1]
    vm, hbm = pl.BlockSpec(memory_space=pltpu.VMEM), pl.BlockSpec(memory_space=pl.ANY)
    dma = pltpu.SemaphoreType.DMA
    cosine, sine = rotary_tables(length, group // 2)
    return pl.pallas_call(
        fused_kernel,
        out_shape=jax.ShapeDtypeStruct((half, width), bf),
        in_specs=[hbm] * 11 + [pl.BlockSpec(memory_space=pltpu.SMEM)] + [hbm] * 2,
        out_specs=vm,
        scratch_shapes=[
            pltpu.VMEM((half, width), bf),
            pltpu.VMEM((half, width), bf),
            pltpu.VMEM((2, length, width // nsp), bf),
            pltpu.VMEM((4, 4 * rows, group), bf),
            pltpu.VMEM((2, steps, span, group), bf),
            pltpu.VMEM((2, steps, span, group), bf),
            pltpu.VMEM((2, pool_back.shape[0], across), bf),
            pltpu.VMEM((1, width), f32),
            pltpu.VMEM((2, rs, group), f32),
            pltpu.VMEM((2, rs, group), bf),
            pltpu.VMEM((nsp * rs, group), bf),
            pltpu.VMEM((length, group // 2), f32),
            pltpu.VMEM((length, group // 2), f32),
            pltpu.VMEM((group, group), bf),
            pltpu.VMEM((1, group), f32),
            pltpu.VMEM((length, group), bf),
            pltpu.VMEM((HALO + length, group), bf),
            pltpu.VMEM((nsp, span, span), f32),
            pltpu.VMEM((2, nsp, span, group), bf),
            pltpu.VMEM((2, 2, nsp, span, group), bf),
            pltpu.VMEM((nsp, span, across), f32),
            pltpu.VMEM((nsp, half, across), bf),
            pltpu.VMEM((nsp, half, across), bf),
            pltpu.VMEM((nsp, half, across), bf),
            dma((7,)), dma((4,)), dma((2,)), dma((4,)), dma((4,)), dma((4,)), dma((4, 4)),
            dma((3,)), dma((4,)), dma((8,)), dma((2, nsp, 2)),
            dma((2,)), dma((nsp,)), dma((2, 3)), dma((2, 4)), dma((2, steps)), dma((2, steps)),
            dma((2, nsp)), dma((2, 2, nsp)), dma((2, 2, nsp)), dma((nsp,)), dma((nsp,)), dma((nsp,)), dma((nsp,)),
        ],
        compiler_params=pltpu.CompilerParams(collective_id=0, has_side_effects=True, vmem_limit_bytes=60 * 2**20),
        name="fused",
    )(
        tok, norm_gain[None, :], pool_proj, query_proj, key_proj, value_proj,
        start_state[0], pool_back, retention_back, pool_map,
        pool_scale.reshape(pool_map.shape[0], 1, group), decay_rate, jnp.asarray(cosine), jnp.asarray(sine),
    )[None]


def solution(mesh):
    sizes = mesh.shape
    small = sizes["sp"] == 4 and sizes["fs"] == 4 and sizes["tp"] == 2
    placed = (
        P("fs", "sp", None),
        P(),
        P(("sp", "fs"), "tp"),
        P(("sp", "fs"), "tp"),
        P(("sp", "fs"), "tp"),
        P(("sp", "fs"), "tp"),
        P(),
        P(),
        P("tp"),
        P("fs", "tp", "sp", None),
        P("tp", ("sp", "fs")),
        P("tp", ("sp", "fs")),
    )
    return jax.shard_map(
        paired if small else on_device,
        mesh=mesh,
        in_specs=placed,
        out_specs=P("fs", ("sp", "tp"), None),
        check_vma=False,
    )
```

```python
import numpy as np
from jax.experimental import pallas as pl
from jax.experimental.pallas import tpu as pltpu

import jax
import jax.numpy as jnp
from jax import lax
from jax.sharding import PartitionSpec as P

GROUPS = 4
BLOCK = 128
HALO = 16


eps = 1e-06
rope_base = 10000.0
highest_precision = lax.Precision.HIGHEST
window_list = (2, 4, 8, 16)


def shortened(x):
    return jax.tree.map(lambda a: a.astype(jnp.bfloat16) if a.dtype == jnp.float32 else a, x)


def shifted(x, axis, by):
    devices = lax.axis_size(axis)
    pairs = [(i, i + by) for i in range(devices) if 0 <= i + by < devices]
    return lax.ppermute(x, axis, pairs)


def carried_in(value, axis, join, neutral):
    count, mine = (lax.axis_size(axis), lax.axis_index(axis))
    pieces = jax.tree.map(lambda part: lax.all_gather(part, axis), value)
    running = jax.tree.map(
        lambda part, zero: jnp.full_like(part, 0) + jnp.asarray(zero, part.dtype), value, neutral
    )

    def turn(position, running):
        longer = join(running, jax.tree.map(lambda part: part[position], pieces))
        return jax.tree.map(lambda new, old: jnp.where(position < mine, new, old), longer, running)

    return lax.fori_loop(0, count - 1, turn, running)


def rotate(values, positions):
    half_dim = values.shape[-1] // 2
    inv_freq = 1.0 / rope_base ** jnp.linspace(0.0, 1.0, half_dim, dtype=jnp.float32)
    angles = positions.astype(jnp.float32)[:, None] * inv_freq[None, :]
    cosine = jnp.cos(angles)[:, None, :]
    sine = jnp.sin(angles)[:, None, :]
    first_half = values[..., :half_dim]
    second_half = values[..., half_dim:]
    return jnp.concatenate(
        [first_half * cosine - second_half * sine, first_half * sine + second_half * cosine],
        axis=-1,
    )


def trailing_sums(extended, length):
    begin = extended.shape[0] - length
    running = extended[begin:]
    results = []
    for behind in range(1, 16):
        running = running + extended[begin - behind : begin - behind + length]
        if behind + 1 in window_list:
            results.append(running)
    return results


def reshape_blocks(array):
    return array.reshape((array.shape[0] // BLOCK, BLOCK) + array.shape[1:])


def block_retention(queries, keys_in, values_in, decay_rate, initial):
    length, head_count, head_dim = queries.shape
    within = jnp.arange(BLOCK, dtype=jnp.float32)
    distance = within[:, None] - within[None, :]
    decay_mask = jnp.where(
        distance[None] >= 0,
        jnp.exp(-jnp.maximum(distance, 0.0)[None] * decay_rate[:, None, None]),
        0.0,
    )
    query_decay_factor = jnp.exp(-(within + 1.0)[:, None] * decay_rate[None, :])
    key_decay_factor = jnp.exp(-(BLOCK - 1.0 - within)[:, None] * decay_rate[None, :])
    block_decay_factor = jnp.exp(-BLOCK * decay_rate)

    def advance(state_carry, inputs):
        block_queries, block_keys, block_values = inputs
        scores = (
            jnp.einsum("ihk,jhk->hij", block_queries, block_keys, precision=highest_precision)
            * decay_mask
        )
        inside = jnp.einsum("hij,jhv->ihv", scores, block_values, precision=highest_precision)
        across_blocks = jnp.einsum(
            "bzy,zyx->bzx",
            block_queries * query_decay_factor[:, :, None],
            state_carry,
            precision=highest_precision,
        )
        state_carry = state_carry * block_decay_factor[:, None, None] + jnp.einsum(
            "flm,fld->lmd",
            block_keys * key_decay_factor[:, :, None],
            block_values,
            precision=highest_precision,
        )
        return (state_carry, inside + across_blocks)

    final_state, outputs = lax.scan(
        advance,
        initial,
        (reshape_blocks(queries), reshape_blocks(keys_in), reshape_blocks(values_in)),
    )
    return (outputs.reshape(length, head_count, values_in.shape[-1]), final_state)


def combine_states(earlier, latter):
    return (earlier[0] * latter[0], latter[0][:, None, None] * earlier[1] + latter[1])


def on_device(
    tokens,
    norm_gain,
    pool_proj,
    query_proj,
    key_proj,
    value_proj,
    pool_map,
    pool_scale,
    decay_rate,
    start_state,
    pool_back,
    retention_back,
):
    sequence = tokens[0]
    length = sequence.shape[0]
    tp_index = lax.axis_index("tp")
    sp_index = lax.axis_index("sp")
    tp_count = lax.axis_size("tp")
    floats = sequence.astype(jnp.float32)
    normed = (
        floats * lax.rsqrt(jnp.mean(floats * floats, axis=-1, keepdims=True) + eps) * norm_gain
    ).astype(jnp.bfloat16)
    group_normed = lax.all_gather(normed, "fs", axis=0, tiled=True)
    quarters = (
        lax.all_to_all(pool_proj, "fs", split_axis=1, concat_axis=0, tiled=True),
        lax.all_to_all(query_proj, "fs", split_axis=1, concat_axis=0, tiled=True),
        lax.all_to_all(key_proj, "fs", split_axis=1, concat_axis=0, tiled=True),
        lax.all_to_all(value_proj, "fs", split_axis=1, concat_axis=0, tiled=True),
    )
    pieces = (
        lax.all_gather(quarters[0], "sp", axis=0, tiled=True),
        lax.all_gather(quarters[1], "sp", axis=0, tiled=True),
        lax.all_gather(quarters[2], "sp", axis=0, tiled=True),
        lax.all_gather(quarters[3], "sp", axis=0, tiled=True),
    )
    partial_cols = tuple(
        (jnp.dot(group_normed, piece_w, preferred_element_type=jnp.float32) for piece_w in pieces)
    )
    rounded = tuple((result.astype(jnp.bfloat16) for result in partial_cols))
    pool_in, query_bf, key_bf, value_bf = jax.tree.map(
        lambda part, own: part.astype(own.dtype),
        lax.all_to_all(shortened(rounded), "fs", split_axis=0, concat_axis=1, tiled=True),
        rounded,
    )
    positions = jnp.arange(length, dtype=jnp.int32) + sp_index * length
    before = shifted(pool_in[length - HALO :], "sp", 1)
    extended = jnp.concatenate([before, pool_in], axis=0).astype(jnp.float32)
    stacked = jnp.stack(trailing_sums(extended, length))
    local_groups = GROUPS // tp_count
    channels = pool_in.shape[1]
    group_dim = channels // local_groups
    group_maps = lax.dynamic_slice_in_dim(pool_map, tp_index * local_groups, local_groups, 0)
    scales = lax.dynamic_slice_in_dim(pool_scale, tp_index * channels, channels, 0)
    windows = jnp.array(window_list, dtype=jnp.int32)
    pieces = []
    for group_idx in range(local_groups):
        chosen_group = tp_index * local_groups + group_idx
        lower = group_idx * group_dim
        chosen = lax.dynamic_index_in_dim(stacked, chosen_group, 0, keepdims=False)[
            :, lower : lower + group_dim
        ]
        counts = jnp.minimum(windows[chosen_group], positions + 1).astype(jnp.float32)
        inputs = extended[HALO:, lower : lower + group_dim]
        differ = (chosen / counts[:, None] - inputs).astype(jnp.bfloat16)
        pieces.append(jnp.dot(differ, group_maps[group_idx], preferred_element_type=jnp.float32))
    pool_out = (jnp.concatenate(pieces, axis=1) * scales).astype(jnp.bfloat16)
    head_count = decay_rate.shape[0]
    head_dim = query_bf.shape[1] // head_count
    queries = rotate(query_bf.astype(jnp.float32).reshape(length, head_count, head_dim), positions)
    keys_in = rotate(
        key_bf.astype(jnp.float32).reshape(length, head_count, head_dim), positions
    ) * head_dim ** (-0.5)
    values_in = value_bf.astype(jnp.float32).reshape(length, head_count, head_dim)
    zeros_state = jnp.zeros((head_count, head_dim, head_dim), jnp.float32)
    local_output, local_state = block_retention(
        queries, keys_in, values_in, decay_rate, zeros_state
    )
    span_decay = jnp.exp(-decay_rate * length)
    whole_start = lax.all_gather(start_state, "sp", axis=2, tiled=True)[0]
    span_factor, carried_over = carried_in(
        (span_decay, local_state), "sp", combine_states, (jnp.ones_like(span_decay), zeros_state)
    )
    offset_float = (sp_index * length).astype(jnp.float32)
    carried_over = carried_over + jnp.exp(-decay_rate * offset_float)[:, None, None] * whole_start
    steps_in = jnp.arange(length, dtype=jnp.float32) + 1.0
    query_rows_scaled = queries * jnp.exp(-steps_in[:, None] * decay_rate[None, :])[:, :, None]
    retained_output = local_output + jnp.einsum(
        "lpi,pib->lpb", query_rows_scaled, carried_over, precision=highest_precision
    )
    retained_output = retained_output * lax.rsqrt(
        jnp.mean(retained_output * retained_output, axis=-1, keepdims=True) + eps
    )
    ret_out = retained_output.reshape(length, head_count * head_dim).astype(jnp.bfloat16)
    pool_cols, retention_cols = (
        lax.all_gather(pool_back, ("sp", "fs"), axis=1, tiled=True),
        lax.all_gather(retention_back, ("sp", "fs"), axis=1, tiled=True),
    )
    weight_local = jnp.concatenate([pool_cols, retention_cols], axis=0)
    joined = jnp.concatenate([pool_out, ret_out], axis=1)
    mixed = lax.psum_scatter(
        jnp.dot(joined, weight_local, preferred_element_type=jnp.float32).astype(jnp.bfloat16),
        "tp",
        scatter_dimension=0,
        tiled=True,
    )
    return mixed[None]


MESH = pl.DeviceIdType.MESH
ORDER = (0, 3, 1, 2)
STEPS = (
    (0, 0, 0, 10.0), (0, 0, 1, 10.7), (0, 1, 0, 14.0), (0, 1, 1, 14.7), (0, 0, 2, 15.4), (0, 1, 2, 16.1), (0, 0, 3, 16.8), (0, 1, 3, 17.5),
    (1, 0, 1, 18.2), (1, 1, 1, 18.9), (0, 2, 0, 20.3), (0, 2, 1, 21.0), (0, 2, 2, 21.7), (0, 2, 3, 22.4),
    (1, 2, 1, 23.1), (1, 0, 0, 23.8), (1, 1, 0, 24.5), (1, 2, 0, 25.2),
    (0, 3, 0, 25.9), (0, 3, 1, 26.6), (0, 3, 2, 27.3), (0, 3, 3, 28.0),
    (1, 0, 2, 28.7), (1, 1, 2, 29.4), (1, 2, 2, 30.1), (1, 0, 3, 30.8), (1, 1, 3, 31.5), (1, 2, 3, 32.2),
    (1, 3, 0, 32.9), (1, 3, 1, 33.6), (1, 3, 2, 34.3), (1, 3, 3, 35.0),
)
HOP = 2.7
NEAR = ((1, 2, 3), (0, 2, 3), (3, 1, 0), (2, 1, 0))


def places(when, needs):
    result = []
    for hop in range(4):
        due = [n for n, step in enumerate(STEPS) if step[3] + HOP * hop >= when] + [len(STEPS)]
        used = [n for n, step in enumerate(STEPS) if needs(hop, *step[:3])] + [len(STEPS)]
        result.append(min(due[0], used[0]))
    return tuple(result)


def where_am_i():
    sp, fs, tp = (lax.axis_index(name) for name in ("sp", "fs", "tp"))
    return sp, fs // 2, fs % 2, tp


def at(z, y, x, p):
    return (z, 2 * y + x, p)


def remote(src, dst, send, recv, target):
    return pltpu.make_async_remote_copy(
        src_ref=src, dst_ref=dst, send_sem=send, recv_sem=recv, device_id=target, device_id_type=MESH
    )


def piece(index, size):
    return pl.ds(pl.multiple_of(index * size, size), size)


def fused_kernel(
    tok, gain, wp, wq, wk, wv, state, pb, rb, pmap, pscale, rate, cos_t, sin_t,
    out,
    xt, xn, xg, wg, obuf, rbuf, backs, gv, st, stb, start, cosv, sinv, mapv, scv,
    krot, pool, mask, yb, yg, keep, give, take, done,
    l_sem, wl_sem, bl_sem, wy_send, wx_send, wf_send, w_recv,
    xz_send, xy_send, xp_send, x_recv,
    s_send, s_recv, b_send, b_recv, r_send, r_recv,
    h_send, c_send, y_recv, g_send, g_recv, o_send, o_recv,
):
    f32, bf = jnp.float32, jnp.bfloat16
    z, y, x, p = where_am_i()
    nz = 4
    half, width = xt.shape
    span = 2 * half
    feats = width // nz
    rows = wp.shape[0]
    group = wp.shape[1] // 2
    steps = 4 * nz
    mats = (wk, wq, wv, wp)
    fs = 2 * y + x
    me = at(z, y, x, p)
    partner = at(z, y, x, 1 - p)
    ypeer = at(z, 1 - y, x, p)
    xpeer = at(z, y, 1 - x, p)
    head = 2 * p + y

    barrier = pltpu.get_barrier_semaphore()
    others = [partner, xpeer]
    for dz in range(nz):
        for dy in range(2):
            if dz or dy:
                others.append(at((z + dz) % nz, (y + dy) % 2, x, p))
    for other in others:
        pl.semaphore_signal(barrier, inc=1, device_id=other, device_id_type=MESH)

    loads = [
        pltpu.make_async_copy(tok.at[piece(p, half)], xt, l_sem.at[0]),
        pltpu.make_async_copy(gain, gv, l_sem.at[1]),
        pltpu.make_async_copy(state, st, l_sem.at[2]),
        pltpu.make_async_copy(cos_t, cosv, l_sem.at[3]),
        pltpu.make_async_copy(sin_t, sinv, l_sem.at[4]),
        pltpu.make_async_copy(pmap.at[head], mapv, l_sem.at[5]),
        pltpu.make_async_copy(pscale.at[head], scv, l_sem.at[6]),
    ]
    for c in loads:
        c.start()
    own_w = []
    for m in range(4):
        c = pltpu.make_async_copy(mats[m].at[:, piece(y, group)], wg.at[m, piece(fs, rows)], wl_sem.at[m])
        c.start()
        own_w.append(c)
    loads[0].wait()
    loads[1].wait()

    block = 16
    for i in range(half // block):
        floats = xt[i * block : (i + 1) * block, :].astype(f32)
        xn[i * block : (i + 1) * block, :] = (
            floats * lax.rsqrt(jnp.mean(floats * floats, axis=-1, keepdims=True) + eps) * gv[...]
        ).astype(bf)

    def slot(ref, s, c, h):
        return ref.at[s, pl.ds(pl.multiple_of(c * span + h * half, half), half)]

    pl.semaphore_wait(barrier, len(others))

    sent = []

    def go(c):
        c.start()
        sent.append(c)

    def w_y(m):
        go(remote(mats[m].at[:, piece(1 - y, group)], wg.at[m, piece(fs, rows)], wy_send.at[m], w_recv.at[m, fs], ypeer))

    def w_copy_x(m):
        return remote(mats[m].at[:, piece(y, group)], wg.at[m, piece(fs, rows)], wx_send.at[m], w_recv.at[m, fs], xpeer)

    def w_x(m):
        go(w_copy_x(m))

    def w_wait(m, f):
        view = wg.at[m, piece(f, rows)]
        remote(view, view, wf_send.at[m], w_recv.at[m, f], partner).wait_recv()

    fy = 2 * (1 - y) + x

    def w_relay(m):
        w_wait(m, fy)
        view = wg.at[m, piece(fy, rows)]
        return remote(view, view, wf_send.at[m], w_recv.at[m, fy], xpeer)

    hi = z // 2
    zz = z * (1 - hi) + (3 - z) * hi
    near = [o * (1 - hi) + (3 - o) * hi for o in (1 - zz, 2, 3)]
    hop = (nz - 1 - z) * (1 - p) + z * p
    toward = at(z - 1 + 2 * p, y, x, p)
    onward = at(z + 1 - 2 * p, y, x, p)
    goal = (nz - 1) * p

    w_y(0)
    w_x(0)
    for i, c in enumerate(near):
        go(remote(xn.at[:, piece(c, feats)], slot(xg, y, z, p), xz_send.at[i], x_recv.at[y, z, p], at(c, y, x, p)))
    xg[y, pl.ds(pl.multiple_of(z * span + p * half, half), half), :] = xn[:, piece(z, feats)]

    def x_wait(s, c, h):
        view = slot(xg, s, c, h)
        remote(view, view, xp_send.at[0], x_recv.at[s, c, h], partner).wait_recv()

    def x_to_y(i, c):
        view = slot(xg, y, c, p)
        go(remote(view, view, xy_send.at[i], x_recv.at[y, c, p], ypeer))

    def x_to_partner(i, s, c):
        view = slot(xg, s, c, p)
        return remote(view, view, xp_send.at[i], x_recv.at[s, c, p], partner)

    w_y(1)
    w_x(1)
    go(remote(xn.at[:, piece(z, feats)], slot(xg, y, z, p), xp_send.at[3], x_recv.at[y, z, p], partner))
    go(remote(xn.at[:, piece(z, feats)], slot(xg, y, z, p), xy_send.at[3], x_recv.at[y, z, p], ypeer))
    w_y(2)

    loads[2].wait()
    for j in range(2):
        stb[j] = st[j].astype(bf)
    rs = st.shape[1]
    for j in range(2):
        same = (z == goal) & (y == j)
        dst = start.at[y, piece(z, rs)]

        @pl.when(same)
        def _():
            pltpu.make_async_copy(stb.at[j], dst, s_recv.at[y, z]).start()

        @pl.when(jnp.logical_not(same))
        def _():
            remote(stb.at[j], dst, s_send.at[j], s_recv.at[y, z], at(goal, j, x, p)).start()

    r = rate[y]
    row = lax.broadcasted_iota(jnp.int32, (span, span), 0)
    col = lax.broadcasted_iota(jnp.int32, (span, span), 1)
    gap = row - col
    for k in range(nz):
        dist = (gap + k * span).astype(f32)
        value = jnp.exp(-jnp.maximum(dist, 0.0) * r)
        mask[k] = jnp.where(dist >= 0.0, value, 0.0) if k == 0 else value
    for c in loads[3:]:
        c.wait()

    x_wait(y, near[0], p)
    x_to_y(0, near[0])
    go(x_to_partner(0, y, near[0]))
    go(w_relay(0))
    w_y(3)
    go(w_relay(1))
    w_x(2)
    own_b = []
    for b, back in enumerate((pb, rb)):
        c = pltpu.make_async_copy(back, backs.at[b, :, piece(fs, rows)], bl_sem.at[b])
        c.start()
        own_b.append(c)
    fx = 2 * y + 1 - x
    fd = 2 * (1 - y) + 1 - x

    def b_own(b, i):
        back = (pb, rb)[b]
        target = ((xpeer, ypeer), (ypeer, xpeer))[b][i]
        return remote(back, backs.at[b, :, piece(fs, rows)], b_send.at[b, i], b_recv.at[b, fs], target)

    def b_wait(b, f):
        view = backs.at[b, :, piece(f, rows)]
        remote(view, view, b_send.at[b, 2], b_recv.at[b, f], partner).wait_recv()

    def b_relay(b):
        f, second = ((fx, ypeer), (fy, xpeer))[b]
        view = backs.at[b, :, piece(f, rows)]
        return remote(view, view, b_send.at[b, 2], b_recv.at[b, f], second)

    def by_place(values):
        result = values[3]
        for h in (2, 1, 0):
            result = jnp.where(hop == h, values[h], result)
        return result

    def listed(table, n):
        words = []
        for part in (table[:16], table[16:]):
            word = sum(v << (2 * i) for i, v in enumerate(part))
            words.append(np.int32(word - 2**32 if word >= 2**31 else word))
        return lax.shift_right_logical(jnp.where(n < 16, words[0], words[1]), 2 * (n % 16)) & 3

    def step(n):
        e, m, i = (listed([entry[k] for entry in STEPS], n) for k in range(3))
        s = y + e * (1 - 2 * y)
        c = (nz - 1 - i) * (1 - p) + i * p
        at_slot = m * nz + c

        @pl.when(m == 0)
        def _():
            x_wait(s, c, 1 - p)

        acc = jnp.dot(xg[s, piece(c, span), :], wg[m], preferred_element_type=f32)
        send, recv = r_send.at[e, at_slot], r_recv.at[e, at_slot]

        @pl.when(hop == 0)
        def _():
            obuf[e, at_slot] = acc.astype(bf)

        @pl.when(hop > 0)
        def _():
            remote(rbuf.at[e, at_slot], rbuf.at[e, at_slot], send, recv, partner).wait_recv()
            obuf[e, at_slot] = (acc + rbuf[e, at_slot].astype(f32)).astype(bf)

        @pl.when(hop < nz - 1)
        def _():
            remote(obuf.at[e, at_slot], rbuf.at[e, at_slot], send, recv, toward).start()

    def w_ready(m):
        own_w[m].wait()
        w_wait(m, fx)
        w_wait(m, fd)

    def event(n, when, act):
        @pl.when(n == by_place(when))
        def _():
            act()

    def a_next(i):
        x_wait(y, near[i], p)
        view = slot(xg, y, near[i], p)
        remote(view, view, xy_send.at[i], x_recv.at[y, near[i], p], ypeer).start()
        x_to_partner(i, y, near[i]).start()

    def b_next(i, c):
        x_wait(1 - y, c, p)
        x_to_partner(4 + i, 1 - y, c).start()

    def relay2():
        w_relay(2).start()
        w_copy_x(3).start()

    def back_own():
        for i in range(2):
            for b in range(2):
                b_own(b, i).start()

    def back_relay():
        for b in range(2):
            b_wait(b, (fx, fy)[b])
            b_relay(b).start()

    def chain(b, q, c):
        view = yg.at[b, q, c]
        return remote(view, view, c_send.at[b, q, c], y_recv.at[b, q, c], onward)

    def heads(e):
        s = y if e == 0 else 1 - y
        for k in range(nz):
            view = start.at[s, piece(k, rs)]
            remote(view, view, s_send.at[0], s_recv.at[s, k], partner).wait_recv()
        small = group // 2

        def value_at(m, c):
            return obuf[e, m * nz + c]

        pool[0:HALO, :] = jnp.zeros((HALO, group), bf)
        for c in range(nz):
            cosine, sine = cosv[c * span : (c + 1) * span, :], sinv[c * span : (c + 1) * span, :]
            k_c = value_at(0, c).astype(f32)
            a, b = k_c[:, :small], k_c[:, small:]
            scale = group ** (-0.5)
            krot[c * span : (c + 1) * span, :small] = ((a * cosine - b * sine) * scale).astype(bf)
            krot[c * span : (c + 1) * span, small:] = ((a * sine + b * cosine) * scale).astype(bf)
            pool[HALO + c * span : HALO + (c + 1) * span, :] = value_at(3, c)
        window = 2 * (1 + y) * (1 + 3 * p)
        brow = lax.broadcasted_iota(jnp.int32, (span, span + HALO), 0)
        bcol = lax.broadcasted_iota(jnp.int32, (span, span + HALO), 1)
        behind = brow + HALO - bcol
        band = jnp.where((behind >= 0) & (behind < window), 1.0, 0.0).astype(bf)
        place = lax.broadcasted_iota(jnp.int32, (span, 1), 0)
        for c in ORDER:
            cosine, sine = cosv[c * span : (c + 1) * span, :], sinv[c * span : (c + 1) * span, :]
            q_c = value_at(1, c).astype(f32)
            a, b = q_c[:, :small], q_c[:, small:]
            rq = jnp.concatenate([a * cosine - b * sine, a * sine + b * cosine], axis=-1)
            fade = jnp.exp(-((place + c * span).astype(f32) + 1.0) * r)
            acc = jnp.dot((rq * fade).astype(bf), start[s], preferred_element_type=f32)
            rq = rq.astype(bf)
            for g in range(c + 1):
                scores = lax.dot_general(
                    rq, krot[g * span : (g + 1) * span, :], (((1,), (1,)), ((), ())), preferred_element_type=f32
                )
                scores = (scores * mask[c - g]).astype(bf)
                acc += jnp.dot(scores, value_at(2, g), preferred_element_type=f32)
            ret = (acc * lax.rsqrt(jnp.mean(acc * acc, axis=-1, keepdims=True) + eps)).astype(bf)
            rows_c = pool[c * span : (c + 1) * span + HALO, :]
            trail = jnp.dot(band, rows_c, preferred_element_type=f32)
            counts = jnp.minimum(window, place + c * span + 1).astype(f32)
            differ = (trail / counts - value_at(3, c).astype(f32)).astype(bf)
            pooled = (jnp.dot(differ, mapv[...], preferred_element_type=f32) * scv[...]).astype(bf)

            if e == 0:
                yg[1, y, c] = ret
                yg[0, y, c] = pooled
                for b in (1, 0):
                    chain(b, y, c).start()
            else:
                yb[1, c] = ret
                yb[0, c] = pooled
                for b in (1, 0):
                    remote(yb.at[b, c], yg.at[b, y, c], h_send.at[b, c], y_recv.at[b, y, c], ypeer).start()

    def early_heads():
        @pl.when(hop == nz - 1)
        def _():
            heads(0)

    done_early = 1 + max(n for n, entry in enumerate(STEPS) if entry[0] == 0)
    events = (
        (places(0.0, lambda h, e, m, i: m == 0), lambda: w_ready(0)),
        (places(10.5, lambda h, e, m, i: e == 1 and i == h), lambda: b_next(3, z)),
        (places(12.5, lambda h, e, m, i: e == 0 and i == NEAR[h][1]), lambda: a_next(1)),
        (places(13.2, lambda h, e, m, i: e == 0 and i == NEAR[h][2]), lambda: a_next(2)),
        (places(13.3, lambda h, e, m, i: m == 2), relay2),
        (places(13.5, lambda h, e, m, i: m == 1), lambda: w_ready(1)),
        (places(16.4, lambda h, e, m, i: e == 1 and i == NEAR[h][0]), lambda: b_next(0, near[0])),
        (places(18.5, lambda h, e, m, i: m == 3), lambda: w_relay(3).start()),
        (places(20.0, lambda h, e, m, i: m == 2), lambda: w_ready(2)),
        (places(22.0, lambda h, e, m, i: e == 1 and i == NEAR[h][1]), lambda: b_next(1, near[1])),
        (places(24.8, lambda h, e, m, i: e == 1 and i == NEAR[h][2]), lambda: b_next(2, near[2])),
        (places(25.2, lambda h, e, m, i: False), back_own),
        (places(25.5, lambda h, e, m, i: m == 3), lambda: w_ready(3)),
        ((done_early,) * 4, early_heads),
        (places(36.5, lambda h, e, m, i: False), back_relay),
    )

    def body(n, carry):
        for when, act in events:
            event(n, when, act)
        step(n)
        return carry

    lax.fori_loop(0, 2 * steps, body, 0)
    event(2 * steps, *events[-1])

    @pl.when(hop == nz - 1)
    def _():
        heads(1)

    far = nz - 1 - hop

    def arrive(b, q, c):
        view = yg.at[b, q, c]
        remote(view, view, c_send.at[b, q, c], y_recv.at[b, q, c], partner).wait_recv()

    def pass_on(b, q, c):
        arrive(b, q, c)

        @pl.when(far < nz - 1)
        def _():
            chain(b, q, c).start()

    across = backs.shape[2]

    def product(q, c):
        acc = jnp.zeros((span, across), f32)
        for b in range(2):
            acc += jnp.dot(yg[b, q, c], backs[b, piece(q, group), :], preferred_element_type=f32)
        return acc

    def early(c):
        @pl.when(far > 0)
        def _():
            for b in (1, 0):
                pass_on(b, y, c)

    def give_copy(c):
        return remote(give.at[c], take.at[c], g_send.at[c], g_recv.at[c], partner)

    def multiply(c):
        keep[c] = keep[c] + product(1 - y, c)
        give[c] = keep[c, piece(1 - p, half), :].astype(bf)
        give_copy(c).start()

    def finish(c):
        give_copy(c).wait_recv()
        done[c] = (keep[c, piece(p, half), :] + take[c].astype(f32)).astype(bf)
        dst = out.at[:, piece(z, across)]

        @pl.when(z == c)
        def _():
            pltpu.make_async_copy(done.at[c], dst, o_recv.at[z]).start()

        @pl.when(z != c)
        def _():
            remote(done.at[c], dst, o_send.at[c], o_recv.at[z], at(c, y, x, p)).start()

    for c in ORDER:
        early(c)
    for b in range(2):
        own_b[b].wait()
        b_wait(b, (fy, fx)[b])
        b_wait(b, fd)
    for c in ORDER:
        keep[c] = product(y, c)
    for i, c in enumerate(ORDER):
        for b in (1, 0):
            pass_on(b, 1 - y, c)
        multiply(c)

        for late in range(3):
            then = i - late
            if late == 0 and then >= 0:

                @pl.when(far >= 2)
                def _():
                    finish(ORDER[then])
            if late == 2 and then >= 0:

                @pl.when(far == 1)
                def _():
                    finish(ORDER[then])

    @pl.when(far == 1)
    def _():
        for c in ORDER[2:]:
            finish(c)

    @pl.when(far == 0)
    def _():
        for c in ORDER:
            finish(c)

    for k in range(nz):
        view = out.at[:, k * across : (k + 1) * across]
        remote(done.at[k], view, o_send.at[k], o_recv.at[k], partner).wait_recv()

        @pl.when(z != k)
        def _():
            remote(done.at[k], view, o_send.at[k], o_recv.at[k], partner).wait_send()

    @pl.when(hop > 0)
    def _():
        for b in range(2):
            for q in range(2):
                for c in range(nz):
                    chain(b, q, c).wait_send()

    @pl.when(hop == nz - 1)
    def _():
        for b in range(2):
            for c in range(nz):
                remote(yb.at[b, c], yb.at[b, c], h_send.at[b, c], y_recv.at[b, 0, c], partner).wait_send()

    @pl.when(hop < nz - 1)
    def _():
        for e in range(2):

            def drain(j, carry):
                remote(obuf.at[e, j], rbuf.at[e, j], r_send.at[e, j], r_recv.at[e, j], partner).wait_send()
                return carry

            lax.fori_loop(0, steps, drain, 0)

    for j in range(2):

        @pl.when(jnp.logical_not((z == goal) & (y == j)))
        def _():
            remote(stb.at[j], stb.at[j], s_send.at[j], s_recv.at[0, 0], partner).wait_send()

    for c in range(nz):
        give_copy(c).wait_send()
    for m in (2, 3):
        view = wg.at[m, piece(fy, rows)]
        remote(view, view, wf_send.at[m], w_recv.at[m, fy], partner).wait_send()
    for b in range(2):
        for i in range(2):
            b_own(b, i).wait_send()
        b_relay(b).wait_send()
    w_copy_x(3).wait_send()
    for i in (1, 2, 4, 5, 6, 7):
        view = slot(xg, y, z, p)
        remote(view, view, xp_send.at[i], x_recv.at[y, z, p], partner).wait_send()
    view = slot(xg, y, z, p)
    for i in (1, 2):
        remote(view, view, xy_send.at[i], x_recv.at[y, z, p], partner).wait_send()
    for c in sent:
        c.wait_send()


def rotary_tables(length, half_dim):
    inv_freq = np.float32(1.0) / np.power(
        np.float32(rope_base), np.linspace(0.0, 1.0, half_dim, dtype=np.float32)
    )
    angles = np.arange(length, dtype=np.float32)[:, None] * inv_freq[None, :].astype(np.float32)
    return np.cos(angles).astype(np.float32), np.sin(angles).astype(np.float32)


def paired(
    tokens, norm_gain, pool_proj, query_proj, key_proj, value_proj, pool_map, pool_scale,
    decay_rate, start_state, pool_back, retention_back,
):
    bf, f32 = jnp.bfloat16, jnp.float32
    nsp = lax.axis_size("sp")
    tok = tokens[0]
    span, width = tok.shape
    rows, two = pool_proj.shape
    group = two // 2
    length = nsp * span
    half = span // 2
    rs = start_state.shape[2]
    steps = 4 * nsp
    across = 4 * pool_back.shape[1]
    vm, hbm = pl.BlockSpec(memory_space=pltpu.VMEM), pl.BlockSpec(memory_space=pl.ANY)
    dma = pltpu.SemaphoreType.DMA
    cosine, sine = rotary_tables(length, group // 2)
    return pl.pallas_call(
        fused_kernel,
        out_shape=jax.ShapeDtypeStruct((half, width), bf),
        in_specs=[hbm] * 11 + [pl.BlockSpec(memory_space=pltpu.SMEM)] + [hbm] * 2,
        out_specs=vm,
        scratch_shapes=[
            pltpu.VMEM((half, width), bf),
            pltpu.VMEM((half, width), bf),
            pltpu.VMEM((2, length, width // nsp), bf),
            pltpu.VMEM((4, 4 * rows, group), bf),
            pltpu.VMEM((2, steps, span, group), bf),
            pltpu.VMEM((2, steps, span, group), bf),
            pltpu.VMEM((2, pool_back.shape[0], across), bf),
            pltpu.VMEM((1, width), f32),
            pltpu.VMEM((2, rs, group), f32),
            pltpu.VMEM((2, rs, group), bf),
            pltpu.VMEM((2, nsp * rs, group), bf),
            pltpu.VMEM((length, group // 2), f32),
            pltpu.VMEM((length, group // 2), f32),
            pltpu.VMEM((group, group), bf),
            pltpu.VMEM((1, group), f32),
            pltpu.VMEM((length, group), bf),
            pltpu.VMEM((HALO + length, group), bf),
            pltpu.VMEM((nsp, span, span), f32),
            pltpu.VMEM((2, nsp, span, group), bf),
            pltpu.VMEM((2, 2, nsp, span, group), bf),
            pltpu.VMEM((nsp, span, across), f32),
            pltpu.VMEM((nsp, half, across), bf),
            pltpu.VMEM((nsp, half, across), bf),
            pltpu.VMEM((nsp, half, across), bf),
            dma((7,)), dma((4,)), dma((2,)), dma((4,)), dma((4,)), dma((4,)), dma((4, 4)),
            dma((3,)), dma((4,)), dma((8,)), dma((2, nsp, 2)),
            dma((2,)), dma((2, nsp)), dma((2, 3)), dma((2, 4)), dma((2, steps)), dma((2, steps)),
            dma((2, nsp)), dma((2, 2, nsp)), dma((2, 2, nsp)), dma((nsp,)), dma((nsp,)), dma((nsp,)), dma((nsp,)),
        ],
        compiler_params=pltpu.CompilerParams(collective_id=0, has_side_effects=True, vmem_limit_bytes=60 * 2**20),
        name="fused",
    )(
        tok, norm_gain[None, :], pool_proj, query_proj, key_proj, value_proj,
        start_state[0], pool_back, retention_back, pool_map,
        pool_scale.reshape(pool_map.shape[0], 1, group), decay_rate, jnp.asarray(cosine), jnp.asarray(sine),
    )[None]


def solution(mesh):
    sizes = mesh.shape
    small = sizes["sp"] == 4 and sizes["fs"] == 4 and sizes["tp"] == 2
    placed = (
        P("fs", "sp", None),
        P(),
        P(("sp", "fs"), "tp"),
        P(("sp", "fs"), "tp"),
        P(("sp", "fs"), "tp"),
        P(("sp", "fs"), "tp"),
        P(),
        P(),
        P("tp"),
        P("fs", "tp", "sp", None),
        P("tp", ("sp", "fs")),
        P("tp", ("sp", "fs")),
    )
    return jax.shard_map(
        paired if small else on_device,
        mesh=mesh,
        in_specs=placed,
        out_specs=P("fs", ("sp", "tp"), None),
        check_vma=False,
    )
```

```python
import numpy as np
from jax.experimental import pallas as pl
from jax.experimental.pallas import tpu as pltpu

import jax
import jax.numpy as jnp
from jax import lax
from jax.sharding import PartitionSpec as P

GROUPS = 4
BLOCK = 128
HALO = 16


eps = 1e-06
rope_base = 10000.0
highest_precision = lax.Precision.HIGHEST
window_list = (2, 4, 8, 16)


def shortened(x):
    return jax.tree.map(lambda a: a.astype(jnp.bfloat16) if a.dtype == jnp.float32 else a, x)


def shifted(x, axis, by):
    devices = lax.axis_size(axis)
    pairs = [(i, i + by) for i in range(devices) if 0 <= i + by < devices]
    return lax.ppermute(x, axis, pairs)


def carried_in(value, axis, join, neutral):
    count, mine = (lax.axis_size(axis), lax.axis_index(axis))
    pieces = jax.tree.map(lambda part: lax.all_gather(part, axis), value)
    running = jax.tree.map(
        lambda part, zero: jnp.full_like(part, 0) + jnp.asarray(zero, part.dtype), value, neutral
    )

    def turn(position, running):
        longer = join(running, jax.tree.map(lambda part: part[position], pieces))
        return jax.tree.map(lambda new, old: jnp.where(position < mine, new, old), longer, running)

    return lax.fori_loop(0, count - 1, turn, running)


def rotate(values, positions):
    half_dim = values.shape[-1] // 2
    inv_freq = 1.0 / rope_base ** jnp.linspace(0.0, 1.0, half_dim, dtype=jnp.float32)
    angles = positions.astype(jnp.float32)[:, None] * inv_freq[None, :]
    cosine = jnp.cos(angles)[:, None, :]
    sine = jnp.sin(angles)[:, None, :]
    first_half = values[..., :half_dim]
    second_half = values[..., half_dim:]
    return jnp.concatenate(
        [first_half * cosine - second_half * sine, first_half * sine + second_half * cosine],
        axis=-1,
    )


def trailing_sums(extended, length):
    begin = extended.shape[0] - length
    running = extended[begin:]
    results = []
    for behind in range(1, 16):
        running = running + extended[begin - behind : begin - behind + length]
        if behind + 1 in window_list:
            results.append(running)
    return results


def reshape_blocks(array):
    return array.reshape((array.shape[0] // BLOCK, BLOCK) + array.shape[1:])


def block_retention(queries, keys_in, values_in, decay_rate, initial):
    length, head_count, head_dim = queries.shape
    within = jnp.arange(BLOCK, dtype=jnp.float32)
    distance = within[:, None] - within[None, :]
    decay_mask = jnp.where(
        distance[None] >= 0,
        jnp.exp(-jnp.maximum(distance, 0.0)[None] * decay_rate[:, None, None]),
        0.0,
    )
    query_decay_factor = jnp.exp(-(within + 1.0)[:, None] * decay_rate[None, :])
    key_decay_factor = jnp.exp(-(BLOCK - 1.0 - within)[:, None] * decay_rate[None, :])
    block_decay_factor = jnp.exp(-BLOCK * decay_rate)

    def advance(state_carry, inputs):
        block_queries, block_keys, block_values = inputs
        scores = (
            jnp.einsum("ihk,jhk->hij", block_queries, block_keys, precision=highest_precision)
            * decay_mask
        )
        inside = jnp.einsum("hij,jhv->ihv", scores, block_values, precision=highest_precision)
        across_blocks = jnp.einsum(
            "bzy,zyx->bzx",
            block_queries * query_decay_factor[:, :, None],
            state_carry,
            precision=highest_precision,
        )
        state_carry = state_carry * block_decay_factor[:, None, None] + jnp.einsum(
            "flm,fld->lmd",
            block_keys * key_decay_factor[:, :, None],
            block_values,
            precision=highest_precision,
        )
        return (state_carry, inside + across_blocks)

    final_state, outputs = lax.scan(
        advance,
        initial,
        (reshape_blocks(queries), reshape_blocks(keys_in), reshape_blocks(values_in)),
    )
    return (outputs.reshape(length, head_count, values_in.shape[-1]), final_state)


def combine_states(earlier, latter):
    return (earlier[0] * latter[0], latter[0][:, None, None] * earlier[1] + latter[1])


def on_device(
    tokens,
    norm_gain,
    pool_proj,
    query_proj,
    key_proj,
    value_proj,
    pool_map,
    pool_scale,
    decay_rate,
    start_state,
    pool_back,
    retention_back,
):
    sequence = tokens[0]
    length = sequence.shape[0]
    tp_index = lax.axis_index("tp")
    sp_index = lax.axis_index("sp")
    tp_count = lax.axis_size("tp")
    floats = sequence.astype(jnp.float32)
    normed = (
        floats * lax.rsqrt(jnp.mean(floats * floats, axis=-1, keepdims=True) + eps) * norm_gain
    ).astype(jnp.bfloat16)
    group_normed = lax.all_gather(normed, "fs", axis=0, tiled=True)
    quarters = (
        lax.all_to_all(pool_proj, "fs", split_axis=1, concat_axis=0, tiled=True),
        lax.all_to_all(query_proj, "fs", split_axis=1, concat_axis=0, tiled=True),
        lax.all_to_all(key_proj, "fs", split_axis=1, concat_axis=0, tiled=True),
        lax.all_to_all(value_proj, "fs", split_axis=1, concat_axis=0, tiled=True),
    )
    pieces = (
        lax.all_gather(quarters[0], "sp", axis=0, tiled=True),
        lax.all_gather(quarters[1], "sp", axis=0, tiled=True),
        lax.all_gather(quarters[2], "sp", axis=0, tiled=True),
        lax.all_gather(quarters[3], "sp", axis=0, tiled=True),
    )
    partial_cols = tuple(
        (jnp.dot(group_normed, piece_w, preferred_element_type=jnp.float32) for piece_w in pieces)
    )
    rounded = tuple((result.astype(jnp.bfloat16) for result in partial_cols))
    pool_in, query_bf, key_bf, value_bf = jax.tree.map(
        lambda part, own: part.astype(own.dtype),
        lax.all_to_all(shortened(rounded), "fs", split_axis=0, concat_axis=1, tiled=True),
        rounded,
    )
    positions = jnp.arange(length, dtype=jnp.int32) + sp_index * length
    before = shifted(pool_in[length - HALO :], "sp", 1)
    extended = jnp.concatenate([before, pool_in], axis=0).astype(jnp.float32)
    stacked = jnp.stack(trailing_sums(extended, length))
    local_groups = GROUPS // tp_count
    channels = pool_in.shape[1]
    group_dim = channels // local_groups
    group_maps = lax.dynamic_slice_in_dim(pool_map, tp_index * local_groups, local_groups, 0)
    scales = lax.dynamic_slice_in_dim(pool_scale, tp_index * channels, channels, 0)
    windows = jnp.array(window_list, dtype=jnp.int32)
    pieces = []
    for group_idx in range(local_groups):
        chosen_group = tp_index * local_groups + group_idx
        lower = group_idx * group_dim
        chosen = lax.dynamic_index_in_dim(stacked, chosen_group, 0, keepdims=False)[
            :, lower : lower + group_dim
        ]
        counts = jnp.minimum(windows[chosen_group], positions + 1).astype(jnp.float32)
        inputs = extended[HALO:, lower : lower + group_dim]
        differ = (chosen / counts[:, None] - inputs).astype(jnp.bfloat16)
        pieces.append(jnp.dot(differ, group_maps[group_idx], preferred_element_type=jnp.float32))
    pool_out = (jnp.concatenate(pieces, axis=1) * scales).astype(jnp.bfloat16)
    head_count = decay_rate.shape[0]
    head_dim = query_bf.shape[1] // head_count
    queries = rotate(query_bf.astype(jnp.float32).reshape(length, head_count, head_dim), positions)
    keys_in = rotate(
        key_bf.astype(jnp.float32).reshape(length, head_count, head_dim), positions
    ) * head_dim ** (-0.5)
    values_in = value_bf.astype(jnp.float32).reshape(length, head_count, head_dim)
    zeros_state = jnp.zeros((head_count, head_dim, head_dim), jnp.float32)
    local_output, local_state = block_retention(
        queries, keys_in, values_in, decay_rate, zeros_state
    )
    span_decay = jnp.exp(-decay_rate * length)
    whole_start = lax.all_gather(start_state, "sp", axis=2, tiled=True)[0]
    span_factor, carried_over = carried_in(
        (span_decay, local_state), "sp", combine_states, (jnp.ones_like(span_decay), zeros_state)
    )
    offset_float = (sp_index * length).astype(jnp.float32)
    carried_over = carried_over + jnp.exp(-decay_rate * offset_float)[:, None, None] * whole_start
    steps_in = jnp.arange(length, dtype=jnp.float32) + 1.0
    query_rows_scaled = queries * jnp.exp(-steps_in[:, None] * decay_rate[None, :])[:, :, None]
    retained_output = local_output + jnp.einsum(
        "lpi,pib->lpb", query_rows_scaled, carried_over, precision=highest_precision
    )
    retained_output = retained_output * lax.rsqrt(
        jnp.mean(retained_output * retained_output, axis=-1, keepdims=True) + eps
    )
    ret_out = retained_output.reshape(length, head_count * head_dim).astype(jnp.bfloat16)
    pool_cols, retention_cols = (
        lax.all_gather(pool_back, ("sp", "fs"), axis=1, tiled=True),
        lax.all_gather(retention_back, ("sp", "fs"), axis=1, tiled=True),
    )
    weight_local = jnp.concatenate([pool_cols, retention_cols], axis=0)
    joined = jnp.concatenate([pool_out, ret_out], axis=1)
    mixed = lax.psum_scatter(
        jnp.dot(joined, weight_local, preferred_element_type=jnp.float32).astype(jnp.bfloat16),
        "tp",
        scatter_dimension=0,
        tiled=True,
    )
    return mixed[None]


MESH = pl.DeviceIdType.MESH
ORDER = (1, 2, 0, 3)
STEPS = (
    (0, 0, 0, 10.0), (0, 0, 1, 10.7), (0, 1, 0, 14.0), (0, 1, 1, 14.7), (0, 0, 2, 15.4), (0, 1, 2, 16.1), (0, 0, 3, 16.8), (0, 1, 3, 17.5),
    (1, 0, 1, 18.2), (1, 1, 1, 18.9), (0, 2, 0, 20.3), (0, 2, 1, 21.0), (0, 2, 2, 21.7), (0, 2, 3, 22.4),
    (1, 2, 1, 23.1), (1, 0, 0, 23.8), (1, 1, 0, 24.5), (1, 2, 0, 25.2),
    (0, 3, 0, 25.9), (0, 3, 1, 26.6), (0, 3, 2, 27.3), (0, 3, 3, 28.0),
    (1, 0, 2, 28.7), (1, 1, 2, 29.4), (1, 2, 2, 30.1), (1, 0, 3, 30.8), (1, 1, 3, 31.5), (1, 2, 3, 32.2),
    (1, 3, 0, 32.9), (1, 3, 1, 33.6), (1, 3, 2, 34.3), (1, 3, 3, 35.0),
)
HOP = 2.7
NEAR = ((1, 2, 3), (0, 2, 3), (3, 1, 0), (2, 1, 0))


def places(when, needs):
    result = []
    for hop in range(4):
        due = [n for n, step in enumerate(STEPS) if step[3] + HOP * hop >= when] + [len(STEPS)]
        used = [n for n, step in enumerate(STEPS) if needs(hop, *step[:3])] + [len(STEPS)]
        result.append(min(due[0], used[0]))
    return tuple(result)


def where_am_i():
    sp, fs, tp = (lax.axis_index(name) for name in ("sp", "fs", "tp"))
    return sp, fs // 2, fs % 2, tp


def at(z, y, x, p):
    return (z, 2 * y + x, p)


def remote(src, dst, send, recv, target):
    return pltpu.make_async_remote_copy(
        src_ref=src, dst_ref=dst, send_sem=send, recv_sem=recv, device_id=target, device_id_type=MESH
    )


def piece(index, size):
    return pl.ds(pl.multiple_of(index * size, size), size)


def fused_kernel(
    tok, gain, wp, wq, wk, wv, state, pb, rb, pmap, pscale, rate, cos_t, sin_t,
    out,
    xt, xn, xg, wg, obuf, rbuf, backs, gv, st, stb, start, cosv, sinv, mapv, scv,
    krot, pool, mask, yb, yg, keep, give, take, done,
    l_sem, wl_sem, bl_sem, wy_send, wx_send, wf_send, w_recv,
    xz_send, xy_send, xp_send, x_recv,
    s_send, s_recv, b_send, b_recv, r_send, r_recv,
    h_send, c_send, y_recv, g_send, g_recv, o_send, o_recv,
):
    f32, bf = jnp.float32, jnp.bfloat16
    z, y, x, p = where_am_i()
    nz = 4
    half, width = xt.shape
    span = 2 * half
    feats = width // nz
    rows = wp.shape[0]
    group = wp.shape[1] // 2
    steps = 4 * nz
    mats = (wk, wq, wv, wp)
    fs = 2 * y + x
    me = at(z, y, x, p)
    partner = at(z, y, x, 1 - p)
    ypeer = at(z, 1 - y, x, p)
    xpeer = at(z, y, 1 - x, p)
    head = 2 * p + y

    barrier = pltpu.get_barrier_semaphore()
    others = [partner, xpeer]
    for dz in range(nz):
        for dy in range(2):
            if dz or dy:
                others.append(at((z + dz) % nz, (y + dy) % 2, x, p))
    for other in others:
        pl.semaphore_signal(barrier, inc=1, device_id=other, device_id_type=MESH)

    loads = [
        pltpu.make_async_copy(tok.at[piece(p, half)], xt, l_sem.at[0]),
        pltpu.make_async_copy(gain, gv, l_sem.at[1]),
        pltpu.make_async_copy(state, st, l_sem.at[2]),
        pltpu.make_async_copy(cos_t, cosv, l_sem.at[3]),
        pltpu.make_async_copy(sin_t, sinv, l_sem.at[4]),
        pltpu.make_async_copy(pmap.at[head], mapv, l_sem.at[5]),
        pltpu.make_async_copy(pscale.at[head], scv, l_sem.at[6]),
    ]
    for c in loads:
        c.start()
    own_w = []
    for m in range(4):
        c = pltpu.make_async_copy(mats[m].at[:, piece(y, group)], wg.at[m, piece(fs, rows)], wl_sem.at[m])
        c.start()
        own_w.append(c)
    def slot(ref, s, c, h):
        return ref.at[s, pl.ds(pl.multiple_of(c * span + h * half, half), half)]

    pl.semaphore_wait(barrier, len(others))

    sent = []

    def go(c):
        c.start()
        sent.append(c)

    def w_y(m):
        go(remote(mats[m].at[:, piece(1 - y, group)], wg.at[m, piece(fs, rows)], wy_send.at[m], w_recv.at[m, fs], ypeer))

    def w_copy_x(m):
        return remote(mats[m].at[:, piece(y, group)], wg.at[m, piece(fs, rows)], wx_send.at[m], w_recv.at[m, fs], xpeer)

    def w_x(m):
        go(w_copy_x(m))

    def w_wait(m, f):
        view = wg.at[m, piece(f, rows)]
        remote(view, view, wf_send.at[m], w_recv.at[m, f], partner).wait_recv()

    fy = 2 * (1 - y) + x

    def w_relay(m):
        w_wait(m, fy)
        view = wg.at[m, piece(fy, rows)]
        return remote(view, view, wf_send.at[m], w_recv.at[m, fy], xpeer)

    hi = z // 2
    zz = z * (1 - hi) + (3 - z) * hi
    near = [o * (1 - hi) + (3 - o) * hi for o in (1 - zz, 2, 3)]
    hop = (nz - 1 - z) * (1 - p) + z * p
    toward = at(z - 1 + 2 * p, y, x, p)
    onward = at(z + 1 - 2 * p, y, x, p)
    goal = (nz - 1) * p

    w_y(0)
    w_x(0)
    loads[0].wait()
    loads[1].wait()
    block = 16
    for i in range(half // block):
        floats = xt[i * block : (i + 1) * block, :].astype(f32)
        xn[i * block : (i + 1) * block, :] = (
            floats * lax.rsqrt(jnp.mean(floats * floats, axis=-1, keepdims=True) + eps) * gv[...]
        ).astype(bf)

    for i, c in enumerate(near):
        go(remote(xn.at[:, piece(c, feats)], slot(xg, y, z, p), xz_send.at[i], x_recv.at[y, z, p], at(c, y, x, p)))
    xg[y, pl.ds(pl.multiple_of(z * span + p * half, half), half), :] = xn[:, piece(z, feats)]

    def x_wait(s, c, h):
        view = slot(xg, s, c, h)
        remote(view, view, xp_send.at[0], x_recv.at[s, c, h], partner).wait_recv()

    def x_to_y(i, c):
        view = slot(xg, y, c, p)
        go(remote(view, view, xy_send.at[i], x_recv.at[y, c, p], ypeer))

    def x_to_partner(i, s, c):
        view = slot(xg, s, c, p)
        return remote(view, view, xp_send.at[i], x_recv.at[s, c, p], partner)

    w_y(1)
    w_x(1)
    go(remote(xn.at[:, piece(z, feats)], slot(xg, y, z, p), xp_send.at[3], x_recv.at[y, z, p], partner))
    go(remote(xn.at[:, piece(z, feats)], slot(xg, y, z, p), xy_send.at[3], x_recv.at[y, z, p], ypeer))
    w_y(2)

    loads[2].wait()
    for j in range(2):
        stb[j] = st[j].astype(bf)
    rs = st.shape[1]
    for j in range(2):
        same = (z == goal) & (y == j)
        dst = start.at[y, piece(z, rs)]

        @pl.when(same)
        def _():
            pltpu.make_async_copy(stb.at[j], dst, s_recv.at[y, z]).start()

        @pl.when(jnp.logical_not(same))
        def _():
            remote(stb.at[j], dst, s_send.at[j], s_recv.at[y, z], at(goal, j, x, p)).start()

    r = rate[y]
    row = lax.broadcasted_iota(jnp.int32, (span, span), 0)
    col = lax.broadcasted_iota(jnp.int32, (span, span), 1)
    gap = row - col
    for k in range(nz):
        dist = (gap + k * span).astype(f32)
        value = jnp.exp(-jnp.maximum(dist, 0.0) * r)
        mask[k] = jnp.where(dist >= 0.0, value, 0.0) if k == 0 else value
    for c in loads[3:]:
        c.wait()

    x_wait(y, near[0], p)
    x_to_y(0, near[0])
    go(x_to_partner(0, y, near[0]))
    go(w_relay(0))
    w_y(3)
    go(w_relay(1))
    w_x(2)
    own_b = []
    for b, back in enumerate((pb, rb)):
        c = pltpu.make_async_copy(back, backs.at[b, :, piece(fs, rows)], bl_sem.at[b])
        c.start()
        own_b.append(c)
    fx = 2 * y + 1 - x
    fd = 2 * (1 - y) + 1 - x

    def b_own(b, i):
        back = (pb, rb)[b]
        target = ((xpeer, ypeer), (ypeer, xpeer))[b][i]
        return remote(back, backs.at[b, :, piece(fs, rows)], b_send.at[b, i], b_recv.at[b, fs], target)

    def b_wait(b, f):
        view = backs.at[b, :, piece(f, rows)]
        remote(view, view, b_send.at[b, 2], b_recv.at[b, f], partner).wait_recv()

    def b_relay(b):
        f, second = ((fx, ypeer), (fy, xpeer))[b]
        view = backs.at[b, :, piece(f, rows)]
        return remote(view, view, b_send.at[b, 2], b_recv.at[b, f], second)

    def by_place(values):
        result = values[3]
        for h in (2, 1, 0):
            result = jnp.where(hop == h, values[h], result)
        return result

    def listed(table, n):
        words = []
        for part in (table[:16], table[16:]):
            word = sum(v << (2 * i) for i, v in enumerate(part))
            words.append(np.int32(word - 2**32 if word >= 2**31 else word))
        return lax.shift_right_logical(jnp.where(n < 16, words[0], words[1]), 2 * (n % 16)) & 3

    def step(n):
        e, m, i = (listed([entry[k] for entry in STEPS], n) for k in range(3))
        s = y + e * (1 - 2 * y)
        c = (nz - 1 - i) * (1 - p) + i * p
        at_slot = m * nz + c

        @pl.when(m == 0)
        def _():
            x_wait(s, c, 1 - p)

        acc = jnp.dot(xg[s, piece(c, span), :], wg[m], preferred_element_type=f32)
        send, recv = r_send.at[e, at_slot], r_recv.at[e, at_slot]

        @pl.when(hop == 0)
        def _():
            obuf[e, at_slot] = acc.astype(bf)

        @pl.when(hop > 0)
        def _():
            remote(rbuf.at[e, at_slot], rbuf.at[e, at_slot], send, recv, partner).wait_recv()
            obuf[e, at_slot] = (acc + rbuf[e, at_slot].astype(f32)).astype(bf)

        @pl.when(hop < nz - 1)
        def _():
            remote(obuf.at[e, at_slot], rbuf.at[e, at_slot], send, recv, toward).start()

    def w_ready(m):
        own_w[m].wait()
        w_wait(m, fx)
        w_wait(m, fd)

    def event(n, when, act):
        @pl.when(n == by_place(when))
        def _():
            act()

    def a_next(i):
        x_wait(y, near[i], p)
        view = slot(xg, y, near[i], p)
        remote(view, view, xy_send.at[i], x_recv.at[y, near[i], p], ypeer).start()
        x_to_partner(i, y, near[i]).start()

    def b_next(i, c):
        x_wait(1 - y, c, p)
        x_to_partner(4 + i, 1 - y, c).start()

    def relay2():
        w_relay(2).start()
        w_copy_x(3).start()

    def back_own():
        for i in range(2):
            for b in range(2):
                b_own(b, i).start()

    def back_relay():
        for b in range(2):
            b_wait(b, (fx, fy)[b])
            b_relay(b).start()

    def chain(b, q, c):
        view = yg.at[b, q, c]
        return remote(view, view, c_send.at[b, q, c], y_recv.at[b, q, c], onward)

    small = group // 2

    def turned(values, c):
        cosine, sine = cosv[c * span : (c + 1) * span, :], sinv[c * span : (c + 1) * span, :]
        a, b = values[:, :small], values[:, small:]
        return a * cosine - b * sine, a * sine + b * cosine

    def hand_on(e, b, c, value):
        if e == 0:
            yg[b, y, c] = value
            chain(b, y, c).start()
        else:
            yb[b, c] = value
            remote(yb.at[b, c], yg.at[b, y, c], h_send.at[b, c], y_recv.at[b, y, c], ypeer).start()

    place = lax.broadcasted_iota(jnp.int32, (span, 1), 0)

    def retain(e):
        s = y if e == 0 else 1 - y
        for k in range(nz):
            view = start.at[s, piece(k, rs)]
            remote(view, view, s_send.at[0], s_recv.at[s, k], partner).wait_recv()
        scale = group ** (-0.5)
        for c in range(nz):
            first, second = turned(obuf[e, c].astype(f32), c)
            krot[c * span : (c + 1) * span, :small] = (first * scale).astype(bf)
            krot[c * span : (c + 1) * span, small:] = (second * scale).astype(bf)
        for c in ORDER:
            rq = jnp.concatenate(turned(obuf[e, nz + c].astype(f32), c), axis=-1)
            fade = jnp.exp(-((place + c * span).astype(f32) + 1.0) * r)
            acc = jnp.dot((rq * fade).astype(bf), start[s], preferred_element_type=f32)
            rq = rq.astype(bf)
            for g in range(c + 1):
                scores = lax.dot_general(
                    rq, krot[g * span : (g + 1) * span, :], (((1,), (1,)), ((), ())), preferred_element_type=f32
                )
                scores = (scores * mask[c - g]).astype(bf)
                acc += jnp.dot(scores, obuf[e, 2 * nz + g], preferred_element_type=f32)
            hand_on(e, 1, c, (acc * lax.rsqrt(jnp.mean(acc * acc, axis=-1, keepdims=True) + eps)).astype(bf))

    def gather_windows(e):
        pool[0:HALO, :] = jnp.zeros((HALO, group), bf)
        for c in range(nz):
            pool[HALO + c * span : HALO + (c + 1) * span, :] = obuf[e, 3 * nz + c]
        window = 2 * (1 + y) * (1 + 3 * p)
        behind = (
            lax.broadcasted_iota(jnp.int32, (span, span + HALO), 0) + HALO
            - lax.broadcasted_iota(jnp.int32, (span, span + HALO), 1)
        )
        band = jnp.where((behind >= 0) & (behind < window), 1.0, 0.0).astype(bf)
        for c in ORDER:
            trail = jnp.dot(band, pool[c * span : (c + 1) * span + HALO, :], preferred_element_type=f32)
            counts = jnp.minimum(window, place + c * span + 1).astype(f32)
            differ = (trail / counts - obuf[e, 3 * nz + c].astype(f32)).astype(bf)
            pooled = (jnp.dot(differ, mapv[...], preferred_element_type=f32) * scv[...]).astype(bf)
            hand_on(e, 0, c, pooled)

    def early_heads():
        @pl.when(hop == nz - 1)
        def _():
            retain(0)
            gather_windows(0)

    def late_heads():
        @pl.when(hop == nz - 1)
        def _():
            retain(1)

    done_late = 1 + max(n for n, entry in enumerate(STEPS) if entry[0] == 1 and entry[1] < 3)
    done_early = 1 + max(n for n, entry in enumerate(STEPS) if entry[0] == 0)
    events = (
        (places(0.0, lambda h, e, m, i: m == 0), lambda: w_ready(0)),
        (places(10.5, lambda h, e, m, i: e == 1 and i == h), lambda: b_next(3, z)),
        (places(12.5, lambda h, e, m, i: e == 0 and i == NEAR[h][1]), lambda: a_next(1)),
        (places(13.2, lambda h, e, m, i: e == 0 and i == NEAR[h][2]), lambda: a_next(2)),
        (places(13.3, lambda h, e, m, i: m == 2), relay2),
        (places(13.5, lambda h, e, m, i: m == 1), lambda: w_ready(1)),
        (places(16.4, lambda h, e, m, i: e == 1 and i == NEAR[h][0]), lambda: b_next(0, near[0])),
        (places(18.5, lambda h, e, m, i: m == 3), lambda: w_relay(3).start()),
        (places(20.0, lambda h, e, m, i: m == 2), lambda: w_ready(2)),
        (places(22.0, lambda h, e, m, i: e == 1 and i == NEAR[h][1]), lambda: b_next(1, near[1])),
        (places(24.8, lambda h, e, m, i: e == 1 and i == NEAR[h][2]), lambda: b_next(2, near[2])),
        (places(25.2, lambda h, e, m, i: False), back_own),
        (places(25.5, lambda h, e, m, i: m == 3), lambda: w_ready(3)),
        ((done_early,) * 4, early_heads),
        ((done_late,) * 4, late_heads),
        (places(36.5, lambda h, e, m, i: False), back_relay),
    )

    def body(n, carry):
        for when, act in events:
            event(n, when, act)
        step(n)
        return carry

    lax.fori_loop(0, 2 * steps, body, 0)
    event(2 * steps, *events[-1])

    @pl.when(hop == nz - 1)
    def _():
        gather_windows(1)

    far = nz - 1 - hop

    def arrive(b, q, c):
        view = yg.at[b, q, c]
        remote(view, view, c_send.at[b, q, c], y_recv.at[b, q, c], partner).wait_recv()

    def pass_on(b, q, c):
        arrive(b, q, c)

        @pl.when(far < nz - 1)
        def _():
            chain(b, q, c).start()

    across = backs.shape[2]

    def product(q, c):
        acc = jnp.zeros((span, across), f32)
        for b in range(2):
            acc += jnp.dot(yg[b, q, c], backs[b, piece(q, group), :], preferred_element_type=f32)
        return acc

    def early(c):
        @pl.when(far > 0)
        def _():
            for b in (1, 0):
                pass_on(b, y, c)

    def give_copy(c):
        return remote(give.at[c], take.at[c], g_send.at[c], g_recv.at[c], partner)

    def multiply(c):
        keep[c] = keep[c] + product(1 - y, c)
        give[c] = keep[c, piece(1 - p, half), :].astype(bf)
        give_copy(c).start()

    def finish(c):
        give_copy(c).wait_recv()
        done[c] = (keep[c, piece(p, half), :] + take[c].astype(f32)).astype(bf)
        dst = out.at[:, piece(z, across)]

        @pl.when(z == c)
        def _():
            pltpu.make_async_copy(done.at[c], dst, o_recv.at[z]).start()

        @pl.when(z != c)
        def _():
            remote(done.at[c], dst, o_send.at[c], o_recv.at[z], at(c, y, x, p)).start()

    for c in ORDER:
        early(c)
    for b in range(2):
        own_b[b].wait()
        b_wait(b, (fy, fx)[b])
        b_wait(b, fd)
    for c in ORDER:
        keep[c] = product(y, c)
    for i, c in enumerate(ORDER):
        for b in (1, 0):
            pass_on(b, 1 - y, c)
        multiply(c)

        @pl.when(far >= 2)
        def _():
            finish(c)

    @pl.when(far < 2)
    def _():
        for c in ORDER:
            finish(c)

    for k in range(nz):
        view = out.at[:, k * across : (k + 1) * across]
        remote(done.at[k], view, o_send.at[k], o_recv.at[k], partner).wait_recv()

        @pl.when(z != k)
        def _():
            remote(done.at[k], view, o_send.at[k], o_recv.at[k], partner).wait_send()

    @pl.when(hop > 0)
    def _():
        for b in range(2):
            for q in range(2):
                for c in range(nz):
                    chain(b, q, c).wait_send()

    @pl.when(hop == nz - 1)
    def _():
        for b in range(2):
            for c in range(nz):
                remote(yb.at[b, c], yb.at[b, c], h_send.at[b, c], y_recv.at[b, 0, c], partner).wait_send()

    @pl.when(hop < nz - 1)
    def _():
        for e in range(2):

            def drain(j, carry):
                remote(obuf.at[e, j], rbuf.at[e, j], r_send.at[e, j], r_recv.at[e, j], partner).wait_send()
                return carry

            lax.fori_loop(0, steps, drain, 0)

    for j in range(2):

        @pl.when(jnp.logical_not((z == goal) & (y == j)))
        def _():
            remote(stb.at[j], stb.at[j], s_send.at[j], s_recv.at[0, 0], partner).wait_send()

    for c in range(nz):
        give_copy(c).wait_send()
    for m in (2, 3):
        view = wg.at[m, piece(fy, rows)]
        remote(view, view, wf_send.at[m], w_recv.at[m, fy], partner).wait_send()
    for b in range(2):
        for i in range(2):
            b_own(b, i).wait_send()
        b_relay(b).wait_send()
    w_copy_x(3).wait_send()
    for i in (1, 2, 4, 5, 6, 7):
        view = slot(xg, y, z, p)
        remote(view, view, xp_send.at[i], x_recv.at[y, z, p], partner).wait_send()
    view = slot(xg, y, z, p)
    for i in (1, 2):
        remote(view, view, xy_send.at[i], x_recv.at[y, z, p], partner).wait_send()
    for c in sent:
        c.wait_send()


def rotary_tables(length, half_dim):
    inv_freq = np.float32(1.0) / np.power(
        np.float32(rope_base), np.linspace(0.0, 1.0, half_dim, dtype=np.float32)
    )
    angles = np.arange(length, dtype=np.float32)[:, None] * inv_freq[None, :].astype(np.float32)
    return np.cos(angles).astype(np.float32), np.sin(angles).astype(np.float32)


def paired(
    tokens, norm_gain, pool_proj, query_proj, key_proj, value_proj, pool_map, pool_scale,
    decay_rate, start_state, pool_back, retention_back,
):
    bf, f32 = jnp.bfloat16, jnp.float32
    nsp = lax.axis_size("sp")
    tok = tokens[0]
    span, width = tok.shape
    rows, two = pool_proj.shape
    group = two // 2
    length = nsp * span
    half = span // 2
    rs = start_state.shape[2]
    steps = 4 * nsp
    across = 4 * pool_back.shape[1]
    vm, hbm = pl.BlockSpec(memory_space=pltpu.VMEM), pl.BlockSpec(memory_space=pl.ANY)
    dma = pltpu.SemaphoreType.DMA
    cosine, sine = rotary_tables(length, group // 2)
    return pl.pallas_call(
        fused_kernel,
        out_shape=jax.ShapeDtypeStruct((half, width), bf),
        in_specs=[hbm] * 11 + [pl.BlockSpec(memory_space=pltpu.SMEM)] + [hbm] * 2,
        out_specs=vm,
        scratch_shapes=[
            pltpu.VMEM((half, width), bf),
            pltpu.VMEM((half, width), bf),
            pltpu.VMEM((2, length, width // nsp), bf),
            pltpu.VMEM((4, 4 * rows, group), bf),
            pltpu.VMEM((2, steps, span, group), bf),
            pltpu.VMEM((2, steps, span, group), bf),
            pltpu.VMEM((2, pool_back.shape[0], across), bf),
            pltpu.VMEM((1, width), f32),
            pltpu.VMEM((2, rs, group), f32),
            pltpu.VMEM((2, rs, group), bf),
            pltpu.VMEM((2, nsp * rs, group), bf),
            pltpu.VMEM((length, group // 2), f32),
            pltpu.VMEM((length, group // 2), f32),
            pltpu.VMEM((group, group), bf),
            pltpu.VMEM((1, group), f32),
            pltpu.VMEM((length, group), bf),
            pltpu.VMEM((HALO + length, group), bf),
            pltpu.VMEM((nsp, span, span), f32),
            pltpu.VMEM((2, nsp, span, group), bf),
            pltpu.VMEM((2, 2, nsp, span, group), bf),
            pltpu.VMEM((nsp, span, across), f32),
            pltpu.VMEM((nsp, half, across), bf),
            pltpu.VMEM((nsp, half, across), bf),
            pltpu.VMEM((nsp, half, across), bf),
            dma((7,)), dma((4,)), dma((2,)), dma((4,)), dma((4,)), dma((4,)), dma((4, 4)),
            dma((3,)), dma((4,)), dma((8,)), dma((2, nsp, 2)),
            dma((2,)), dma((2, nsp)), dma((2, 3)), dma((2, 4)), dma((2, steps)), dma((2, steps)),
            dma((2, nsp)), dma((2, 2, nsp)), dma((2, 2, nsp)), dma((nsp,)), dma((nsp,)), dma((nsp,)), dma((nsp,)),
        ],
        compiler_params=pltpu.CompilerParams(collective_id=0, has_side_effects=True, vmem_limit_bytes=60 * 2**20),
        name="fused",
    )(
        tok, norm_gain[None, :], pool_proj, query_proj, key_proj, value_proj,
        start_state[0], pool_back, retention_back, pool_map,
        pool_scale.reshape(pool_map.shape[0], 1, group), decay_rate, jnp.asarray(cosine), jnp.asarray(sine),
    )[None]


def solution(mesh):
    sizes = mesh.shape
    small = sizes["sp"] == 4 and sizes["fs"] == 4 and sizes["tp"] == 2
    placed = (
        P("fs", "sp", None),
        P(),
        P(("sp", "fs"), "tp"),
        P(("sp", "fs"), "tp"),
        P(("sp", "fs"), "tp"),
        P(("sp", "fs"), "tp"),
        P(),
        P(),
        P("tp"),
        P("fs", "tp", "sp", None),
        P("tp", ("sp", "fs")),
        P("tp", ("sp", "fs")),
    )
    return jax.shard_map(
        paired if small else on_device,
        mesh=mesh,
        in_specs=placed,
        out_specs=P("fs", ("sp", "tp"), None),
        check_vma=False,
    )
```

```python
import numpy as np
from jax.experimental import pallas as pl
from jax.experimental.pallas import tpu as pltpu

import jax
import jax.numpy as jnp
from jax import lax
from jax.sharding import PartitionSpec as P

GROUPS = 4
BLOCK = 128
HALO = 16


eps = 1e-06
rope_base = 10000.0
highest_precision = lax.Precision.HIGHEST
window_list = (2, 4, 8, 16)


def shortened(x):
    return jax.tree.map(lambda a: a.astype(jnp.bfloat16) if a.dtype == jnp.float32 else a, x)


def shifted(x, axis, by):
    devices = lax.axis_size(axis)
    pairs = [(i, i + by) for i in range(devices) if 0 <= i + by < devices]
    return lax.ppermute(x, axis, pairs)


def carried_in(value, axis, join, neutral):
    count, mine = (lax.axis_size(axis), lax.axis_index(axis))
    pieces = jax.tree.map(lambda part: lax.all_gather(part, axis), value)
    running = jax.tree.map(
        lambda part, zero: jnp.full_like(part, 0) + jnp.asarray(zero, part.dtype), value, neutral
    )

    def turn(position, running):
        longer = join(running, jax.tree.map(lambda part: part[position], pieces))
        return jax.tree.map(lambda new, old: jnp.where(position < mine, new, old), longer, running)

    return lax.fori_loop(0, count - 1, turn, running)


def rotate(values, positions):
    half_dim = values.shape[-1] // 2
    inv_freq = 1.0 / rope_base ** jnp.linspace(0.0, 1.0, half_dim, dtype=jnp.float32)
    angles = positions.astype(jnp.float32)[:, None] * inv_freq[None, :]
    cosine = jnp.cos(angles)[:, None, :]
    sine = jnp.sin(angles)[:, None, :]
    first_half = values[..., :half_dim]
    second_half = values[..., half_dim:]
    return jnp.concatenate(
        [first_half * cosine - second_half * sine, first_half * sine + second_half * cosine],
        axis=-1,
    )


def trailing_sums(extended, length):
    begin = extended.shape[0] - length
    running = extended[begin:]
    results = []
    for behind in range(1, 16):
        running = running + extended[begin - behind : begin - behind + length]
        if behind + 1 in window_list:
            results.append(running)
    return results


def reshape_blocks(array):
    return array.reshape((array.shape[0] // BLOCK, BLOCK) + array.shape[1:])


def block_retention(queries, keys_in, values_in, decay_rate, initial):
    length, head_count, head_dim = queries.shape
    within = jnp.arange(BLOCK, dtype=jnp.float32)
    distance = within[:, None] - within[None, :]
    decay_mask = jnp.where(
        distance[None] >= 0,
        jnp.exp(-jnp.maximum(distance, 0.0)[None] * decay_rate[:, None, None]),
        0.0,
    )
    query_decay_factor = jnp.exp(-(within + 1.0)[:, None] * decay_rate[None, :])
    key_decay_factor = jnp.exp(-(BLOCK - 1.0 - within)[:, None] * decay_rate[None, :])
    block_decay_factor = jnp.exp(-BLOCK * decay_rate)

    def advance(state_carry, inputs):
        block_queries, block_keys, block_values = inputs
        scores = (
            jnp.einsum("ihk,jhk->hij", block_queries, block_keys, precision=highest_precision)
            * decay_mask
        )
        inside = jnp.einsum("hij,jhv->ihv", scores, block_values, precision=highest_precision)
        across_blocks = jnp.einsum(
            "bzy,zyx->bzx",
            block_queries * query_decay_factor[:, :, None],
            state_carry,
            precision=highest_precision,
        )
        state_carry = state_carry * block_decay_factor[:, None, None] + jnp.einsum(
            "flm,fld->lmd",
            block_keys * key_decay_factor[:, :, None],
            block_values,
            precision=highest_precision,
        )
        return (state_carry, inside + across_blocks)

    final_state, outputs = lax.scan(
        advance,
        initial,
        (reshape_blocks(queries), reshape_blocks(keys_in), reshape_blocks(values_in)),
    )
    return (outputs.reshape(length, head_count, values_in.shape[-1]), final_state)


def combine_states(earlier, latter):
    return (earlier[0] * latter[0], latter[0][:, None, None] * earlier[1] + latter[1])


def on_device(
    tokens,
    norm_gain,
    pool_proj,
    query_proj,
    key_proj,
    value_proj,
    pool_map,
    pool_scale,
    decay_rate,
    start_state,
    pool_back,
    retention_back,
):
    sequence = tokens[0]
    length = sequence.shape[0]
    tp_index = lax.axis_index("tp")
    sp_index = lax.axis_index("sp")
    tp_count = lax.axis_size("tp")
    floats = sequence.astype(jnp.float32)
    normed = (
        floats * lax.rsqrt(jnp.mean(floats * floats, axis=-1, keepdims=True) + eps) * norm_gain
    ).astype(jnp.bfloat16)
    group_normed = lax.all_gather(normed, "fs", axis=0, tiled=True)
    quarters = (
        lax.all_to_all(pool_proj, "fs", split_axis=1, concat_axis=0, tiled=True),
        lax.all_to_all(query_proj, "fs", split_axis=1, concat_axis=0, tiled=True),
        lax.all_to_all(key_proj, "fs", split_axis=1, concat_axis=0, tiled=True),
        lax.all_to_all(value_proj, "fs", split_axis=1, concat_axis=0, tiled=True),
    )
    pieces = (
        lax.all_gather(quarters[0], "sp", axis=0, tiled=True),
        lax.all_gather(quarters[1], "sp", axis=0, tiled=True),
        lax.all_gather(quarters[2], "sp", axis=0, tiled=True),
        lax.all_gather(quarters[3], "sp", axis=0, tiled=True),
    )
    partial_cols = tuple(
        (jnp.dot(group_normed, piece_w, preferred_element_type=jnp.float32) for piece_w in pieces)
    )
    rounded = tuple((result.astype(jnp.bfloat16) for result in partial_cols))
    pool_in, query_bf, key_bf, value_bf = jax.tree.map(
        lambda part, own: part.astype(own.dtype),
        lax.all_to_all(shortened(rounded), "fs", split_axis=0, concat_axis=1, tiled=True),
        rounded,
    )
    positions = jnp.arange(length, dtype=jnp.int32) + sp_index * length
    before = shifted(pool_in[length - HALO :], "sp", 1)
    extended = jnp.concatenate([before, pool_in], axis=0).astype(jnp.float32)
    stacked = jnp.stack(trailing_sums(extended, length))
    local_groups = GROUPS // tp_count
    channels = pool_in.shape[1]
    group_dim = channels // local_groups
    group_maps = lax.dynamic_slice_in_dim(pool_map, tp_index * local_groups, local_groups, 0)
    scales = lax.dynamic_slice_in_dim(pool_scale, tp_index * channels, channels, 0)
    windows = jnp.array(window_list, dtype=jnp.int32)
    pieces = []
    for group_idx in range(local_groups):
        chosen_group = tp_index * local_groups + group_idx
        lower = group_idx * group_dim
        chosen = lax.dynamic_index_in_dim(stacked, chosen_group, 0, keepdims=False)[
            :, lower : lower + group_dim
        ]
        counts = jnp.minimum(windows[chosen_group], positions + 1).astype(jnp.float32)
        inputs = extended[HALO:, lower : lower + group_dim]
        differ = (chosen / counts[:, None] - inputs).astype(jnp.bfloat16)
        pieces.append(jnp.dot(differ, group_maps[group_idx], preferred_element_type=jnp.float32))
    pool_out = (jnp.concatenate(pieces, axis=1) * scales).astype(jnp.bfloat16)
    head_count = decay_rate.shape[0]
    head_dim = query_bf.shape[1] // head_count
    queries = rotate(query_bf.astype(jnp.float32).reshape(length, head_count, head_dim), positions)
    keys_in = rotate(
        key_bf.astype(jnp.float32).reshape(length, head_count, head_dim), positions
    ) * head_dim ** (-0.5)
    values_in = value_bf.astype(jnp.float32).reshape(length, head_count, head_dim)
    zeros_state = jnp.zeros((head_count, head_dim, head_dim), jnp.float32)
    local_output, local_state = block_retention(
        queries, keys_in, values_in, decay_rate, zeros_state
    )
    span_decay = jnp.exp(-decay_rate * length)
    whole_start = lax.all_gather(start_state, "sp", axis=2, tiled=True)[0]
    span_factor, carried_over = carried_in(
        (span_decay, local_state), "sp", combine_states, (jnp.ones_like(span_decay), zeros_state)
    )
    offset_float = (sp_index * length).astype(jnp.float32)
    carried_over = carried_over + jnp.exp(-decay_rate * offset_float)[:, None, None] * whole_start
    steps_in = jnp.arange(length, dtype=jnp.float32) + 1.0
    query_rows_scaled = queries * jnp.exp(-steps_in[:, None] * decay_rate[None, :])[:, :, None]
    retained_output = local_output + jnp.einsum(
        "lpi,pib->lpb", query_rows_scaled, carried_over, precision=highest_precision
    )
    retained_output = retained_output * lax.rsqrt(
        jnp.mean(retained_output * retained_output, axis=-1, keepdims=True) + eps
    )
    ret_out = retained_output.reshape(length, head_count * head_dim).astype(jnp.bfloat16)
    pool_cols, retention_cols = (
        lax.all_gather(pool_back, ("sp", "fs"), axis=1, tiled=True),
        lax.all_gather(retention_back, ("sp", "fs"), axis=1, tiled=True),
    )
    weight_local = jnp.concatenate([pool_cols, retention_cols], axis=0)
    joined = jnp.concatenate([pool_out, ret_out], axis=1)
    mixed = lax.psum_scatter(
        jnp.dot(joined, weight_local, preferred_element_type=jnp.float32).astype(jnp.bfloat16),
        "tp",
        scatter_dimension=0,
        tiled=True,
    )
    return mixed[None]


MESH = pl.DeviceIdType.MESH
ORDER = (1, 2, 0, 3)
STEPS = (
    (0, 0, 0, 10.0), (0, 0, 1, 10.7), (0, 1, 0, 14.0), (0, 1, 1, 14.7), (0, 0, 2, 15.4), (0, 1, 2, 16.1), (0, 0, 3, 16.8), (0, 1, 3, 17.5),
    (1, 0, 1, 18.2), (1, 1, 1, 18.9), (0, 2, 0, 20.3), (0, 2, 1, 21.0), (0, 2, 2, 21.7), (0, 2, 3, 22.4),
    (1, 2, 1, 23.1), (1, 0, 0, 23.8), (1, 1, 0, 24.5), (1, 2, 0, 25.2),
    (0, 3, 0, 25.9), (0, 3, 1, 26.6), (0, 3, 2, 27.3), (0, 3, 3, 28.0),
    (1, 0, 2, 28.7), (1, 1, 2, 29.4), (1, 2, 2, 30.1), (1, 0, 3, 30.8), (1, 1, 3, 31.5), (1, 2, 3, 32.2),
    (1, 3, 0, 32.9), (1, 3, 1, 33.6), (1, 3, 2, 34.3), (1, 3, 3, 35.0),
)
HOP = 2.7
NEAR = ((1, 2, 3), (0, 2, 3), (3, 1, 0), (2, 1, 0))


def places(when, needs):
    result = []
    for hop in range(4):
        due = [n for n, step in enumerate(STEPS) if step[3] + HOP * hop >= when] + [len(STEPS)]
        used = [n for n, step in enumerate(STEPS) if needs(hop, *step[:3])] + [len(STEPS)]
        result.append(min(due[0], used[0]))
    return tuple(result)


def where_am_i():
    sp, fs, tp = (lax.axis_index(name) for name in ("sp", "fs", "tp"))
    return sp, fs // 2, fs % 2, tp


def at(z, y, x, p):
    return (z, 2 * y + x, p)


def remote(src, dst, send, recv, target):
    return pltpu.make_async_remote_copy(
        src_ref=src, dst_ref=dst, send_sem=send, recv_sem=recv, device_id=target, device_id_type=MESH
    )


def piece(index, size):
    return pl.ds(pl.multiple_of(index * size, size), size)


def fused_kernel(
    tok, gain, wp, wq, wk, wv, state, pb, rb, pmap, pscale, rate, cos_t, sin_t,
    out,
    xt, xn, xg, wg, obuf, rbuf, backs, gv, st, stb, start, cosv, sinv, mapv, scv,
    krot, pool, mask, yb, yg, keep, give, take, done,
    l_sem, wl_sem, bl_sem, wy_send, wx_send, wf_send, w_recv,
    xz_send, xy_send, xp_send, x_recv,
    s_send, s_recv, b_send, b_recv, r_send, r_recv,
    h_send, c_send, y_recv, g_send, g_recv, o_send, o_recv,
):
    f32, bf = jnp.float32, jnp.bfloat16
    z, y, x, p = where_am_i()
    nz = 4
    half, width = xt.shape
    span = 2 * half
    feats = width // nz
    rows = wp.shape[0]
    group = wp.shape[1] // 2
    steps = 4 * nz
    mats = (wk, wq, wv, wp)
    fs = 2 * y + x
    me = at(z, y, x, p)
    partner = at(z, y, x, 1 - p)
    ypeer = at(z, 1 - y, x, p)
    xpeer = at(z, y, 1 - x, p)
    head = 2 * p + y

    barrier = pltpu.get_barrier_semaphore()
    others = [partner, xpeer]
    for dz in range(nz):
        for dy in range(2):
            if dz or dy:
                others.append(at((z + dz) % nz, (y + dy) % 2, x, p))
    for other in others:
        pl.semaphore_signal(barrier, inc=1, device_id=other, device_id_type=MESH)

    loads = [
        pltpu.make_async_copy(tok.at[piece(p, half)], xt, l_sem.at[0]),
        pltpu.make_async_copy(gain, gv, l_sem.at[1]),
        pltpu.make_async_copy(state, st, l_sem.at[2]),
        pltpu.make_async_copy(cos_t, cosv, l_sem.at[3]),
        pltpu.make_async_copy(sin_t, sinv, l_sem.at[4]),
        pltpu.make_async_copy(pmap.at[head], mapv, l_sem.at[5]),
        pltpu.make_async_copy(pscale.at[head], scv, l_sem.at[6]),
    ]
    for c in loads:
        c.start()
    own_w = []
    for m in range(4):
        c = pltpu.make_async_copy(mats[m].at[:, piece(y, group)], wg.at[m, piece(fs, rows)], wl_sem.at[m])
        c.start()
        own_w.append(c)
    def slot(ref, s, c, h):
        return ref.at[s, pl.ds(pl.multiple_of(c * span + h * half, half), half)]

    pl.semaphore_wait(barrier, len(others))

    sent = []

    def go(c):
        c.start()
        sent.append(c)

    def w_y(m):
        go(remote(mats[m].at[:, piece(1 - y, group)], wg.at[m, piece(fs, rows)], wy_send.at[m], w_recv.at[m, fs], ypeer))

    def w_copy_x(m):
        return remote(mats[m].at[:, piece(y, group)], wg.at[m, piece(fs, rows)], wx_send.at[m], w_recv.at[m, fs], xpeer)

    def w_x(m):
        go(w_copy_x(m))

    def w_wait(m, f):
        view = wg.at[m, piece(f, rows)]
        remote(view, view, wf_send.at[m], w_recv.at[m, f], partner).wait_recv()

    fy = 2 * (1 - y) + x

    def w_relay(m):
        w_wait(m, fy)
        view = wg.at[m, piece(fy, rows)]
        return remote(view, view, wf_send.at[m], w_recv.at[m, fy], xpeer)

    hi = z // 2
    zz = z * (1 - hi) + (3 - z) * hi
    near = [o * (1 - hi) + (3 - o) * hi for o in (1 - zz, 2, 3)]
    hop = (nz - 1 - z) * (1 - p) + z * p
    toward = at(z - 1 + 2 * p, y, x, p)
    onward = at(z + 1 - 2 * p, y, x, p)
    goal = (nz - 1) * p

    w_y(0)
    w_x(0)
    loads[0].wait()
    loads[1].wait()
    block = 16
    for i in range(half // block):
        floats = xt[i * block : (i + 1) * block, :].astype(f32)
        xn[i * block : (i + 1) * block, :] = (
            floats * lax.rsqrt(jnp.mean(floats * floats, axis=-1, keepdims=True) + eps) * gv[...]
        ).astype(bf)

    for i, c in enumerate(near):
        go(remote(xn.at[:, piece(c, feats)], slot(xg, y, z, p), xz_send.at[i], x_recv.at[y, z, p], at(c, y, x, p)))
    xg[y, pl.ds(pl.multiple_of(z * span + p * half, half), half), :] = xn[:, piece(z, feats)]

    def x_wait(s, c, h):
        view = slot(xg, s, c, h)
        remote(view, view, xp_send.at[0], x_recv.at[s, c, h], partner).wait_recv()

    def x_to_y(i, c):
        view = slot(xg, y, c, p)
        go(remote(view, view, xy_send.at[i], x_recv.at[y, c, p], ypeer))

    def x_to_partner(i, s, c):
        view = slot(xg, s, c, p)
        return remote(view, view, xp_send.at[i], x_recv.at[s, c, p], partner)

    w_y(1)
    w_x(1)
    go(remote(xn.at[:, piece(z, feats)], slot(xg, y, z, p), xp_send.at[3], x_recv.at[y, z, p], partner))
    go(remote(xn.at[:, piece(z, feats)], slot(xg, y, z, p), xy_send.at[3], x_recv.at[y, z, p], ypeer))
    w_y(2)

    loads[2].wait()
    for j in range(2):
        stb[j] = st[j].astype(bf)
    rs = st.shape[1]
    for j in range(2):
        same = (z == goal) & (y == j)
        dst = start.at[y, piece(z, rs)]

        @pl.when(same)
        def _():
            pltpu.make_async_copy(stb.at[j], dst, s_recv.at[y, z]).start()

        @pl.when(jnp.logical_not(same))
        def _():
            remote(stb.at[j], dst, s_send.at[j], s_recv.at[y, z], at(goal, j, x, p)).start()

    r = rate[y]
    row = lax.broadcasted_iota(jnp.int32, (span, span), 0)
    col = lax.broadcasted_iota(jnp.int32, (span, span), 1)
    gap = row - col
    for k in range(nz):
        dist = (gap + k * span).astype(f32)
        value = jnp.exp(-jnp.maximum(dist, 0.0) * r)
        mask[k] = jnp.where(dist >= 0.0, value, 0.0) if k == 0 else value
    for c in loads[3:]:
        c.wait()

    x_wait(y, near[0], p)
    x_to_y(0, near[0])
    go(x_to_partner(0, y, near[0]))
    go(w_relay(0))
    w_y(3)
    go(w_relay(1))
    w_x(2)
    own_b = []
    for b, back in enumerate((pb, rb)):
        c = pltpu.make_async_copy(back, backs.at[b, :, piece(fs, rows)], bl_sem.at[b])
        c.start()
        own_b.append(c)
    fx = 2 * y + 1 - x
    fd = 2 * (1 - y) + 1 - x

    def b_own(b, i):
        back = (pb, rb)[b]
        target = ((xpeer, ypeer), (ypeer, xpeer))[b][i]
        return remote(back, backs.at[b, :, piece(fs, rows)], b_send.at[b, i], b_recv.at[b, fs], target)

    def b_wait(b, f):
        view = backs.at[b, :, piece(f, rows)]
        remote(view, view, b_send.at[b, 2], b_recv.at[b, f], partner).wait_recv()

    def b_relay(b):
        f, second = ((fx, ypeer), (fy, xpeer))[b]
        view = backs.at[b, :, piece(f, rows)]
        return remote(view, view, b_send.at[b, 2], b_recv.at[b, f], second)

    def by_place(values):
        result = values[3]
        for h in (2, 1, 0):
            result = jnp.where(hop == h, values[h], result)
        return result

    def listed(table, n):
        words = []
        for part in (table[:16], table[16:]):
            word = sum(v << (2 * i) for i, v in enumerate(part))
            words.append(np.int32(word - 2**32 if word >= 2**31 else word))
        return lax.shift_right_logical(jnp.where(n < 16, words[0], words[1]), 2 * (n % 16)) & 3

    def step(n):
        e, m, i = (listed([entry[k] for entry in STEPS], n) for k in range(3))
        s = y + e * (1 - 2 * y)
        c = (nz - 1 - i) * (1 - p) + i * p
        at_slot = m * nz + c

        @pl.when(m == 0)
        def _():
            x_wait(s, c, 1 - p)

        acc = jnp.dot(xg[s, piece(c, span), :], wg[m], preferred_element_type=f32)
        send, recv = r_send.at[e, at_slot], r_recv.at[e, at_slot]

        @pl.when(hop == 0)
        def _():
            obuf[e, at_slot] = acc.astype(bf)

        @pl.when(hop > 0)
        def _():
            remote(rbuf.at[e, at_slot], rbuf.at[e, at_slot], send, recv, partner).wait_recv()
            obuf[e, at_slot] = (acc + rbuf[e, at_slot].astype(f32)).astype(bf)

        @pl.when(hop < nz - 1)
        def _():
            remote(obuf.at[e, at_slot], rbuf.at[e, at_slot], send, recv, toward).start()

    def w_ready(m):
        own_w[m].wait()
        w_wait(m, fx)
        w_wait(m, fd)

    def event(n, when, act):
        @pl.when(n == by_place(when))
        def _():
            act()

    def a_next(i):
        x_wait(y, near[i], p)
        view = slot(xg, y, near[i], p)
        remote(view, view, xy_send.at[i], x_recv.at[y, near[i], p], ypeer).start()
        x_to_partner(i, y, near[i]).start()

    def b_next(i, c):
        x_wait(1 - y, c, p)
        x_to_partner(4 + i, 1 - y, c).start()

    def relay2():
        w_relay(2).start()
        w_copy_x(3).start()

    def back_own():
        for i in range(2):
            for b in range(2):
                b_own(b, i).start()

    def back_relay():
        for b in range(2):
            b_wait(b, (fx, fy)[b])
            b_relay(b).start()

    def chain(b, q, c):
        view = yg.at[b, q, c]
        return remote(view, view, c_send.at[b, q, c], y_recv.at[b, q, c], onward)

    small = group // 2

    def turned(values, c):
        cosine, sine = cosv[c * span : (c + 1) * span, :], sinv[c * span : (c + 1) * span, :]
        a, b = values[:, :small], values[:, small:]
        return a * cosine - b * sine, a * sine + b * cosine

    def hand_on(e, b, c, value):
        if e == 0:
            yg[b, y, c] = value
            chain(b, y, c).start()
        else:
            yb[b, c] = value
            remote(yb.at[b, c], yg.at[b, y, c], h_send.at[b, c], y_recv.at[b, y, c], ypeer).start()

    place = lax.broadcasted_iota(jnp.int32, (span, 1), 0)

    def turn_keys(e):
        s = y if e == 0 else 1 - y
        for k in range(nz):
            view = start.at[s, piece(k, rs)]
            remote(view, view, s_send.at[0], s_recv.at[s, k], partner).wait_recv()
        scale = group ** (-0.5)
        for c in range(nz):
            first, second = turned(obuf[e, c].astype(f32), c)
            krot[c * span : (c + 1) * span, :small] = (first * scale).astype(bf)
            krot[c * span : (c + 1) * span, small:] = (second * scale).astype(bf)

    def heads(e):
        s = y if e == 0 else 1 - y
        pool[0:HALO, :] = jnp.zeros((HALO, group), bf)
        for c in range(nz):
            pool[HALO + c * span : HALO + (c + 1) * span, :] = obuf[e, 3 * nz + c]
        window = 2 * (1 + y) * (1 + 3 * p)
        behind = (
            lax.broadcasted_iota(jnp.int32, (span, span + HALO), 0) + HALO
            - lax.broadcasted_iota(jnp.int32, (span, span + HALO), 1)
        )
        band = jnp.where((behind >= 0) & (behind < window), 1.0, 0.0).astype(bf)
        for c in ORDER:
            rq = jnp.concatenate(turned(obuf[e, nz + c].astype(f32), c), axis=-1)
            fade = jnp.exp(-((place + c * span).astype(f32) + 1.0) * r)
            acc = jnp.dot((rq * fade).astype(bf), start[s], preferred_element_type=f32)
            rq = rq.astype(bf)
            for g in range(c + 1):
                scores = lax.dot_general(
                    rq, krot[g * span : (g + 1) * span, :], (((1,), (1,)), ((), ())), preferred_element_type=f32
                )
                scores = (scores * mask[c - g]).astype(bf)
                acc += jnp.dot(scores, obuf[e, 2 * nz + g], preferred_element_type=f32)
            hand_on(e, 1, c, (acc * lax.rsqrt(jnp.mean(acc * acc, axis=-1, keepdims=True) + eps)).astype(bf))
            trail = jnp.dot(band, pool[c * span : (c + 1) * span + HALO, :], preferred_element_type=f32)
            counts = jnp.minimum(window, place + c * span + 1).astype(f32)
            differ = (trail / counts - obuf[e, 3 * nz + c].astype(f32)).astype(bf)
            pooled = (jnp.dot(differ, mapv[...], preferred_element_type=f32) * scv[...]).astype(bf)
            hand_on(e, 0, c, pooled)

    def early_heads():
        @pl.when(hop == nz - 1)
        def _():
            turn_keys(0)
            heads(0)

    def late_heads():
        @pl.when(hop == nz - 1)
        def _():
            turn_keys(1)

    done_late = 1 + max(n for n, entry in enumerate(STEPS) if entry[0] == 1 and entry[1] < 3)
    done_early = 1 + max(n for n, entry in enumerate(STEPS) if entry[0] == 0)
    events = (
        (places(0.0, lambda h, e, m, i: m == 0), lambda: w_ready(0)),
        (places(10.5, lambda h, e, m, i: e == 1 and i == h), lambda: b_next(3, z)),
        (places(12.5, lambda h, e, m, i: e == 0 and i == NEAR[h][1]), lambda: a_next(1)),
        (places(13.2, lambda h, e, m, i: e == 0 and i == NEAR[h][2]), lambda: a_next(2)),
        (places(13.3, lambda h, e, m, i: m == 2), relay2),
        (places(13.5, lambda h, e, m, i: m == 1), lambda: w_ready(1)),
        (places(16.4, lambda h, e, m, i: e == 1 and i == NEAR[h][0]), lambda: b_next(0, near[0])),
        (places(18.5, lambda h, e, m, i: m == 3), lambda: w_relay(3).start()),
        (places(20.0, lambda h, e, m, i: m == 2), lambda: w_ready(2)),
        (places(22.0, lambda h, e, m, i: e == 1 and i == NEAR[h][1]), lambda: b_next(1, near[1])),
        (places(24.8, lambda h, e, m, i: e == 1 and i == NEAR[h][2]), lambda: b_next(2, near[2])),
        (places(25.2, lambda h, e, m, i: False), back_own),
        (places(25.5, lambda h, e, m, i: m == 3), lambda: w_ready(3)),
        ((done_early,) * 4, early_heads),
        ((done_late,) * 4, late_heads),
        (places(36.5, lambda h, e, m, i: False), back_relay),
    )

    def body(n, carry):
        for when, act in events:
            event(n, when, act)
        step(n)
        return carry

    lax.fori_loop(0, 2 * steps, body, 0)
    event(2 * steps, *events[-1])

    @pl.when(hop == nz - 1)
    def _():
        heads(1)

    far = nz - 1 - hop

    def arrive(b, q, c):
        view = yg.at[b, q, c]
        remote(view, view, c_send.at[b, q, c], y_recv.at[b, q, c], partner).wait_recv()

    def pass_on(b, q, c):
        arrive(b, q, c)

        @pl.when(far < nz - 1)
        def _():
            chain(b, q, c).start()

    across = backs.shape[2]

    def product(q, c):
        acc = jnp.zeros((span, across), f32)
        for b in range(2):
            acc += jnp.dot(yg[b, q, c], backs[b, piece(q, group), :], preferred_element_type=f32)
        return acc

    def early(c):
        @pl.when(far > 0)
        def _():
            for b in (1, 0):
                pass_on(b, y, c)

    def give_copy(c):
        return remote(give.at[c], take.at[c], g_send.at[c], g_recv.at[c], partner)

    def multiply(c):
        keep[c] = keep[c] + product(1 - y, c)
        give[c] = keep[c, piece(1 - p, half), :].astype(bf)
        give_copy(c).start()

    def finish(c):
        give_copy(c).wait_recv()
        done[c] = (keep[c, piece(p, half), :] + take[c].astype(f32)).astype(bf)
        dst = out.at[:, piece(z, across)]

        @pl.when(z == c)
        def _():
            pltpu.make_async_copy(done.at[c], dst, o_recv.at[z]).start()

        @pl.when(z != c)
        def _():
            remote(done.at[c], dst, o_send.at[c], o_recv.at[z], at(c, y, x, p)).start()

    for c in ORDER:
        early(c)
    for b in range(2):
        own_b[b].wait()
        b_wait(b, (fy, fx)[b])
        b_wait(b, fd)
    for c in ORDER:
        keep[c] = product(y, c)
    for i, c in enumerate(ORDER):
        for b in (1, 0):
            pass_on(b, 1 - y, c)
        multiply(c)

        @pl.when(far >= 2)
        def _():
            finish(c)

    @pl.when(far < 2)
    def _():
        for c in ORDER:
            finish(c)

    for k in range(nz):
        view = out.at[:, k * across : (k + 1) * across]
        remote(done.at[k], view, o_send.at[k], o_recv.at[k], partner).wait_recv()

        @pl.when(z != k)
        def _():
            remote(done.at[k], view, o_send.at[k], o_recv.at[k], partner).wait_send()

    @pl.when(hop > 0)
    def _():
        for b in range(2):
            for q in range(2):
                for c in range(nz):
                    chain(b, q, c).wait_send()

    @pl.when(hop == nz - 1)
    def _():
        for b in range(2):
            for c in range(nz):
                remote(yb.at[b, c], yb.at[b, c], h_send.at[b, c], y_recv.at[b, 0, c], partner).wait_send()

    @pl.when(hop < nz - 1)
    def _():
        for e in range(2):

            def drain(j, carry):
                remote(obuf.at[e, j], rbuf.at[e, j], r_send.at[e, j], r_recv.at[e, j], partner).wait_send()
                return carry

            lax.fori_loop(0, steps, drain, 0)

    for j in range(2):

        @pl.when(jnp.logical_not((z == goal) & (y == j)))
        def _():
            remote(stb.at[j], stb.at[j], s_send.at[j], s_recv.at[0, 0], partner).wait_send()

    for c in range(nz):
        give_copy(c).wait_send()
    for m in (2, 3):
        view = wg.at[m, piece(fy, rows)]
        remote(view, view, wf_send.at[m], w_recv.at[m, fy], partner).wait_send()
    for b in range(2):
        for i in range(2):
            b_own(b, i).wait_send()
        b_relay(b).wait_send()
    w_copy_x(3).wait_send()
    for i in (1, 2, 4, 5, 6, 7):
        view = slot(xg, y, z, p)
        remote(view, view, xp_send.at[i], x_recv.at[y, z, p], partner).wait_send()
    view = slot(xg, y, z, p)
    for i in (1, 2):
        remote(view, view, xy_send.at[i], x_recv.at[y, z, p], partner).wait_send()
    for c in sent:
        c.wait_send()


def rotary_tables(length, half_dim):
    inv_freq = np.float32(1.0) / np.power(
        np.float32(rope_base), np.linspace(0.0, 1.0, half_dim, dtype=np.float32)
    )
    angles = np.arange(length, dtype=np.float32)[:, None] * inv_freq[None, :].astype(np.float32)
    return np.cos(angles).astype(np.float32), np.sin(angles).astype(np.float32)


def paired(
    tokens, norm_gain, pool_proj, query_proj, key_proj, value_proj, pool_map, pool_scale,
    decay_rate, start_state, pool_back, retention_back,
):
    bf, f32 = jnp.bfloat16, jnp.float32
    nsp = lax.axis_size("sp")
    tok = tokens[0]
    span, width = tok.shape
    rows, two = pool_proj.shape
    group = two // 2
    length = nsp * span
    half = span // 2
    rs = start_state.shape[2]
    steps = 4 * nsp
    across = 4 * pool_back.shape[1]
    vm, hbm = pl.BlockSpec(memory_space=pltpu.VMEM), pl.BlockSpec(memory_space=pl.ANY)
    dma = pltpu.SemaphoreType.DMA
    cosine, sine = rotary_tables(length, group // 2)
    return pl.pallas_call(
        fused_kernel,
        out_shape=jax.ShapeDtypeStruct((half, width), bf),
        in_specs=[hbm] * 11 + [pl.BlockSpec(memory_space=pltpu.SMEM)] + [hbm] * 2,
        out_specs=vm,
        scratch_shapes=[
            pltpu.VMEM((half, width), bf),
            pltpu.VMEM((half, width), bf),
            pltpu.VMEM((2, length, width // nsp), bf),
            pltpu.VMEM((4, 4 * rows, group), bf),
            pltpu.VMEM((2, steps, span, group), bf),
            pltpu.VMEM((2, steps, span, group), bf),
            pltpu.VMEM((2, pool_back.shape[0], across), bf),
            pltpu.VMEM((1, width), f32),
            pltpu.VMEM((2, rs, group), f32),
            pltpu.VMEM((2, rs, group), bf),
            pltpu.VMEM((2, nsp * rs, group), bf),
            pltpu.VMEM((length, group // 2), f32),
            pltpu.VMEM((length, group // 2), f32),
            pltpu.VMEM((group, group), bf),
            pltpu.VMEM((1, group), f32),
            pltpu.VMEM((length, group), bf),
            pltpu.VMEM((HALO + length, group), bf),
            pltpu.VMEM((nsp, span, span), f32),
            pltpu.VMEM((2, nsp, span, group), bf),
            pltpu.VMEM((2, 2, nsp, span, group), bf),
            pltpu.VMEM((nsp, span, across), f32),
            pltpu.VMEM((nsp, half, across), bf),
            pltpu.VMEM((nsp, half, across), bf),
            pltpu.VMEM((nsp, half, across), bf),
            dma((7,)), dma((4,)), dma((2,)), dma((4,)), dma((4,)), dma((4,)), dma((4, 4)),
            dma((3,)), dma((4,)), dma((8,)), dma((2, nsp, 2)),
            dma((2,)), dma((2, nsp)), dma((2, 3)), dma((2, 4)), dma((2, steps)), dma((2, steps)),
            dma((2, nsp)), dma((2, 2, nsp)), dma((2, 2, nsp)), dma((nsp,)), dma((nsp,)), dma((nsp,)), dma((nsp,)),
        ],
        compiler_params=pltpu.CompilerParams(collective_id=0, has_side_effects=True, vmem_limit_bytes=60 * 2**20),
        name="fused",
    )(
        tok, norm_gain[None, :], pool_proj, query_proj, key_proj, value_proj,
        start_state[0], pool_back, retention_back, pool_map,
        pool_scale.reshape(pool_map.shape[0], 1, group), decay_rate, jnp.asarray(cosine), jnp.asarray(sine),
    )[None]


def solution(mesh):
    sizes = mesh.shape
    small = sizes["sp"] == 4 and sizes["fs"] == 4 and sizes["tp"] == 2
    placed = (
        P("fs", "sp", None),
        P(),
        P(("sp", "fs"), "tp"),
        P(("sp", "fs"), "tp"),
        P(("sp", "fs"), "tp"),
        P(("sp", "fs"), "tp"),
        P(),
        P(),
        P("tp"),
        P("fs", "tp", "sp", None),
        P("tp", ("sp", "fs")),
        P("tp", ("sp", "fs")),
    )
    return jax.shard_map(
        paired if small else on_device,
        mesh=mesh,
        in_specs=placed,
        out_specs=P("fs", ("sp", "tp"), None),
        check_vma=False,
    )
```

```python
import numpy as np
from jax.experimental import pallas as pl
from jax.experimental.pallas import tpu as pltpu

import jax
import jax.numpy as jnp
from jax import lax
from jax.sharding import PartitionSpec as P

GROUPS = 4
BLOCK = 128
HALO = 16


eps = 1e-06
rope_base = 10000.0
highest_precision = lax.Precision.HIGHEST
window_list = (2, 4, 8, 16)


def shortened(x):
    return jax.tree.map(lambda a: a.astype(jnp.bfloat16) if a.dtype == jnp.float32 else a, x)


def shifted(x, axis, by):
    devices = lax.axis_size(axis)
    pairs = [(i, i + by) for i in range(devices) if 0 <= i + by < devices]
    return lax.ppermute(x, axis, pairs)


def carried_in(value, axis, join, neutral):
    count, mine = (lax.axis_size(axis), lax.axis_index(axis))
    pieces = jax.tree.map(lambda part: lax.all_gather(part, axis), value)
    running = jax.tree.map(
        lambda part, zero: jnp.full_like(part, 0) + jnp.asarray(zero, part.dtype), value, neutral
    )

    def turn(position, running):
        longer = join(running, jax.tree.map(lambda part: part[position], pieces))
        return jax.tree.map(lambda new, old: jnp.where(position < mine, new, old), longer, running)

    return lax.fori_loop(0, count - 1, turn, running)


def rotate(values, positions):
    half_dim = values.shape[-1] // 2
    inv_freq = 1.0 / rope_base ** jnp.linspace(0.0, 1.0, half_dim, dtype=jnp.float32)
    angles = positions.astype(jnp.float32)[:, None] * inv_freq[None, :]
    cosine = jnp.cos(angles)[:, None, :]
    sine = jnp.sin(angles)[:, None, :]
    first_half = values[..., :half_dim]
    second_half = values[..., half_dim:]
    return jnp.concatenate(
        [first_half * cosine - second_half * sine, first_half * sine + second_half * cosine],
        axis=-1,
    )


def trailing_sums(extended, length):
    begin = extended.shape[0] - length
    running = extended[begin:]
    results = []
    for behind in range(1, 16):
        running = running + extended[begin - behind : begin - behind + length]
        if behind + 1 in window_list:
            results.append(running)
    return results


def reshape_blocks(array):
    return array.reshape((array.shape[0] // BLOCK, BLOCK) + array.shape[1:])


def block_retention(queries, keys_in, values_in, decay_rate, initial):
    length, head_count, head_dim = queries.shape
    within = jnp.arange(BLOCK, dtype=jnp.float32)
    distance = within[:, None] - within[None, :]
    decay_mask = jnp.where(
        distance[None] >= 0,
        jnp.exp(-jnp.maximum(distance, 0.0)[None] * decay_rate[:, None, None]),
        0.0,
    )
    query_decay_factor = jnp.exp(-(within + 1.0)[:, None] * decay_rate[None, :])
    key_decay_factor = jnp.exp(-(BLOCK - 1.0 - within)[:, None] * decay_rate[None, :])
    block_decay_factor = jnp.exp(-BLOCK * decay_rate)

    def advance(state_carry, inputs):
        block_queries, block_keys, block_values = inputs
        scores = (
            jnp.einsum("ihk,jhk->hij", block_queries, block_keys, precision=highest_precision)
            * decay_mask
        )
        inside = jnp.einsum("hij,jhv->ihv", scores, block_values, precision=highest_precision)
        across_blocks = jnp.einsum(
            "bzy,zyx->bzx",
            block_queries * query_decay_factor[:, :, None],
            state_carry,
            precision=highest_precision,
        )
        state_carry = state_carry * block_decay_factor[:, None, None] + jnp.einsum(
            "flm,fld->lmd",
            block_keys * key_decay_factor[:, :, None],
            block_values,
            precision=highest_precision,
        )
        return (state_carry, inside + across_blocks)

    final_state, outputs = lax.scan(
        advance,
        initial,
        (reshape_blocks(queries), reshape_blocks(keys_in), reshape_blocks(values_in)),
    )
    return (outputs.reshape(length, head_count, values_in.shape[-1]), final_state)


def combine_states(earlier, latter):
    return (earlier[0] * latter[0], latter[0][:, None, None] * earlier[1] + latter[1])


def on_device(
    tokens,
    norm_gain,
    pool_proj,
    query_proj,
    key_proj,
    value_proj,
    pool_map,
    pool_scale,
    decay_rate,
    start_state,
    pool_back,
    retention_back,
):
    sequence = tokens[0]
    length = sequence.shape[0]
    tp_index = lax.axis_index("tp")
    sp_index = lax.axis_index("sp")
    tp_count = lax.axis_size("tp")
    floats = sequence.astype(jnp.float32)
    normed = (
        floats * lax.rsqrt(jnp.mean(floats * floats, axis=-1, keepdims=True) + eps) * norm_gain
    ).astype(jnp.bfloat16)
    group_normed = lax.all_gather(normed, "fs", axis=0, tiled=True)
    quarters = (
        lax.all_to_all(pool_proj, "fs", split_axis=1, concat_axis=0, tiled=True),
        lax.all_to_all(query_proj, "fs", split_axis=1, concat_axis=0, tiled=True),
        lax.all_to_all(key_proj, "fs", split_axis=1, concat_axis=0, tiled=True),
        lax.all_to_all(value_proj, "fs", split_axis=1, concat_axis=0, tiled=True),
    )
    pieces = (
        lax.all_gather(quarters[0], "sp", axis=0, tiled=True),
        lax.all_gather(quarters[1], "sp", axis=0, tiled=True),
        lax.all_gather(quarters[2], "sp", axis=0, tiled=True),
        lax.all_gather(quarters[3], "sp", axis=0, tiled=True),
    )
    partial_cols = tuple(
        (jnp.dot(group_normed, piece_w, preferred_element_type=jnp.float32) for piece_w in pieces)
    )
    rounded = tuple((result.astype(jnp.bfloat16) for result in partial_cols))
    pool_in, query_bf, key_bf, value_bf = jax.tree.map(
        lambda part, own: part.astype(own.dtype),
        lax.all_to_all(shortened(rounded), "fs", split_axis=0, concat_axis=1, tiled=True),
        rounded,
    )
    positions = jnp.arange(length, dtype=jnp.int32) + sp_index * length
    before = shifted(pool_in[length - HALO :], "sp", 1)
    extended = jnp.concatenate([before, pool_in], axis=0).astype(jnp.float32)
    stacked = jnp.stack(trailing_sums(extended, length))
    local_groups = GROUPS // tp_count
    channels = pool_in.shape[1]
    group_dim = channels // local_groups
    group_maps = lax.dynamic_slice_in_dim(pool_map, tp_index * local_groups, local_groups, 0)
    scales = lax.dynamic_slice_in_dim(pool_scale, tp_index * channels, channels, 0)
    windows = jnp.array(window_list, dtype=jnp.int32)
    pieces = []
    for group_idx in range(local_groups):
        chosen_group = tp_index * local_groups + group_idx
        lower = group_idx * group_dim
        chosen = lax.dynamic_index_in_dim(stacked, chosen_group, 0, keepdims=False)[
            :, lower : lower + group_dim
        ]
        counts = jnp.minimum(windows[chosen_group], positions + 1).astype(jnp.float32)
        inputs = extended[HALO:, lower : lower + group_dim]
        differ = (chosen / counts[:, None] - inputs).astype(jnp.bfloat16)
        pieces.append(jnp.dot(differ, group_maps[group_idx], preferred_element_type=jnp.float32))
    pool_out = (jnp.concatenate(pieces, axis=1) * scales).astype(jnp.bfloat16)
    head_count = decay_rate.shape[0]
    head_dim = query_bf.shape[1] // head_count
    queries = rotate(query_bf.astype(jnp.float32).reshape(length, head_count, head_dim), positions)
    keys_in = rotate(
        key_bf.astype(jnp.float32).reshape(length, head_count, head_dim), positions
    ) * head_dim ** (-0.5)
    values_in = value_bf.astype(jnp.float32).reshape(length, head_count, head_dim)
    zeros_state = jnp.zeros((head_count, head_dim, head_dim), jnp.float32)
    local_output, local_state = block_retention(
        queries, keys_in, values_in, decay_rate, zeros_state
    )
    span_decay = jnp.exp(-decay_rate * length)
    whole_start = lax.all_gather(start_state, "sp", axis=2, tiled=True)[0]
    span_factor, carried_over = carried_in(
        (span_decay, local_state), "sp", combine_states, (jnp.ones_like(span_decay), zeros_state)
    )
    offset_float = (sp_index * length).astype(jnp.float32)
    carried_over = carried_over + jnp.exp(-decay_rate * offset_float)[:, None, None] * whole_start
    steps_in = jnp.arange(length, dtype=jnp.float32) + 1.0
    query_rows_scaled = queries * jnp.exp(-steps_in[:, None] * decay_rate[None, :])[:, :, None]
    retained_output = local_output + jnp.einsum(
        "lpi,pib->lpb", query_rows_scaled, carried_over, precision=highest_precision
    )
    retained_output = retained_output * lax.rsqrt(
        jnp.mean(retained_output * retained_output, axis=-1, keepdims=True) + eps
    )
    ret_out = retained_output.reshape(length, head_count * head_dim).astype(jnp.bfloat16)
    pool_cols, retention_cols = (
        lax.all_gather(pool_back, ("sp", "fs"), axis=1, tiled=True),
        lax.all_gather(retention_back, ("sp", "fs"), axis=1, tiled=True),
    )
    weight_local = jnp.concatenate([pool_cols, retention_cols], axis=0)
    joined = jnp.concatenate([pool_out, ret_out], axis=1)
    mixed = lax.psum_scatter(
        jnp.dot(joined, weight_local, preferred_element_type=jnp.float32).astype(jnp.bfloat16),
        "tp",
        scatter_dimension=0,
        tiled=True,
    )
    return mixed[None]


MESH = pl.DeviceIdType.MESH
ORDER = (1, 2, 0, 3)
STEPS = (
    (0, 0, 0, 10.0), (0, 0, 1, 10.7), (0, 1, 0, 14.0), (0, 1, 1, 14.7), (0, 0, 2, 15.4), (0, 1, 2, 16.1), (0, 0, 3, 16.8), (0, 1, 3, 17.5),
    (1, 0, 1, 18.2), (1, 1, 1, 18.9), (0, 2, 0, 20.3), (0, 2, 1, 21.0), (0, 2, 2, 21.7), (0, 2, 3, 22.4),
    (1, 2, 1, 23.1), (1, 0, 0, 23.8), (1, 1, 0, 24.5), (1, 2, 0, 25.2),
    (0, 3, 0, 25.9), (0, 3, 1, 26.6), (0, 3, 2, 27.3), (0, 3, 3, 28.0),
    (1, 0, 2, 28.7), (1, 1, 2, 29.4), (1, 2, 2, 30.1), (1, 0, 3, 30.8), (1, 1, 3, 31.5), (1, 2, 3, 32.2),
    (1, 3, 0, 32.9), (1, 3, 1, 33.6), (1, 3, 2, 34.3), (1, 3, 3, 35.0),
)
HOP = 2.7
NEAR = ((1, 2, 3), (0, 2, 3), (3, 1, 0), (2, 1, 0))


def places(when, needs):
    result = []
    for hop in range(4):
        due = [n for n, step in enumerate(STEPS) if step[3] + HOP * hop >= when] + [len(STEPS)]
        used = [n for n, step in enumerate(STEPS) if needs(hop, *step[:3])] + [len(STEPS)]
        result.append(min(due[0], used[0]))
    return tuple(result)


def where_am_i():
    sp, fs, tp = (lax.axis_index(name) for name in ("sp", "fs", "tp"))
    return sp, fs // 2, fs % 2, tp


def at(z, y, x, p):
    return (z, 2 * y + x, p)


def remote(src, dst, send, recv, target):
    return pltpu.make_async_remote_copy(
        src_ref=src, dst_ref=dst, send_sem=send, recv_sem=recv, device_id=target, device_id_type=MESH
    )


def piece(index, size):
    return pl.ds(pl.multiple_of(index * size, size), size)


def fused_kernel(
    tok, gain, wp, wq, wk, wv, state, pb, rb, pmap, pscale, rate, cos_t, sin_t,
    out,
    xt, xn, xg, wg, obuf, rbuf, backs, gv, st, stb, start, cosv, sinv, mapv, scv,
    krot, pool, mask, yb, yg, keep, give, take, done,
    l_sem, wl_sem, bl_sem, wy_send, wx_send, wf_send, w_recv,
    xz_send, xy_send, xp_send, x_recv,
    s_send, s_recv, b_send, b_recv, r_send, r_recv,
    h_send, c_send, y_recv, g_send, g_recv, o_send, o_recv,
):
    f32, bf = jnp.float32, jnp.bfloat16
    z, y, x, p = where_am_i()
    nz = 4
    half, width = xt.shape
    span = 2 * half
    feats = width // nz
    rows = wp.shape[0]
    group = wp.shape[1] // 2
    steps = 4 * nz
    mats = (wk, wq, wv, wp)
    fs = 2 * y + x
    me = at(z, y, x, p)
    partner = at(z, y, x, 1 - p)
    ypeer = at(z, 1 - y, x, p)
    xpeer = at(z, y, 1 - x, p)
    head = 2 * p + y

    barrier = pltpu.get_barrier_semaphore()
    others = [partner, xpeer]
    for dz in range(nz):
        for dy in range(2):
            if dz or dy:
                others.append(at((z + dz) % nz, (y + dy) % 2, x, p))
    for other in others:
        pl.semaphore_signal(barrier, inc=1, device_id=other, device_id_type=MESH)

    loads = [
        pltpu.make_async_copy(tok.at[piece(p, half)], xt, l_sem.at[0]),
        pltpu.make_async_copy(gain, gv, l_sem.at[1]),
        pltpu.make_async_copy(state, st, l_sem.at[2]),
        pltpu.make_async_copy(cos_t, cosv, l_sem.at[3]),
        pltpu.make_async_copy(sin_t, sinv, l_sem.at[4]),
        pltpu.make_async_copy(pmap.at[head], mapv, l_sem.at[5]),
        pltpu.make_async_copy(pscale.at[head], scv, l_sem.at[6]),
    ]
    for c in loads:
        c.start()
    own_w = []
    for m in range(4):
        c = pltpu.make_async_copy(mats[m].at[:, piece(y, group)], wg.at[m, piece(fs, rows)], wl_sem.at[m])
        c.start()
        own_w.append(c)
    def slot(ref, s, c, h):
        return ref.at[s, pl.ds(pl.multiple_of(c * span + h * half, half), half)]

    pl.semaphore_wait(barrier, len(others))

    sent = []

    def go(c):
        c.start()
        sent.append(c)

    def w_y(m):
        go(remote(mats[m].at[:, piece(1 - y, group)], wg.at[m, piece(fs, rows)], wy_send.at[m], w_recv.at[m, fs], ypeer))

    def w_copy_x(m):
        return remote(mats[m].at[:, piece(y, group)], wg.at[m, piece(fs, rows)], wx_send.at[m], w_recv.at[m, fs], xpeer)

    def w_x(m):
        go(w_copy_x(m))

    def w_wait(m, f):
        view = wg.at[m, piece(f, rows)]
        remote(view, view, wf_send.at[m], w_recv.at[m, f], partner).wait_recv()

    fy = 2 * (1 - y) + x

    def w_relay(m):
        w_wait(m, fy)
        view = wg.at[m, piece(fy, rows)]
        return remote(view, view, wf_send.at[m], w_recv.at[m, fy], xpeer)

    hi = z // 2
    zz = z * (1 - hi) + (3 - z) * hi
    near = [o * (1 - hi) + (3 - o) * hi for o in (1 - zz, 2, 3)]
    hop = (nz - 1 - z) * (1 - p) + z * p
    toward = at(z - 1 + 2 * p, y, x, p)
    onward = at(z + 1 - 2 * p, y, x, p)
    goal = (nz - 1) * p

    w_y(0)
    w_x(0)
    loads[0].wait()
    loads[1].wait()
    block = 16
    for i in range(half // block):
        floats = xt[i * block : (i + 1) * block, :].astype(f32)
        xn[i * block : (i + 1) * block, :] = (
            floats * lax.rsqrt(jnp.mean(floats * floats, axis=-1, keepdims=True) + eps) * gv[...]
        ).astype(bf)

    for i, c in enumerate(near):
        go(remote(xn.at[:, piece(c, feats)], slot(xg, y, z, p), xz_send.at[i], x_recv.at[y, z, p], at(c, y, x, p)))
    xg[y, pl.ds(pl.multiple_of(z * span + p * half, half), half), :] = xn[:, piece(z, feats)]

    def x_wait(s, c, h):
        view = slot(xg, s, c, h)
        remote(view, view, xp_send.at[0], x_recv.at[s, c, h], partner).wait_recv()

    def x_to_y(i, c):
        view = slot(xg, y, c, p)
        go(remote(view, view, xy_send.at[i], x_recv.at[y, c, p], ypeer))

    def x_to_partner(i, s, c):
        view = slot(xg, s, c, p)
        return remote(view, view, xp_send.at[i], x_recv.at[s, c, p], partner)

    w_y(1)
    w_x(1)
    go(remote(xn.at[:, piece(z, feats)], slot(xg, y, z, p), xp_send.at[3], x_recv.at[y, z, p], partner))
    go(remote(xn.at[:, piece(z, feats)], slot(xg, y, z, p), xy_send.at[3], x_recv.at[y, z, p], ypeer))
    w_y(2)

    loads[2].wait()
    for j in range(2):
        stb[j] = st[j].astype(bf)
    rs = st.shape[1]
    for j in range(2):
        same = (z == goal) & (y == j)
        dst = start.at[y, piece(z, rs)]

        @pl.when(same)
        def _():
            pltpu.make_async_copy(stb.at[j], dst, s_recv.at[y, z]).start()

        @pl.when(jnp.logical_not(same))
        def _():
            remote(stb.at[j], dst, s_send.at[j], s_recv.at[y, z], at(goal, j, x, p)).start()

    r = rate[y]
    row = lax.broadcasted_iota(jnp.int32, (span, span), 0)
    col = lax.broadcasted_iota(jnp.int32, (span, span), 1)
    gap = row - col
    for k in range(nz):
        dist = (gap + k * span).astype(f32)
        value = jnp.exp(-jnp.maximum(dist, 0.0) * r)
        mask[k] = jnp.where(dist >= 0.0, value, 0.0) if k == 0 else value
    for c in loads[3:]:
        c.wait()

    x_wait(y, near[0], p)
    x_to_y(0, near[0])
    go(x_to_partner(0, y, near[0]))
    go(w_relay(0))
    w_y(3)
    go(w_relay(1))
    w_x(2)
    own_b = []
    for b, back in enumerate((pb, rb)):
        c = pltpu.make_async_copy(back, backs.at[b, :, piece(fs, rows)], bl_sem.at[b])
        c.start()
        own_b.append(c)
    fx = 2 * y + 1 - x
    fd = 2 * (1 - y) + 1 - x

    def b_own(b, i):
        back = (pb, rb)[b]
        target = ((xpeer, ypeer), (ypeer, xpeer))[b][i]
        return remote(back, backs.at[b, :, piece(fs, rows)], b_send.at[b, i], b_recv.at[b, fs], target)

    def b_wait(b, f):
        view = backs.at[b, :, piece(f, rows)]
        remote(view, view, b_send.at[b, 2], b_recv.at[b, f], partner).wait_recv()

    def b_relay(b):
        f, second = ((fx, ypeer), (fy, xpeer))[b]
        view = backs.at[b, :, piece(f, rows)]
        return remote(view, view, b_send.at[b, 2], b_recv.at[b, f], second)

    def by_place(values):
        result = values[3]
        for h in (2, 1, 0):
            result = jnp.where(hop == h, values[h], result)
        return result

    def listed(table, n):
        words = []
        for part in (table[:16], table[16:]):
            word = sum(v << (2 * i) for i, v in enumerate(part))
            words.append(np.int32(word - 2**32 if word >= 2**31 else word))
        return lax.shift_right_logical(jnp.where(n < 16, words[0], words[1]), 2 * (n % 16)) & 3

    def step(n):
        e, m, i = (listed([entry[k] for entry in STEPS], n) for k in range(3))
        s = y + e * (1 - 2 * y)
        c = (nz - 1 - i) * (1 - p) + i * p
        at_slot = m * nz + c

        @pl.when(m == 0)
        def _():
            x_wait(s, c, 1 - p)

        acc = jnp.dot(xg[s, piece(c, span), :], wg[m], preferred_element_type=f32)
        send, recv = r_send.at[e, at_slot], r_recv.at[e, at_slot]

        @pl.when(hop == 0)
        def _():
            obuf[e, at_slot] = acc.astype(bf)

        @pl.when(hop > 0)
        def _():
            remote(rbuf.at[e, at_slot], rbuf.at[e, at_slot], send, recv, partner).wait_recv()
            obuf[e, at_slot] = (acc + rbuf[e, at_slot].astype(f32)).astype(bf)

        @pl.when(hop < nz - 1)
        def _():
            remote(obuf.at[e, at_slot], rbuf.at[e, at_slot], send, recv, toward).start()

    def w_ready(m):
        own_w[m].wait()
        w_wait(m, fx)
        w_wait(m, fd)

    def event(n, when, act):
        @pl.when(n == by_place(when))
        def _():
            act()

    def a_next(i):
        x_wait(y, near[i], p)
        view = slot(xg, y, near[i], p)
        remote(view, view, xy_send.at[i], x_recv.at[y, near[i], p], ypeer).start()
        x_to_partner(i, y, near[i]).start()

    def b_next(i, c):
        x_wait(1 - y, c, p)
        x_to_partner(4 + i, 1 - y, c).start()

    def relay2():
        w_relay(2).start()
        w_copy_x(3).start()

    def back_own():
        for i in range(2):
            for b in range(2):
                b_own(b, i).start()

    def back_relay():
        for b in range(2):
            b_wait(b, (fx, fy)[b])
            b_relay(b).start()

    def chain(b, q, c):
        view = yg.at[b, q, c]
        return remote(view, view, c_send.at[b, q, c], y_recv.at[b, q, c], onward)

    small = group // 2

    def turned(values, c):
        cosine, sine = cosv[c * span : (c + 1) * span, :], sinv[c * span : (c + 1) * span, :]
        a, b = values[:, :small], values[:, small:]
        return a * cosine - b * sine, a * sine + b * cosine

    def hand_on(e, b, c, value):
        if e == 0:
            yg[b, y, c] = value
            chain(b, y, c).start()
        else:
            yb[b, c] = value
            remote(yb.at[b, c], yg.at[b, y, c], h_send.at[b, c], y_recv.at[b, y, c], ypeer).start()

    place = lax.broadcasted_iota(jnp.int32, (span, 1), 0)

    def turn_keys(e):
        s = y if e == 0 else 1 - y
        for k in range(nz):
            view = start.at[s, piece(k, rs)]
            remote(view, view, s_send.at[0], s_recv.at[s, k], partner).wait_recv()
        scale = group ** (-0.5)
        for c in range(nz):
            first, second = turned(obuf[e, c].astype(f32), c)
            krot[c * span : (c + 1) * span, :small] = (first * scale).astype(bf)
            krot[c * span : (c + 1) * span, small:] = (second * scale).astype(bf)

    def heads(e):
        s = y if e == 0 else 1 - y
        pool[0:HALO, :] = jnp.zeros((HALO, group), bf)
        for c in range(nz):
            pool[HALO + c * span : HALO + (c + 1) * span, :] = obuf[e, 3 * nz + c]
        window = 2 * (1 + y) * (1 + 3 * p)
        behind = (
            lax.broadcasted_iota(jnp.int32, (span, span + HALO), 0) + HALO
            - lax.broadcasted_iota(jnp.int32, (span, span + HALO), 1)
        )
        band = jnp.where((behind >= 0) & (behind < window), 1.0, 0.0).astype(bf)
        for c in ORDER:
            rq = jnp.concatenate(turned(obuf[e, nz + c].astype(f32), c), axis=-1)
            fade = jnp.exp(-((place + c * span).astype(f32) + 1.0) * r)
            acc = jnp.dot((rq * fade).astype(bf), start[s], preferred_element_type=f32)
            rq = rq.astype(bf)
            for g in range(c + 1):
                scores = lax.dot_general(
                    rq, krot[g * span : (g + 1) * span, :], (((1,), (1,)), ((), ())), preferred_element_type=f32
                )
                scores = (scores * mask[c - g]).astype(bf)
                acc += jnp.dot(scores, obuf[e, 2 * nz + g], preferred_element_type=f32)
            ret = (acc * lax.rsqrt(jnp.mean(acc * acc, axis=-1, keepdims=True) + eps)).astype(bf)
            trail = jnp.dot(band, pool[c * span : (c + 1) * span + HALO, :], preferred_element_type=f32)
            counts = jnp.minimum(window, place + c * span + 1).astype(f32)
            differ = (trail / counts - obuf[e, 3 * nz + c].astype(f32)).astype(bf)
            pooled = (jnp.dot(differ, mapv[...], preferred_element_type=f32) * scv[...]).astype(bf)
            hand_on(e, 1, c, ret)
            hand_on(e, 0, c, pooled)

    def early_heads():
        @pl.when(hop == nz - 1)
        def _():
            turn_keys(0)
            heads(0)

    def late_heads():
        @pl.when(hop == nz - 1)
        def _():
            turn_keys(1)

    done_late = 1 + max(n for n, entry in enumerate(STEPS) if entry[0] == 1 and entry[1] < 3)
    done_early = 1 + max(n for n, entry in enumerate(STEPS) if entry[0] == 0)
    events = (
        (places(0.0, lambda h, e, m, i: m == 0), lambda: w_ready(0)),
        (places(10.5, lambda h, e, m, i: e == 1 and i == h), lambda: b_next(3, z)),
        ((4, 1, 0, 0), lambda: a_next(1)),
        ((4, 1, 0, 0), lambda: a_next(2)),
        ((4, 2, 0, 0), relay2),
        (places(13.5, lambda h, e, m, i: m == 1), lambda: w_ready(1)),
        (places(16.4, lambda h, e, m, i: e == 1 and i == NEAR[h][0]), lambda: b_next(0, near[0])),
        (places(18.5, lambda h, e, m, i: m == 3), lambda: w_relay(3).start()),
        (places(20.0, lambda h, e, m, i: m == 2), lambda: w_ready(2)),
        (places(22.0, lambda h, e, m, i: e == 1 and i == NEAR[h][1]), lambda: b_next(1, near[1])),
        (places(24.8, lambda h, e, m, i: e == 1 and i == NEAR[h][2]), lambda: b_next(2, near[2])),
        (places(25.2, lambda h, e, m, i: False), back_own),
        (places(25.5, lambda h, e, m, i: m == 3), lambda: w_ready(3)),
        ((done_early,) * 4, early_heads),
        ((done_late,) * 4, late_heads),
        (places(36.5, lambda h, e, m, i: False), back_relay),
    )

    def body(n, carry):
        for when, act in events:
            event(n, when, act)
        step(n)
        return carry

    lax.fori_loop(0, 2 * steps, body, 0)
    event(2 * steps, *events[-1])

    @pl.when(hop == nz - 1)
    def _():
        heads(1)

    far = nz - 1 - hop

    def arrive(b, q, c):
        view = yg.at[b, q, c]
        remote(view, view, c_send.at[b, q, c], y_recv.at[b, q, c], partner).wait_recv()

    def pass_on(b, q, c):
        arrive(b, q, c)

        @pl.when(far < nz - 1)
        def _():
            chain(b, q, c).start()

    across = backs.shape[2]

    def product(q, c):
        acc = jnp.zeros((span, across), f32)
        for b in range(2):
            acc += jnp.dot(yg[b, q, c], backs[b, piece(q, group), :], preferred_element_type=f32)
        return acc

    def early(c):
        @pl.when(far > 0)
        def _():
            for b in (1, 0):
                pass_on(b, y, c)

    def give_copy(c):
        return remote(give.at[c], take.at[c], g_send.at[c], g_recv.at[c], partner)

    def multiply(c):
        keep[c] = keep[c] + product(1 - y, c)
        give[c] = keep[c, piece(1 - p, half), :].astype(bf)
        give_copy(c).start()

    def finish(c):
        give_copy(c).wait_recv()
        done[c] = (keep[c, piece(p, half), :] + take[c].astype(f32)).astype(bf)
        dst = out.at[:, piece(z, across)]

        @pl.when(z == c)
        def _():
            pltpu.make_async_copy(done.at[c], dst, o_recv.at[z]).start()

        @pl.when(z != c)
        def _():
            remote(done.at[c], dst, o_send.at[c], o_recv.at[z], at(c, y, x, p)).start()

    for c in ORDER:
        early(c)
    for b in range(2):
        own_b[b].wait()
        b_wait(b, (fy, fx)[b])
        b_wait(b, fd)
    for c in ORDER:
        keep[c] = product(y, c)
    for i, c in enumerate(ORDER):
        for b in (1, 0):
            pass_on(b, 1 - y, c)
        multiply(c)

        @pl.when(far >= 2)
        def _():
            finish(c)

    @pl.when(far < 2)
    def _():
        for c in ORDER:
            finish(c)

    for k in range(nz):
        view = out.at[:, k * across : (k + 1) * across]
        remote(done.at[k], view, o_send.at[k], o_recv.at[k], partner).wait_recv()

        @pl.when(z != k)
        def _():
            remote(done.at[k], view, o_send.at[k], o_recv.at[k], partner).wait_send()

    @pl.when(hop > 0)
    def _():
        for b in range(2):
            for q in range(2):
                for c in range(nz):
                    chain(b, q, c).wait_send()

    @pl.when(hop == nz - 1)
    def _():
        for b in range(2):
            for c in range(nz):
                remote(yb.at[b, c], yb.at[b, c], h_send.at[b, c], y_recv.at[b, 0, c], partner).wait_send()

    @pl.when(hop < nz - 1)
    def _():
        for e in range(2):

            def drain(j, carry):
                remote(obuf.at[e, j], rbuf.at[e, j], r_send.at[e, j], r_recv.at[e, j], partner).wait_send()
                return carry

            lax.fori_loop(0, steps, drain, 0)

    for j in range(2):

        @pl.when(jnp.logical_not((z == goal) & (y == j)))
        def _():
            remote(stb.at[j], stb.at[j], s_send.at[j], s_recv.at[0, 0], partner).wait_send()

    for c in range(nz):
        give_copy(c).wait_send()
    for m in (2, 3):
        view = wg.at[m, piece(fy, rows)]
        remote(view, view, wf_send.at[m], w_recv.at[m, fy], partner).wait_send()
    for b in range(2):
        for i in range(2):
            b_own(b, i).wait_send()
        b_relay(b).wait_send()
    w_copy_x(3).wait_send()
    for i in (1, 2, 4, 5, 6, 7):
        view = slot(xg, y, z, p)
        remote(view, view, xp_send.at[i], x_recv.at[y, z, p], partner).wait_send()
    view = slot(xg, y, z, p)
    for i in (1, 2):
        remote(view, view, xy_send.at[i], x_recv.at[y, z, p], partner).wait_send()
    for c in sent:
        c.wait_send()


def rotary_tables(length, half_dim):
    inv_freq = np.float32(1.0) / np.power(
        np.float32(rope_base), np.linspace(0.0, 1.0, half_dim, dtype=np.float32)
    )
    angles = np.arange(length, dtype=np.float32)[:, None] * inv_freq[None, :].astype(np.float32)
    return np.cos(angles).astype(np.float32), np.sin(angles).astype(np.float32)


def paired(
    tokens, norm_gain, pool_proj, query_proj, key_proj, value_proj, pool_map, pool_scale,
    decay_rate, start_state, pool_back, retention_back,
):
    bf, f32 = jnp.bfloat16, jnp.float32
    nsp = lax.axis_size("sp")
    tok = tokens[0]
    span, width = tok.shape
    rows, two = pool_proj.shape
    group = two // 2
    length = nsp * span
    half = span // 2
    rs = start_state.shape[2]
    steps = 4 * nsp
    across = 4 * pool_back.shape[1]
    vm, hbm = pl.BlockSpec(memory_space=pltpu.VMEM), pl.BlockSpec(memory_space=pl.ANY)
    dma = pltpu.SemaphoreType.DMA
    cosine, sine = rotary_tables(length, group // 2)
    return pl.pallas_call(
        fused_kernel,
        out_shape=jax.ShapeDtypeStruct((half, width), bf),
        in_specs=[hbm] * 11 + [pl.BlockSpec(memory_space=pltpu.SMEM)] + [hbm] * 2,
        out_specs=hbm,
        scratch_shapes=[
            pltpu.VMEM((half, width), bf),
            pltpu.VMEM((half, width), bf),
            pltpu.VMEM((2, length, width // nsp), bf),
            pltpu.VMEM((4, 4 * rows, group), bf),
            pltpu.VMEM((2, steps, span, group), bf),
            pltpu.VMEM((2, steps, span, group), bf),
            pltpu.VMEM((2, pool_back.shape[0], across), bf),
            pltpu.VMEM((1, width), f32),
            pltpu.VMEM((2, rs, group), f32),
            pltpu.VMEM((2, rs, group), bf),
            pltpu.VMEM((2, nsp * rs, group), bf),
            pltpu.VMEM((length, group // 2), f32),
            pltpu.VMEM((length, group // 2), f32),
            pltpu.VMEM((group, group), bf),
            pltpu.VMEM((1, group), f32),
            pltpu.VMEM((length, group), bf),
            pltpu.VMEM((HALO + length, group), bf),
            pltpu.VMEM((nsp, span, span), f32),
            pltpu.VMEM((2, nsp, span, group), bf),
            pltpu.VMEM((2, 2, nsp, span, group), bf),
            pltpu.VMEM((nsp, span, across), f32),
            pltpu.VMEM((nsp, half, across), bf),
            pltpu.VMEM((nsp, half, across), bf),
            pltpu.VMEM((nsp, half, across), bf),
            dma((7,)), dma((4,)), dma((2,)), dma((4,)), dma((4,)), dma((4,)), dma((4, 4)),
            dma((3,)), dma((4,)), dma((8,)), dma((2, nsp, 2)),
            dma((2,)), dma((2, nsp)), dma((2, 3)), dma((2, 4)), dma((2, steps)), dma((2, steps)),
            dma((2, nsp)), dma((2, 2, nsp)), dma((2, 2, nsp)), dma((nsp,)), dma((nsp,)), dma((nsp,)), dma((nsp,)),
        ],
        compiler_params=pltpu.CompilerParams(collective_id=0, has_side_effects=True, vmem_limit_bytes=60 * 2**20),
        name="fused",
    )(
        tok, norm_gain[None, :], pool_proj, query_proj, key_proj, value_proj,
        start_state[0], pool_back, retention_back, pool_map,
        pool_scale.reshape(pool_map.shape[0], 1, group), decay_rate, jnp.asarray(cosine), jnp.asarray(sine),
    )[None]


def solution(mesh):
    sizes = mesh.shape
    small = sizes["sp"] == 4 and sizes["fs"] == 4 and sizes["tp"] == 2
    placed = (
        P("fs", "sp", None),
        P(),
        P(("sp", "fs"), "tp"),
        P(("sp", "fs"), "tp"),
        P(("sp", "fs"), "tp"),
        P(("sp", "fs"), "tp"),
        P(),
        P(),
        P("tp"),
        P("fs", "tp", "sp", None),
        P("tp", ("sp", "fs")),
        P("tp", ("sp", "fs")),
    )
    return jax.shard_map(
        paired if small else on_device,
        mesh=mesh,
        in_specs=placed,
        out_specs=P("fs", ("sp", "tp"), None),
        check_vma=False,
    )
```

```python
import numpy as np
from jax.experimental import pallas as pl
from jax.experimental.pallas import tpu as pltpu

import jax
import jax.numpy as jnp
from jax import lax
from jax.sharding import PartitionSpec as P

GROUPS = 4
BLOCK = 128
HALO = 16


eps = 1e-06
rope_base = 10000.0
highest_precision = lax.Precision.HIGHEST
window_list = (2, 4, 8, 16)


def shortened(x):
    return jax.tree.map(lambda a: a.astype(jnp.bfloat16) if a.dtype == jnp.float32 else a, x)


def shifted(x, axis, by):
    devices = lax.axis_size(axis)
    pairs = [(i, i + by) for i in range(devices) if 0 <= i + by < devices]
    return lax.ppermute(x, axis, pairs)


def carried_in(value, axis, join, neutral):
    count, mine = (lax.axis_size(axis), lax.axis_index(axis))
    pieces = jax.tree.map(lambda part: lax.all_gather(part, axis), value)
    running = jax.tree.map(
        lambda part, zero: jnp.full_like(part, 0) + jnp.asarray(zero, part.dtype), value, neutral
    )

    def turn(position, running):
        longer = join(running, jax.tree.map(lambda part: part[position], pieces))
        return jax.tree.map(lambda new, old: jnp.where(position < mine, new, old), longer, running)

    return lax.fori_loop(0, count - 1, turn, running)


def rotate(values, positions):
    half_dim = values.shape[-1] // 2
    inv_freq = 1.0 / rope_base ** jnp.linspace(0.0, 1.0, half_dim, dtype=jnp.float32)
    angles = positions.astype(jnp.float32)[:, None] * inv_freq[None, :]
    cosine = jnp.cos(angles)[:, None, :]
    sine = jnp.sin(angles)[:, None, :]
    first_half = values[..., :half_dim]
    second_half = values[..., half_dim:]
    return jnp.concatenate(
        [first_half * cosine - second_half * sine, first_half * sine + second_half * cosine],
        axis=-1,
    )


def trailing_sums(extended, length):
    begin = extended.shape[0] - length
    running = extended[begin:]
    results = []
    for behind in range(1, 16):
        running = running + extended[begin - behind : begin - behind + length]
        if behind + 1 in window_list:
            results.append(running)
    return results


def reshape_blocks(array):
    return array.reshape((array.shape[0] // BLOCK, BLOCK) + array.shape[1:])


def block_retention(queries, keys_in, values_in, decay_rate, initial):
    length, head_count, head_dim = queries.shape
    within = jnp.arange(BLOCK, dtype=jnp.float32)
    distance = within[:, None] - within[None, :]
    decay_mask = jnp.where(
        distance[None] >= 0,
        jnp.exp(-jnp.maximum(distance, 0.0)[None] * decay_rate[:, None, None]),
        0.0,
    )
    query_decay_factor = jnp.exp(-(within + 1.0)[:, None] * decay_rate[None, :])
    key_decay_factor = jnp.exp(-(BLOCK - 1.0 - within)[:, None] * decay_rate[None, :])
    block_decay_factor = jnp.exp(-BLOCK * decay_rate)

    def advance(state_carry, inputs):
        block_queries, block_keys, block_values = inputs
        scores = (
            jnp.einsum("ihk,jhk->hij", block_queries, block_keys, precision=highest_precision)
            * decay_mask
        )
        inside = jnp.einsum("hij,jhv->ihv", scores, block_values, precision=highest_precision)
        across_blocks = jnp.einsum(
            "bzy,zyx->bzx",
            block_queries * query_decay_factor[:, :, None],
            state_carry,
            precision=highest_precision,
        )
        state_carry = state_carry * block_decay_factor[:, None, None] + jnp.einsum(
            "flm,fld->lmd",
            block_keys * key_decay_factor[:, :, None],
            block_values,
            precision=highest_precision,
        )
        return (state_carry, inside + across_blocks)

    final_state, outputs = lax.scan(
        advance,
        initial,
        (reshape_blocks(queries), reshape_blocks(keys_in), reshape_blocks(values_in)),
    )
    return (outputs.reshape(length, head_count, values_in.shape[-1]), final_state)


def combine_states(earlier, latter):
    return (earlier[0] * latter[0], latter[0][:, None, None] * earlier[1] + latter[1])


def on_device(
    tokens,
    norm_gain,
    pool_proj,
    query_proj,
    key_proj,
    value_proj,
    pool_map,
    pool_scale,
    decay_rate,
    start_state,
    pool_back,
    retention_back,
):
    sequence = tokens[0]
    length = sequence.shape[0]
    tp_index = lax.axis_index("tp")
    sp_index = lax.axis_index("sp")
    tp_count = lax.axis_size("tp")
    floats = sequence.astype(jnp.float32)
    normed = (
        floats * lax.rsqrt(jnp.mean(floats * floats, axis=-1, keepdims=True) + eps) * norm_gain
    ).astype(jnp.bfloat16)
    group_normed = lax.all_gather(normed, "fs", axis=0, tiled=True)
    quarters = (
        lax.all_to_all(pool_proj, "fs", split_axis=1, concat_axis=0, tiled=True),
        lax.all_to_all(query_proj, "fs", split_axis=1, concat_axis=0, tiled=True),
        lax.all_to_all(key_proj, "fs", split_axis=1, concat_axis=0, tiled=True),
        lax.all_to_all(value_proj, "fs", split_axis=1, concat_axis=0, tiled=True),
    )
    pieces = (
        lax.all_gather(quarters[0], "sp", axis=0, tiled=True),
        lax.all_gather(quarters[1], "sp", axis=0, tiled=True),
        lax.all_gather(quarters[2], "sp", axis=0, tiled=True),
        lax.all_gather(quarters[3], "sp", axis=0, tiled=True),
    )
    partial_cols = tuple(
        (jnp.dot(group_normed, piece_w, preferred_element_type=jnp.float32) for piece_w in pieces)
    )
    rounded = tuple((result.astype(jnp.bfloat16) for result in partial_cols))
    pool_in, query_bf, key_bf, value_bf = jax.tree.map(
        lambda part, own: part.astype(own.dtype),
        lax.all_to_all(shortened(rounded), "fs", split_axis=0, concat_axis=1, tiled=True),
        rounded,
    )
    positions = jnp.arange(length, dtype=jnp.int32) + sp_index * length
    before = shifted(pool_in[length - HALO :], "sp", 1)
    extended = jnp.concatenate([before, pool_in], axis=0).astype(jnp.float32)
    stacked = jnp.stack(trailing_sums(extended, length))
    local_groups = GROUPS // tp_count
    channels = pool_in.shape[1]
    group_dim = channels // local_groups
    group_maps = lax.dynamic_slice_in_dim(pool_map, tp_index * local_groups, local_groups, 0)
    scales = lax.dynamic_slice_in_dim(pool_scale, tp_index * channels, channels, 0)
    windows = jnp.array(window_list, dtype=jnp.int32)
    pieces = []
    for group_idx in range(local_groups):
        chosen_group = tp_index * local_groups + group_idx
        lower = group_idx * group_dim
        chosen = lax.dynamic_index_in_dim(stacked, chosen_group, 0, keepdims=False)[
            :, lower : lower + group_dim
        ]
        counts = jnp.minimum(windows[chosen_group], positions + 1).astype(jnp.float32)
        inputs = extended[HALO:, lower : lower + group_dim]
        differ = (chosen / counts[:, None] - inputs).astype(jnp.bfloat16)
        pieces.append(jnp.dot(differ, group_maps[group_idx], preferred_element_type=jnp.float32))
    pool_out = (jnp.concatenate(pieces, axis=1) * scales).astype(jnp.bfloat16)
    head_count = decay_rate.shape[0]
    head_dim = query_bf.shape[1] // head_count
    queries = rotate(query_bf.astype(jnp.float32).reshape(length, head_count, head_dim), positions)
    keys_in = rotate(
        key_bf.astype(jnp.float32).reshape(length, head_count, head_dim), positions
    ) * head_dim ** (-0.5)
    values_in = value_bf.astype(jnp.float32).reshape(length, head_count, head_dim)
    zeros_state = jnp.zeros((head_count, head_dim, head_dim), jnp.float32)
    local_output, local_state = block_retention(
        queries, keys_in, values_in, decay_rate, zeros_state
    )
    span_decay = jnp.exp(-decay_rate * length)
    whole_start = lax.all_gather(start_state, "sp", axis=2, tiled=True)[0]
    span_factor, carried_over = carried_in(
        (span_decay, local_state), "sp", combine_states, (jnp.ones_like(span_decay), zeros_state)
    )
    offset_float = (sp_index * length).astype(jnp.float32)
    carried_over = carried_over + jnp.exp(-decay_rate * offset_float)[:, None, None] * whole_start
    steps_in = jnp.arange(length, dtype=jnp.float32) + 1.0
    query_rows_scaled = queries * jnp.exp(-steps_in[:, None] * decay_rate[None, :])[:, :, None]
    retained_output = local_output + jnp.einsum(
        "lpi,pib->lpb", query_rows_scaled, carried_over, precision=highest_precision
    )
    retained_output = retained_output * lax.rsqrt(
        jnp.mean(retained_output * retained_output, axis=-1, keepdims=True) + eps
    )
    ret_out = retained_output.reshape(length, head_count * head_dim).astype(jnp.bfloat16)
    pool_cols, retention_cols = (
        lax.all_gather(pool_back, ("sp", "fs"), axis=1, tiled=True),
        lax.all_gather(retention_back, ("sp", "fs"), axis=1, tiled=True),
    )
    weight_local = jnp.concatenate([pool_cols, retention_cols], axis=0)
    joined = jnp.concatenate([pool_out, ret_out], axis=1)
    mixed = lax.psum_scatter(
        jnp.dot(joined, weight_local, preferred_element_type=jnp.float32).astype(jnp.bfloat16),
        "tp",
        scatter_dimension=0,
        tiled=True,
    )
    return mixed[None]


MESH = pl.DeviceIdType.MESH
ORDER = (1, 2, 0, 3)
STEPS = (
    (0, 0, 0, 10.0), (0, 0, 1, 10.7), (0, 1, 0, 14.0), (0, 1, 1, 14.7), (0, 0, 2, 15.4), (0, 1, 2, 16.1), (0, 0, 3, 16.8), (0, 1, 3, 17.5),
    (1, 0, 1, 18.2), (1, 1, 1, 18.9), (0, 2, 0, 20.3), (0, 2, 1, 21.0), (0, 2, 2, 21.7), (0, 2, 3, 22.4),
    (1, 2, 1, 23.1), (1, 0, 0, 23.8), (1, 1, 0, 24.5), (1, 2, 0, 25.2),
    (0, 3, 0, 25.9), (0, 3, 1, 26.6), (0, 3, 2, 27.3), (0, 3, 3, 28.0),
    (1, 0, 2, 28.7), (1, 1, 2, 29.4), (1, 2, 2, 30.1), (1, 0, 3, 30.8), (1, 1, 3, 31.5), (1, 2, 3, 32.2),
    (1, 3, 0, 32.9), (1, 3, 1, 33.6), (1, 3, 2, 34.3), (1, 3, 3, 35.0),
)
HOP = 2.7
NEAR = ((1, 2, 3), (0, 2, 3), (3, 1, 0), (2, 1, 0))


def places(when, needs):
    result = []
    for hop in range(4):
        due = [n for n, step in enumerate(STEPS) if step[3] + HOP * hop >= when] + [len(STEPS)]
        used = [n for n, step in enumerate(STEPS) if needs(hop, *step[:3])] + [len(STEPS)]
        result.append(min(due[0], used[0]))
    return tuple(result)


def where_am_i():
    sp, fs, tp = (lax.axis_index(name) for name in ("sp", "fs", "tp"))
    return sp, fs // 2, fs % 2, tp


def at(z, y, x, p):
    return (z, 2 * y + x, p)


def remote(src, dst, send, recv, target):
    return pltpu.make_async_remote_copy(
        src_ref=src, dst_ref=dst, send_sem=send, recv_sem=recv, device_id=target, device_id_type=MESH
    )


def piece(index, size):
    return pl.ds(pl.multiple_of(index * size, size), size)


def fused_kernel(
    tok, gain, wp, wq, wk, wv, state, pb, rb, pmap, pscale, rate, cos_t, sin_t,
    out,
    xt, xn, xg, wg, obuf, rbuf, backs, gv, st, stb, start, cosv, sinv, mapv, scv,
    krot, pool, mask, yb, yg, keep, give, take, done,
    l_sem, wl_sem, bl_sem, wy_send, wx_send, wf_send, w_recv,
    xz_send, xy_send, xp_send, x_recv,
    s_send, s_recv, b_send, b_recv, r_send, r_recv,
    h_send, c_send, y_recv, g_send, g_recv, o_send, o_recv,
):
    f32, bf = jnp.float32, jnp.bfloat16
    z, y, x, p = where_am_i()
    nz = 4
    half, width = xt.shape
    span = 2 * half
    feats = width // nz
    rows = wp.shape[0]
    group = wp.shape[1] // 2
    steps = 4 * nz
    mats = (wk, wq, wv, wp)
    fs = 2 * y + x
    me = at(z, y, x, p)
    partner = at(z, y, x, 1 - p)
    ypeer = at(z, 1 - y, x, p)
    xpeer = at(z, y, 1 - x, p)
    head = 2 * p + y

    barrier = pltpu.get_barrier_semaphore()
    others = [partner, xpeer]
    for dz in range(nz):
        for dy in range(2):
            if dz or dy:
                others.append(at((z + dz) % nz, (y + dy) % 2, x, p))
    for other in others:
        pl.semaphore_signal(barrier, inc=1, device_id=other, device_id_type=MESH)

    loads = [
        pltpu.make_async_copy(tok.at[piece(p, half)], xt, l_sem.at[0]),
        pltpu.make_async_copy(gain, gv, l_sem.at[1]),
        pltpu.make_async_copy(state, st, l_sem.at[2]),
        pltpu.make_async_copy(cos_t, cosv, l_sem.at[3]),
        pltpu.make_async_copy(sin_t, sinv, l_sem.at[4]),
        pltpu.make_async_copy(pmap.at[head], mapv, l_sem.at[5]),
        pltpu.make_async_copy(pscale.at[head], scv, l_sem.at[6]),
    ]
    for c in loads:
        c.start()
    own_w = []
    for m in range(4):
        c = pltpu.make_async_copy(mats[m].at[:, piece(y, group)], wg.at[m, piece(fs, rows)], wl_sem.at[m])
        c.start()
        own_w.append(c)
    def slot(ref, s, c, h):
        return ref.at[s, pl.ds(pl.multiple_of(c * span + h * half, half), half)]

    pl.semaphore_wait(barrier, len(others))

    sent = []

    def go(c):
        c.start()
        sent.append(c)

    def w_y(m):
        go(remote(mats[m].at[:, piece(1 - y, group)], wg.at[m, piece(fs, rows)], wy_send.at[m], w_recv.at[m, fs], ypeer))

    def w_copy_x(m):
        return remote(mats[m].at[:, piece(y, group)], wg.at[m, piece(fs, rows)], wx_send.at[m], w_recv.at[m, fs], xpeer)

    def w_x(m):
        go(w_copy_x(m))

    def w_wait(m, f):
        view = wg.at[m, piece(f, rows)]
        remote(view, view, wf_send.at[m], w_recv.at[m, f], partner).wait_recv()

    fy = 2 * (1 - y) + x

    def w_relay(m):
        w_wait(m, fy)
        view = wg.at[m, piece(fy, rows)]
        return remote(view, view, wf_send.at[m], w_recv.at[m, fy], xpeer)

    hi = z // 2
    zz = z * (1 - hi) + (3 - z) * hi
    near = [o * (1 - hi) + (3 - o) * hi for o in (1 - zz, 2, 3)]
    hop = (nz - 1 - z) * (1 - p) + z * p
    toward = at(z - 1 + 2 * p, y, x, p)
    onward = at(z + 1 - 2 * p, y, x, p)
    goal = (nz - 1) * p

    w_y(0)
    w_x(0)
    loads[0].wait()
    loads[1].wait()
    block = 16
    for i in range(half // block):
        floats = xt[i * block : (i + 1) * block, :].astype(f32)
        xn[i * block : (i + 1) * block, :] = (
            floats * lax.rsqrt(jnp.mean(floats * floats, axis=-1, keepdims=True) + eps) * gv[...]
        ).astype(bf)

    for i, c in enumerate(near):
        go(remote(xn.at[:, piece(c, feats)], slot(xg, y, z, p), xz_send.at[i], x_recv.at[y, z, p], at(c, y, x, p)))
    xg[y, pl.ds(pl.multiple_of(z * span + p * half, half), half), :] = xn[:, piece(z, feats)]

    def x_wait(s, c, h):
        view = slot(xg, s, c, h)
        remote(view, view, xp_send.at[0], x_recv.at[s, c, h], partner).wait_recv()

    def x_to_y(i, c):
        view = slot(xg, y, c, p)
        go(remote(view, view, xy_send.at[i], x_recv.at[y, c, p], ypeer))

    def x_to_partner(i, s, c):
        view = slot(xg, s, c, p)
        return remote(view, view, xp_send.at[i], x_recv.at[s, c, p], partner)

    w_y(1)
    w_x(1)
    go(remote(xn.at[:, piece(z, feats)], slot(xg, y, z, p), xp_send.at[3], x_recv.at[y, z, p], partner))
    go(remote(xn.at[:, piece(z, feats)], slot(xg, y, z, p), xy_send.at[3], x_recv.at[y, z, p], ypeer))
    w_y(2)

    loads[2].wait()
    for j in range(2):
        stb[j] = st[j].astype(bf)
    rs = st.shape[1]

    r = rate[y]
    row = lax.broadcasted_iota(jnp.int32, (span, span), 0)
    col = lax.broadcasted_iota(jnp.int32, (span, span), 1)
    gap = row - col
    for k in range(nz):
        dist = (gap + k * span).astype(f32)
        value = jnp.exp(-jnp.maximum(dist, 0.0) * r)
        mask[k] = jnp.where(dist >= 0.0, value, 0.0) if k == 0 else value
    for c in loads[3:]:
        c.wait()

    x_wait(y, near[0], p)
    x_to_y(0, near[0])
    go(x_to_partner(0, y, near[0]))
    go(w_relay(0))
    w_y(3)
    go(w_relay(1))
    w_x(2)
    own_b = []
    for b, back in enumerate((pb, rb)):
        c = pltpu.make_async_copy(back, backs.at[b, :, piece(fs, rows)], bl_sem.at[b])
        c.start()
        own_b.append(c)
    fx = 2 * y + 1 - x
    fd = 2 * (1 - y) + 1 - x

    def b_own(b, i):
        back = (pb, rb)[b]
        target = ((xpeer, ypeer), (ypeer, xpeer))[b][i]
        return remote(back, backs.at[b, :, piece(fs, rows)], b_send.at[b, i], b_recv.at[b, fs], target)

    def b_wait(b, f):
        view = backs.at[b, :, piece(f, rows)]
        remote(view, view, b_send.at[b, 2], b_recv.at[b, f], partner).wait_recv()

    def b_relay(b):
        f, second = ((fx, ypeer), (fy, xpeer))[b]
        view = backs.at[b, :, piece(f, rows)]
        return remote(view, view, b_send.at[b, 2], b_recv.at[b, f], second)

    def by_place(values):
        result = values[3]
        for h in (2, 1, 0):
            result = jnp.where(hop == h, values[h], result)
        return result

    def listed(table, n):
        words = []
        for part in (table[:16], table[16:]):
            word = sum(v << (2 * i) for i, v in enumerate(part))
            words.append(np.int32(word - 2**32 if word >= 2**31 else word))
        return lax.shift_right_logical(jnp.where(n < 16, words[0], words[1]), 2 * (n % 16)) & 3

    def step(n):
        e, m, i = (listed([entry[k] for entry in STEPS], n) for k in range(3))
        s = y + e * (1 - 2 * y)
        c = (nz - 1 - i) * (1 - p) + i * p
        at_slot = m * nz + c

        @pl.when(m == 0)
        def _():
            x_wait(s, c, 1 - p)

        acc = jnp.dot(xg[s, piece(c, span), :], wg[m], preferred_element_type=f32)
        send, recv = r_send.at[e, at_slot], r_recv.at[e, at_slot]

        @pl.when(hop == 0)
        def _():
            obuf[e, at_slot] = acc.astype(bf)

        @pl.when(hop > 0)
        def _():
            remote(rbuf.at[e, at_slot], rbuf.at[e, at_slot], send, recv, partner).wait_recv()
            obuf[e, at_slot] = (acc + rbuf[e, at_slot].astype(f32)).astype(bf)

        @pl.when(hop < nz - 1)
        def _():
            remote(obuf.at[e, at_slot], rbuf.at[e, at_slot], send, recv, toward).start()

    def w_ready(m):
        own_w[m].wait()
        w_wait(m, fx)
        w_wait(m, fd)

    def event(n, when, act):
        @pl.when(n == by_place(when))
        def _():
            act()

    def a_next(i):
        x_wait(y, near[i], p)
        view = slot(xg, y, near[i], p)
        remote(view, view, xy_send.at[i], x_recv.at[y, near[i], p], ypeer).start()
        x_to_partner(i, y, near[i]).start()

    def b_next(i, c):
        x_wait(1 - y, c, p)
        x_to_partner(4 + i, 1 - y, c).start()

    def state_out():
        for j in range(2):
            same = (z == goal) & (y == j)
            dst = start.at[y, piece(z, rs)]

            @pl.when(same)
            def _():
                pltpu.make_async_copy(stb.at[j], dst, s_recv.at[y, z]).start()

            @pl.when(jnp.logical_not(same))
            def _():
                remote(stb.at[j], dst, s_send.at[j], s_recv.at[y, z], at(goal, j, x, p)).start()

    def relay2():
        w_relay(2).start()
        w_copy_x(3).start()

    def back_own():
        for i in range(2):
            for b in range(2):
                b_own(b, i).start()

    def back_relay():
        for b in range(2):
            b_wait(b, (fx, fy)[b])
            b_relay(b).start()

    def chain(b, q, c):
        view = yg.at[b, q, c]
        return remote(view, view, c_send.at[b, q, c], y_recv.at[b, q, c], onward)

    small = group // 2

    def turned(values, c):
        cosine, sine = cosv[c * span : (c + 1) * span, :], sinv[c * span : (c + 1) * span, :]
        a, b = values[:, :small], values[:, small:]
        return a * cosine - b * sine, a * sine + b * cosine

    def hand_on(e, b, c, value):
        if e == 0:
            yg[b, y, c] = value
            chain(b, y, c).start()
        else:
            yb[b, c] = value
            remote(yb.at[b, c], yg.at[b, y, c], h_send.at[b, c], y_recv.at[b, y, c], ypeer).start()

    place = lax.broadcasted_iota(jnp.int32, (span, 1), 0)

    def turn_keys(e):
        s = y if e == 0 else 1 - y
        for k in range(nz):
            view = start.at[s, piece(k, rs)]
            remote(view, view, s_send.at[0], s_recv.at[s, k], partner).wait_recv()
        scale = group ** (-0.5)
        for c in range(nz):
            first, second = turned(obuf[e, c].astype(f32), c)
            krot[c * span : (c + 1) * span, :small] = (first * scale).astype(bf)
            krot[c * span : (c + 1) * span, small:] = (second * scale).astype(bf)

    def heads(e):
        s = y if e == 0 else 1 - y
        pool[0:HALO, :] = jnp.zeros((HALO, group), bf)
        for c in range(nz):
            pool[HALO + c * span : HALO + (c + 1) * span, :] = obuf[e, 3 * nz + c]
        window = 2 * (1 + y) * (1 + 3 * p)
        behind = (
            lax.broadcasted_iota(jnp.int32, (span, span + HALO), 0) + HALO
            - lax.broadcasted_iota(jnp.int32, (span, span + HALO), 1)
        )
        band = jnp.where((behind >= 0) & (behind < window), 1.0, 0.0).astype(bf)
        for c in ORDER:
            rq = jnp.concatenate(turned(obuf[e, nz + c].astype(f32), c), axis=-1)
            fade = jnp.exp(-((place + c * span).astype(f32) + 1.0) * r)
            acc = jnp.dot((rq * fade).astype(bf), start[s], preferred_element_type=f32)
            rq = rq.astype(bf)
            for g in range(c + 1):
                scores = lax.dot_general(
                    rq, krot[g * span : (g + 1) * span, :], (((1,), (1,)), ((), ())), preferred_element_type=f32
                )
                scores = (scores * mask[c - g]).astype(bf)
                acc += jnp.dot(scores, obuf[e, 2 * nz + g], preferred_element_type=f32)
            ret = (acc * lax.rsqrt(jnp.mean(acc * acc, axis=-1, keepdims=True) + eps)).astype(bf)
            trail = jnp.dot(band, pool[c * span : (c + 1) * span + HALO, :], preferred_element_type=f32)
            counts = jnp.minimum(window, place + c * span + 1).astype(f32)
            differ = (trail / counts - obuf[e, 3 * nz + c].astype(f32)).astype(bf)
            pooled = (jnp.dot(differ, mapv[...], preferred_element_type=f32) * scv[...]).astype(bf)
            hand_on(e, 1, c, ret)
            hand_on(e, 0, c, pooled)

    def early_heads():
        @pl.when(hop == nz - 1)
        def _():
            turn_keys(0)
            heads(0)

    def late_heads():
        @pl.when(hop == nz - 1)
        def _():
            turn_keys(1)

    done_late = 1 + max(n for n, entry in enumerate(STEPS) if entry[0] == 1 and entry[1] < 3)
    done_early = 1 + max(n for n, entry in enumerate(STEPS) if entry[0] == 0)
    events = (
        (places(0.0, lambda h, e, m, i: m == 0), lambda: w_ready(0)),
        (places(10.5, lambda h, e, m, i: e == 1 and i == h), lambda: b_next(3, z)),
        ((4, 1, 0, 0), lambda: a_next(1)),
        ((4, 1, 0, 0), lambda: a_next(2)),
        ((4, 2, 0, 0), relay2),
        ((5, 2, 0, 0), state_out),
        (places(13.5, lambda h, e, m, i: m == 1), lambda: w_ready(1)),
        (places(16.4, lambda h, e, m, i: e == 1 and i == NEAR[h][0]), lambda: b_next(0, near[0])),
        (places(18.5, lambda h, e, m, i: m == 3), lambda: w_relay(3).start()),
        (places(20.0, lambda h, e, m, i: m == 2), lambda: w_ready(2)),
        (places(22.0, lambda h, e, m, i: e == 1 and i == NEAR[h][1]), lambda: b_next(1, near[1])),
        (places(24.8, lambda h, e, m, i: e == 1 and i == NEAR[h][2]), lambda: b_next(2, near[2])),
        (places(25.2, lambda h, e, m, i: False), back_own),
        (places(25.5, lambda h, e, m, i: m == 3), lambda: w_ready(3)),
        ((done_early,) * 4, early_heads),
        ((done_late,) * 4, late_heads),
        (places(36.5, lambda h, e, m, i: False), back_relay),
    )

    def body(n, carry):
        for when, act in events:
            event(n, when, act)
        step(n)
        return carry

    lax.fori_loop(0, 2 * steps, body, 0)
    event(2 * steps, *events[-1])

    @pl.when(hop == nz - 1)
    def _():
        heads(1)

    far = nz - 1 - hop

    def arrive(b, q, c):
        view = yg.at[b, q, c]
        remote(view, view, c_send.at[b, q, c], y_recv.at[b, q, c], partner).wait_recv()

    def pass_on(b, q, c):
        arrive(b, q, c)

        @pl.when(far < nz - 1)
        def _():
            chain(b, q, c).start()

    across = backs.shape[2]

    def product(q, c):
        acc = jnp.zeros((span, across), f32)
        for b in range(2):
            acc += jnp.dot(yg[b, q, c], backs[b, piece(q, group), :], preferred_element_type=f32)
        return acc

    def early(c):
        @pl.when(far > 0)
        def _():
            for b in (1, 0):
                pass_on(b, y, c)

    def give_copy(c):
        return remote(give.at[c], take.at[c], g_send.at[c], g_recv.at[c], partner)

    def multiply(c):
        keep[c] = keep[c] + product(1 - y, c)
        give[c] = keep[c, piece(1 - p, half), :].astype(bf)
        give_copy(c).start()

    def finish(c):
        give_copy(c).wait_recv()
        done[c] = (keep[c, piece(p, half), :] + take[c].astype(f32)).astype(bf)
        dst = out.at[:, piece(z, across)]

        @pl.when(z == c)
        def _():
            pltpu.make_async_copy(done.at[c], dst, o_recv.at[z]).start()

        @pl.when(z != c)
        def _():
            remote(done.at[c], dst, o_send.at[c], o_recv.at[z], at(c, y, x, p)).start()

    for c in ORDER:
        early(c)
    for b in range(2):
        own_b[b].wait()
        b_wait(b, (fy, fx)[b])
        b_wait(b, fd)
    for c in ORDER:
        keep[c] = product(y, c)
    for i, c in enumerate(ORDER):
        for b in (1, 0):
            pass_on(b, 1 - y, c)
        multiply(c)

        @pl.when(far >= 2)
        def _():
            finish(c)

    @pl.when(far < 2)
    def _():
        for c in ORDER:
            finish(c)

    for k in range(nz):
        view = out.at[:, k * across : (k + 1) * across]
        remote(done.at[k], view, o_send.at[k], o_recv.at[k], partner).wait_recv()

        @pl.when(z != k)
        def _():
            remote(done.at[k], view, o_send.at[k], o_recv.at[k], partner).wait_send()

    @pl.when(hop > 0)
    def _():
        for b in range(2):
            for q in range(2):
                for c in range(nz):
                    chain(b, q, c).wait_send()

    @pl.when(hop == nz - 1)
    def _():
        for b in range(2):
            for c in range(nz):
                remote(yb.at[b, c], yb.at[b, c], h_send.at[b, c], y_recv.at[b, 0, c], partner).wait_send()

    @pl.when(hop < nz - 1)
    def _():
        for e in range(2):

            def drain(j, carry):
                remote(obuf.at[e, j], rbuf.at[e, j], r_send.at[e, j], r_recv.at[e, j], partner).wait_send()
                return carry

            lax.fori_loop(0, steps, drain, 0)

    for j in range(2):

        @pl.when(jnp.logical_not((z == goal) & (y == j)))
        def _():
            remote(stb.at[j], stb.at[j], s_send.at[j], s_recv.at[0, 0], partner).wait_send()

    for c in range(nz):
        give_copy(c).wait_send()
    for m in (2, 3):
        view = wg.at[m, piece(fy, rows)]
        remote(view, view, wf_send.at[m], w_recv.at[m, fy], partner).wait_send()
    for b in range(2):
        for i in range(2):
            b_own(b, i).wait_send()
        b_relay(b).wait_send()
    w_copy_x(3).wait_send()
    for i in (1, 2, 4, 5, 6, 7):
        view = slot(xg, y, z, p)
        remote(view, view, xp_send.at[i], x_recv.at[y, z, p], partner).wait_send()
    view = slot(xg, y, z, p)
    for i in (1, 2):
        remote(view, view, xy_send.at[i], x_recv.at[y, z, p], partner).wait_send()
    for c in sent:
        c.wait_send()


def rotary_tables(length, half_dim):
    inv_freq = np.float32(1.0) / np.power(
        np.float32(rope_base), np.linspace(0.0, 1.0, half_dim, dtype=np.float32)
    )
    angles = np.arange(length, dtype=np.float32)[:, None] * inv_freq[None, :].astype(np.float32)
    return np.cos(angles).astype(np.float32), np.sin(angles).astype(np.float32)


def paired(
    tokens, norm_gain, pool_proj, query_proj, key_proj, value_proj, pool_map, pool_scale,
    decay_rate, start_state, pool_back, retention_back,
):
    bf, f32 = jnp.bfloat16, jnp.float32
    nsp = lax.axis_size("sp")
    tok = tokens[0]
    span, width = tok.shape
    rows, two = pool_proj.shape
    group = two // 2
    length = nsp * span
    half = span // 2
    rs = start_state.shape[2]
    steps = 4 * nsp
    across = 4 * pool_back.shape[1]
    vm, hbm = pl.BlockSpec(memory_space=pltpu.VMEM), pl.BlockSpec(memory_space=pl.ANY)
    dma = pltpu.SemaphoreType.DMA
    cosine, sine = rotary_tables(length, group // 2)
    return pl.pallas_call(
        fused_kernel,
        out_shape=jax.ShapeDtypeStruct((half, width), bf),
        in_specs=[hbm] * 11 + [pl.BlockSpec(memory_space=pltpu.SMEM)] + [hbm] * 2,
        out_specs=hbm,
        scratch_shapes=[
            pltpu.VMEM((half, width), bf),
            pltpu.VMEM((half, width), bf),
            pltpu.VMEM((2, length, width // nsp), bf),
            pltpu.VMEM((4, 4 * rows, group), bf),
            pltpu.VMEM((2, steps, span, group), bf),
            pltpu.VMEM((2, steps, span, group), bf),
            pltpu.VMEM((2, pool_back.shape[0], across), bf),
            pltpu.VMEM((1, width), f32),
            pltpu.VMEM((2, rs, group), f32),
            pltpu.VMEM((2, rs, group), bf),
            pltpu.VMEM((2, nsp * rs, group), bf),
            pltpu.VMEM((length, group // 2), f32),
            pltpu.VMEM((length, group // 2), f32),
            pltpu.VMEM((group, group), bf),
            pltpu.VMEM((1, group), f32),
            pltpu.VMEM((length, group), bf),
            pltpu.VMEM((HALO + length, group), bf),
            pltpu.VMEM((nsp, span, span), f32),
            pltpu.VMEM((2, nsp, span, group), bf),
            pltpu.VMEM((2, 2, nsp, span, group), bf),
            pltpu.VMEM((nsp, span, across), f32),
            pltpu.VMEM((nsp, half, across), bf),
            pltpu.VMEM((nsp, half, across), bf),
            pltpu.VMEM((nsp, half, across), bf),
            dma((7,)), dma((4,)), dma((2,)), dma((4,)), dma((4,)), dma((4,)), dma((4, 4)),
            dma((3,)), dma((4,)), dma((8,)), dma((2, nsp, 2)),
            dma((2,)), dma((2, nsp)), dma((2, 3)), dma((2, 4)), dma((2, steps)), dma((2, steps)),
            dma((2, nsp)), dma((2, 2, nsp)), dma((2, 2, nsp)), dma((nsp,)), dma((nsp,)), dma((nsp,)), dma((nsp,)),
        ],
        compiler_params=pltpu.CompilerParams(collective_id=0, has_side_effects=True, vmem_limit_bytes=60 * 2**20),
        name="fused",
    )(
        tok, norm_gain[None, :], pool_proj, query_proj, key_proj, value_proj,
        start_state[0], pool_back, retention_back, pool_map,
        pool_scale.reshape(pool_map.shape[0], 1, group), decay_rate, jnp.asarray(cosine), jnp.asarray(sine),
    )[None]


def solution(mesh):
    sizes = mesh.shape
    small = sizes["sp"] == 4 and sizes["fs"] == 4 and sizes["tp"] == 2
    placed = (
        P("fs", "sp", None),
        P(),
        P(("sp", "fs"), "tp"),
        P(("sp", "fs"), "tp"),
        P(("sp", "fs"), "tp"),
        P(("sp", "fs"), "tp"),
        P(),
        P(),
        P("tp"),
        P("fs", "tp", "sp", None),
        P("tp", ("sp", "fs")),
        P("tp", ("sp", "fs")),
    )
    return jax.shard_map(
        paired if small else on_device,
        mesh=mesh,
        in_specs=placed,
        out_specs=P("fs", ("sp", "tp"), None),
        check_vma=False,
    )
```
